32 devices in a mesh: sp: 4 (over y, x), tp: 8 (over z, core).
Axes of the slice: x: 2, y: 2, z: 4, core: 2. Of those that a mesh axis runs over, the one named last changes fastest.
Arguments:
- layer_input: bfloat16 [1024, 4096], P('sp', 'tp'), may hold values from -6 to 6
- out_cotangent: bfloat16 [1024, 4096], P('sp', 'tp'), may hold values from -1.5 to 1.5
- routes: int32 [1024, 2], P('sp'), may hold values from 0 to 3, all different within a row; in each aligned block of 256 rows (0 to 255, 256 to 511, ...) at most 160 rows name the same one
- route_weights: float32 [1024, 2], P('sp'), may hold values from 0.2 to 1
- gate_proj: bfloat16 [4, 4096, 2048], P('sp', None, 'tp'), may hold values from -0.09375 to 0.09375
- up_proj: bfloat16 [4, 4096, 2048], P('sp', None, 'tp'), may hold values from -0.09375 to 0.09375
- down_proj: bfloat16 [4, 2048, 4096], P('sp', 'tp'), may hold values from -0.125 to 0.125
- out_proj: bfloat16 [4096, 4096], P(None, 'tp'), may hold values from -0.09375 to 0.09375
- mixer_output: bfloat16 [1024, 4096], P('sp', 'tp'), may hold values from -0.29882812 to 0.29882812
- queries: bfloat16 [1024, 2048], P('sp', 'tp'), may hold values from -6 to 6
- key_rows: bfloat16 [1024, 2048], P('sp', 'tp'), may hold values from -6 to 6
- value_rows: bfloat16 [1024, 4096], P('sp', 'tp'), may hold values from -0.3984375 to 0.3984375
- log_decay: float32 [1024, 2048], P('sp', 'tp'), may hold values from -1.5 to 0, as said below
- entry_state: float32 [4, 16, 128, 256], P('sp', 'tp'), may hold values from -6 to 6
Outputs:
- gate_proj_grad: bfloat16 [4, 4096, 2048], P('sp', None, 'tp')
- up_proj_grad: bfloat16 [4, 4096, 2048], P('sp', None, 'tp')
- down_proj_grad: bfloat16 [4, 2048, 4096], P('sp', 'tp')
- out_proj_grad: float32 [4096, 4096], P('sp', 'tp')
- query_grad: bfloat16 [1024, 2048], P('sp', 'tp')
- key_grad: bfloat16 [1024, 2048], P('sp', 'tp')
- value_grad: bfloat16 [1024, 4096], P('sp', 'tp')
- decay_grad: float32 [1024, 2048], P('sp', 'tp')
The draws below stay inside these ranges and needn't reach their ends.
Inputs may be any that keep to these rules, and one draw needn't show every extreme that they name: `routes`: each token names 2 different experts. Among the tokens of one index of sp no expert is named more than 160 times, and in every draw some expert is named exactly 160 times by the tokens of some index of sp. `log_decay`: every entry is negative.
All inputs are finite; a program needn't handle non-finite values.
Results may differ from the reference program's by a relative error of at most 0.022.
Values may be sent and summed in bfloat16 or wider, within the bound.
A program may use at most 128 MiB of HBM per device.

```python
import math
import jax
import jax.numpy as jnp
import numpy as np
from jax import lax

D = 4096
HEADS = 16
DK = 128
DV = 256
FF = 2048
TOP = 2
SPAN = 64
TOK_DEV = 256
EXPERTS = 4
TOKEN_COUNT = 1024
CAP = 160
N_SP = 4


def draw_log_decay(key, part):
    key_matrix = jax.random.split(jax.random.fold_in(key, 17), 7)
    channel_count = HEADS * DK
    fast_share = 0.5
    is_fast = jax.random.uniform(key_matrix[0], (channel_count,)) < fast_share
    slow_rate = jax.random.uniform(key_matrix[1], (channel_count,), minval=0.05, maxval=0.35) * (math.log(10.0) / TOKEN_COUNT)
    fast_rate = jax.random.uniform(key_matrix[2], (channel_count,), minval=1.0 / 100.0, maxval=1.0 / 30.0)
    rate = jnp.where(is_fast, fast_rate, slow_rate)
    device_blocks = TOKEN_COUNT // TOK_DEV
    device_factor = jnp.exp(jax.random.uniform(key_matrix[3], (device_blocks, 1, 1), minval=-0.7, maxval=0.7))
    rough = jax.random.uniform(key_matrix[4], (device_blocks, TOK_DEV, channel_count), minval=0.5, maxval=1.5)
    starting_offset = (rate[None, None, :] * device_factor * rough).reshape(TOKEN_COUNT, channel_count)
    group_position = jax.random.randint(key_matrix[5], (3,), 0, TOKEN_COUNT)
    group_length = jax.random.uniform(key_matrix[6], (3, channel_count), minval=0.22, maxval=0.4)
    position_index = jnp.arange(TOKEN_COUNT, dtype=jnp.int32)
    group_slot_hits = (position_index[:, None] == group_position[None, :]).astype(jnp.float32)
    token_groups = jnp.dot(group_slot_hits, group_length)
    return -(starting_offset + token_groups)


def strengthened(drawn, key, source, target, blocks, factor):
    def block_of(dim):
        return (jnp.arange(drawn.shape[dim]) // (drawn.shape[dim] // blocks)).reshape((-1,) + (1,) * (drawn.ndim - 1 - dim))

    one_side = jax.random.permutation(key, blocks)[block_of(target)]
    far = (block_of(target) + blocks // 2) % blocks
    return jnp.where((block_of(source) == one_side) | (block_of(source) == far), factor * drawn, drawn)


def level_of(key, shape, cuts, smallest, largest):
    gain, own = 1.0, jax.random.fold_in(key, 6)
    for axis_at, parts in cuts:
        heights = jnp.exp(jax.random.uniform(jax.random.fold_in(own, axis_at), (parts,), jnp.float32, smallest / len(cuts), largest / len(cuts)))
        gain = gain * jnp.repeat(heights, shape[axis_at] // parts).reshape([-1 if axis == axis_at else 1 for axis in range(len(shape))])
    return gain


def routed_block(rng, own, number, rows, count, top, limit, lean):
    ranking = jax.random.permutation(rng, count)
    packed, usual = load_shares(count, rows * top, limit, lean, True), load_shares(count, rows * top, limit, lean, False)
    places = jnp.arange(count)

    def named(lengths, turn):
        used = int((lengths > 0).sum())
        fixed = max(1, used // 4)
        moved = fixed + (places - fixed + turn * (used - fixed)) % max(1, count - fixed)
        return jnp.zeros((count,), jnp.int32).at[ranking[jnp.where(places < fixed, places, moved)]].set(jnp.asarray(lengths, jnp.int32))

    lengths = jnp.where(number % 4 == 0, named(packed, number // 4), named(usual, number - number // 4 - 1))
    mixed = jax.random.permutation(jax.random.fold_in(own, 3), count)
    giver, taker = mixed[0:count // 2 * 2:2], mixed[1:count // 2 * 2:2]
    slack = jnp.minimum(lengths[giver] - 1, limit - lengths[taker]) // 2
    slack = jnp.where((giver == ranking[0]) | (taker == ranking[0]) | (lengths[taker] == 0), 0, jnp.maximum(slack, 0))
    moved = jax.random.randint(jax.random.fold_in(own, 4), (count // 2,), 0, 1 << 20) % (slack + 1)
    lengths = lengths.at[giver].add(-moved).at[taker].add(moved)
    members = jnp.searchsorted(jnp.cumsum(lengths), jnp.arange(rows * top), side="right").astype(jnp.int32)
    listing = members.reshape(top, rows).T
    listing = listing[jax.random.permutation(jax.random.fold_in(own, 1), rows)]
    turn = jax.random.randint(jax.random.fold_in(own, 2), (rows, 1), 0, top)
    return jnp.take_along_axis(listing, (jnp.arange(top)[None, :] + turn) % top, axis=1)


def load_shares(amount, total, limit, lean, full):
    loads = [(1 << 20) // math.isqrt(rank ** lean) + 1 for rank in range(1, amount + 1)]
    largest = limit if full else min(limit, max(-(-total // amount), total * loads[0] // sum(loads)))
    least = 1 if total - largest >= amount - 1 else 0
    given, rest = [largest] + [least] * (amount - 1), total - largest - least * (amount - 1)
    while rest > 0:
        free = [i for i in range(1, amount) if given[i] < largest] or [i for i in range(1, amount) if given[i] < limit]
        whole, budget = sum([loads[i] for i in free]), rest
        for i in free:
            extra = min(limit - given[i], max(1, budget * loads[i] // whole), rest)
            given[i] = given[i] + extra
            rest = rest - extra
    return np.array(given)


def scatter_about(rng, extent, scale, limit, shards=(), kind=jnp.bfloat16):
    drawn = jax.random.normal(rng, extent, jnp.float32) * scale
    if len(shards) > 0:
        drawn = level_of(rng, extent, shards, -0.22, 0.18) * drawn
    return jnp.clip(drawn, min=-limit, max=limit).astype(kind)


def heavy_noise(stream_key, shape, scale, limit, shards, heavy, kind=jnp.bfloat16):
    result = scale * jax.random.normal(stream_key, shape, jnp.float32)
    if shards:
        result = result * level_of(stream_key, shape, shards, -0.22, 0.18)
    return jnp.clip(strengthened(result, jax.random.fold_in(stream_key, 3), *heavy), -limit, limit).astype(kind)


def setup_inputs(seed: int = 0) -> dict:
    splits = jax.random.split(jax.random.key(seed), 15)
    layer_input = scatter_about(splits[0], (TOKEN_COUNT, D), 1.0, 6.0, ((0, 4), (1, 8)))
    out_cotangent = heavy_noise(splits[1], (TOKEN_COUNT, D), 0.25, 1.5, ((0, 4), (1, 8)), (0, 1, 8, 2.0))
    routes_keys = jax.random.split(jax.random.fold_in(splits[2], 1), TOKEN_COUNT // TOK_DEV)
    routes_turns = jax.random.permutation(jax.random.fold_in(splits[2], 3), TOKEN_COUNT // TOK_DEV)
    routes = jax.vmap(lambda own, number: routed_block(jax.random.fold_in(splits[2], 2), own, number, TOK_DEV, EXPERTS, TOP, CAP, 0))(routes_keys, routes_turns).reshape((TOKEN_COUNT, TOP))
    route_weights = jnp.clip(0.2 + 0.8 * jax.random.uniform(splits[3], (TOKEN_COUNT, TOP), jnp.float32) ** level_of(splits[3], (TOKEN_COUNT, TOP), ((0, 4),), -0.2, 0.2), 0.2, 1.0)
    gate_proj = scatter_about(splits[4], (EXPERTS, D, FF), D ** -0.5, 0.09375, ((0, 4), (2, 8)))
    up_proj = scatter_about(splits[5], (EXPERTS, D, FF), D ** -0.5, 0.09375, ((0, 4), (2, 8)))
    down_proj = scatter_about(splits[6], (EXPERTS, FF, D), FF ** -0.5, 0.125, ((0, 4), (1, 8)))
    out_proj = scatter_about(splits[7], (D, HEADS * DV), (HEADS * DV) ** -0.5, 0.09375, ((1, 8),))
    mixer_output = scatter_about(splits[8], (TOKEN_COUNT, HEADS * DV), 0.05, 0.29882812, ((0, 4), (1, 8)))
    queries = scatter_about(splits[9], (TOKEN_COUNT, HEADS * DK), 1.0, 6.0, ((0, 4), (1, 8)))
    key_rows = scatter_about(splits[10], (TOKEN_COUNT, HEADS * DK), 1.0, 6.0, ((0, 4), (1, 8)))
    value_rows = scatter_about(splits[11], (TOKEN_COUNT, HEADS * DV), 0.0625, 0.3984375, ((0, 4), (1, 8)))
    log_decay = draw_log_decay(jax.random.fold_in(splits[14], 71), 0)
    entry_state = scatter_about(splits[13], (N_SP, HEADS, DK, DV), 1.0, 6.0, ((0, 4), (1, 8)), jnp.float32)
    return {"layer_input": layer_input, "out_cotangent": out_cotangent, "routes": routes, "route_weights": route_weights, "gate_proj": gate_proj, "up_proj": up_proj, "down_proj": down_proj, "out_proj": out_proj, "mixer_output": mixer_output, "queries": queries, "key_rows": key_rows, "value_rows": value_rows, "log_decay": log_decay, "entry_state": entry_state}


PRECISION_LEVEL = lax.Precision.HIGHEST


def expert_backward(inputs, pair_grad, gate_weight, up_weight, down_weight):
    gate_pre = jnp.dot(inputs, gate_weight, preferred_element_type=jnp.float32)
    up_pre = jnp.dot(inputs, up_weight, preferred_element_type=jnp.float32)
    sigmoid_gate = jax.nn.sigmoid(gate_pre)
    activated = gate_pre * sigmoid_gate
    hidden = (activated * up_pre).astype(jnp.bfloat16)
    down_grad = jnp.dot(hidden.T, pair_grad, preferred_element_type=jnp.float32)
    hidden_grad = jnp.dot(pair_grad, down_weight.T, preferred_element_type=jnp.float32)
    gate_delta = (hidden_grad * up_pre * sigmoid_gate * (1.0 + gate_pre * (1.0 - sigmoid_gate))).astype(jnp.bfloat16)
    up_delta = (hidden_grad * activated).astype(jnp.bfloat16)
    gate_grad = jnp.dot(inputs.T, gate_delta, preferred_element_type=jnp.float32)
    up_grad = jnp.dot(inputs.T, up_delta, preferred_element_type=jnp.float32)
    input_grad = jnp.dot(gate_delta, gate_weight.T, preferred_element_type=jnp.float32)
    input_grad = input_grad + jnp.dot(up_delta, up_weight.T, preferred_element_type=jnp.float32)
    return gate_grad.astype(jnp.bfloat16), up_grad.astype(jnp.bfloat16), down_grad.astype(jnp.bfloat16), input_grad


def slot_table(routes):
    blocks = routes.reshape(N_SP, TOK_DEV * TOP).astype(jnp.int32)
    expert_ids = jnp.arange(EXPERTS, dtype=jnp.int32)

    def block_rank(pair_ids):
        onehot = (pair_ids[:, None] == expert_ids[None, :]).astype(jnp.int32)
        return jnp.sum((jnp.cumsum(onehot, axis=0) - onehot) * onehot, axis=1)

    slot_rank = jax.vmap(block_rank)(blocks)
    source = jnp.arange(N_SP, dtype=jnp.int32)[:, None]
    row_pos = (source * CAP + slot_rank).astype(jnp.int32)
    pair_index = (source * (TOK_DEV * TOP) + jnp.arange(TOK_DEV * TOP, dtype=jnp.int32)[None, :]).astype(jnp.int32)
    table = jnp.full((EXPERTS, N_SP * CAP), TOKEN_COUNT * TOP, dtype=jnp.int32)
    return table.at[blocks, row_pos].set(pair_index)


def forward_block(passed_state, block_data):
    scaled_q, key_segment, value_segment, decays, output_gradient = block_data
    position_index = decays.shape[0]
    causal = jnp.tril(jnp.ones((position_index, position_index), dtype=bool))
    running_decay = jnp.cumsum(decays, axis=0)
    growth_multiplier = jnp.exp(running_decay)
    shrink = jnp.exp(-running_decay)
    block_overall_sum = running_decay[-1]
    value_dots = jnp.where(causal[None], jnp.einsum('thv,shv->hts', output_gradient, value_segment, precision=PRECISION_LEVEL), 0.0)
    state_contribution = growth_multiplier * jnp.einsum('gxb,xqb->gxq', output_gradient, passed_state, precision=PRECISION_LEVEL)
    inside = growth_multiplier * jnp.einsum('hts,shk->thk', value_dots, key_segment * shrink, precision=PRECISION_LEVEL)
    state_update = jnp.einsum('rsx,rse->sxe', key_segment * jnp.exp(block_overall_sum - running_decay), value_segment, precision=PRECISION_LEVEL)
    return jnp.exp(block_overall_sum)[:, :, None] * passed_state + state_update, state_contribution + inside


def reverse_block(passed_state, block_data):
    scaled_q, key_segment, value_segment, decays, output_gradient = block_data
    position_index = decays.shape[0]
    causal = jnp.tril(jnp.ones((position_index, position_index), dtype=bool))
    running_decay = jnp.cumsum(decays, axis=0)
    growth_multiplier = jnp.exp(running_decay)
    shrink = jnp.exp(-running_decay)
    block_overall_sum = running_decay[-1]
    decay_remaining = jnp.exp(block_overall_sum - running_decay)
    value_dots = jnp.where(causal[None], jnp.einsum('thv,shv->hts', output_gradient, value_segment, precision=PRECISION_LEVEL), 0.0)
    query_raised = scaled_q * growth_multiplier
    key_portion = decay_remaining * jnp.einsum('gxb,xqb->gxq', value_segment, passed_state, precision=PRECISION_LEVEL)
    key_portion = key_portion + shrink * jnp.einsum('hts,thk->shk', value_dots, query_raised, precision=PRECISION_LEVEL)
    scores = jnp.where(causal[None], jnp.einsum('thk,shk->hts', query_raised, key_segment * shrink, precision=PRECISION_LEVEL), 0.0)
    value_portion = jnp.einsum('qgy,gye->qge', key_segment * decay_remaining, passed_state, precision=PRECISION_LEVEL)
    value_portion = value_portion + jnp.einsum('hts,thv->shv', scores, output_gradient, precision=PRECISION_LEVEL)
    prior_steps = jnp.einsum('rsx,rse->sxe', query_raised, output_gradient, precision=PRECISION_LEVEL) + jnp.exp(block_overall_sum)[:, :, None] * passed_state
    return prior_steps, (key_portion, value_portion)


def mixer_backward(queries, key_rows, value_rows, log_decay, entry_state, mix_grad):
    blocks = TOK_DEV // SPAN

    def split(rows, width):
        return rows.astype(jnp.float32).reshape(N_SP, blocks, SPAN, HEADS, width)

    scaled_q = split(queries, DK) * (DK ** -0.5)
    key_segment = split(key_rows, DK)
    value_segment = split(value_rows, DV)
    decays = split(log_decay, DK)
    output_gradient = split(mix_grad, DV)

    def per_device(device_data):
        return lax.scan(forward_block, device_data[0], device_data[1:])[1]

    query_part = lax.map(per_device, (entry_state.astype(jnp.float32), scaled_q, key_segment, value_segment, decays, output_gradient))

    def joined(rows):
        return rows.reshape(N_SP * blocks, SPAN, HEADS, rows.shape[-1])

    start = jnp.zeros((HEADS, DK, DV), dtype=jnp.float32)
    sequence = (joined(scaled_q), joined(key_segment), joined(value_segment), joined(decays), joined(output_gradient))
    _, (key_portion, value_portion) = lax.scan(reverse_block, start, sequence, reverse=True)
    query_flat = query_part.reshape(TOKEN_COUNT, HEADS, DK)
    key_flattened = key_portion.reshape(TOKEN_COUNT, HEADS, DK)
    change = scaled_q.reshape(TOKEN_COUNT, HEADS, DK) * query_flat - key_segment.reshape(TOKEN_COUNT, HEADS, DK) * key_flattened
    decay_grad = lax.cumsum(change, axis=0, reverse=True).reshape(TOKEN_COUNT, HEADS * DK)
    query_grad = (query_flat * (DK ** -0.5)).reshape(TOKEN_COUNT, HEADS * DK).astype(jnp.bfloat16)
    key_grad = key_flattened.reshape(TOKEN_COUNT, HEADS * DK).astype(jnp.bfloat16)
    value_grad = value_portion.reshape(TOKEN_COUNT, HEADS * DV).astype(jnp.bfloat16)
    return query_grad, key_grad, value_grad, decay_grad


def reference(layer_input, out_cotangent, routes, route_weights, gate_proj, up_proj, down_proj, out_proj,
              mixer_output, queries, key_rows, value_rows, log_decay, entry_state):
    table = slot_table(routes)
    input_pad = jnp.concatenate([layer_input, jnp.zeros((1, D), dtype=layer_input.dtype)], axis=0)
    grad_pad = jnp.concatenate([out_cotangent.astype(jnp.float32), jnp.zeros((1, D), dtype=jnp.float32)], axis=0)
    weight_pad = jnp.concatenate([route_weights.reshape(-1).astype(jnp.float32), jnp.zeros((1,), dtype=jnp.float32)])

    def one_expert(expert_data):
        pair_ids, gate_weight, up_weight, down_weight = expert_data
        token_ids = (pair_ids // TOP).astype(jnp.int32)
        inputs = input_pad[token_ids]
        pair_grad = (weight_pad[pair_ids][:, None] * grad_pad[token_ids]).astype(jnp.bfloat16)
        return expert_backward(inputs, pair_grad, gate_weight, up_weight, down_weight)

    gate_proj_grad, up_proj_grad, down_proj_grad, row_grads = lax.map(one_expert, (table, gate_proj, up_proj, down_proj))
    token_ids = (table // TOP).astype(jnp.int32).reshape(-1)
    moe_grad = jnp.zeros((TOKEN_COUNT + 1, D), dtype=jnp.float32).at[token_ids].add(row_grads.reshape(-1, D))
    token_grad = (out_cotangent.astype(jnp.float32) + moe_grad[:TOKEN_COUNT]).astype(jnp.bfloat16)
    mix_grad = jnp.dot(token_grad, out_proj, preferred_element_type=jnp.float32).astype(jnp.bfloat16)
    out_proj_grad = jnp.dot(token_grad.T, mixer_output, preferred_element_type=jnp.float32)
    query_grad, key_grad, value_grad, decay_grad = mixer_backward(queries, key_rows, value_rows, log_decay, entry_state, mix_grad)
    return (gate_proj_grad, up_proj_grad, down_proj_grad, out_proj_grad, query_grad, key_grad, value_grad, decay_grad)
```

```python
import functools

import jax
import jax.numpy as jnp
from jax import lax
from jax.experimental import pallas as pl
from jax.experimental.pallas import tpu as pltpu
from jax.sharding import PartitionSpec as P

SPAN = 64
MESH = pl.DeviceIdType.MESH


PRECISION_LEVEL = lax.Precision.HIGH


def entering(value, axis, join, neutral, kept=None):
    count = lax.axis_size(axis)
    place = lax.axis_index(axis)
    ahead = count - 1 - place
    if kept is None:
        kept = lax.all_gather(value[0].astype(jnp.bfloat16), axis)
    gathered = (kept, lax.all_gather(value[1].astype(jnp.bfloat16), axis))
    state = jax.tree.map(lambda a, e: jnp.zeros_like(a) + jnp.asarray(e, a.dtype), value, neutral)

    def one(lap, state):
        source = count - 1 - lap
        return join(
            state,
            jax.tree.map(
                lambda a, own: lax.dynamic_index_in_dim(a, source, 0, False).astype(own.dtype),
                gathered,
                value,
            ),
        )

    return lax.fori_loop(0, ahead, one, state)


def prefix(value, axis, join, neutral):
    count, mine = (lax.axis_size(axis), lax.axis_index(axis))
    pieces = lax.all_gather(value, axis)
    pieces = pieces[::-1]
    mine = count - 1 - mine
    subtotal = jnp.full_like(value, 0) + jnp.asarray(neutral, value.dtype)

    def lap(position, subtotal):
        longer = join(subtotal, pieces[position])
        return jnp.where(position < mine, longer, subtotal)

    return lax.fori_loop(0, count - 1, lap, subtotal)


def route_tables(routes, route_weights, experts, capacity):
    tokens = routes.shape[0]
    top_count = routes.shape[1]
    pair_ids = routes.reshape(-1)
    expert_ids = jnp.arange(experts, dtype=jnp.int32)
    onehot = (pair_ids[:, None] == expert_ids[None, :]).astype(jnp.int32)
    slot_rank = jnp.sum((jnp.cumsum(onehot, axis=0) - onehot) * onehot, axis=1)
    target = pair_ids * capacity + slot_rank
    slot_ids = jnp.arange(experts * capacity, dtype=jnp.int32)
    slot_hits = (
        (target[:, None] == slot_ids[None, :])
        .astype(jnp.float32)
        .reshape(tokens, top_count, experts * capacity)
    )
    placed = jnp.sum(slot_hits, axis=1)
    weighted = jnp.einsum("tk,tkp->tp", route_weights, slot_hits, precision=PRECISION_LEVEL)
    return (placed, weighted)


def expert_backward(inputs, pair_grad, gate_proj, up_proj, down_proj):
    gate_pre = jnp.einsum("erd,edf->erf", inputs, gate_proj, preferred_element_type=jnp.float32)
    up_pre = jnp.einsum("erd,edf->erf", inputs, up_proj, preferred_element_type=jnp.float32)
    sigmoid_gate = jax.nn.sigmoid(gate_pre)
    activated = gate_pre * sigmoid_gate
    hidden = (activated * up_pre).astype(jnp.bfloat16)
    down_grad = jnp.einsum("erf,erd->efd", hidden, pair_grad, preferred_element_type=jnp.float32)
    hidden_grad = jnp.einsum(
        "erd,efd->erf", pair_grad, down_proj, preferred_element_type=jnp.float32
    )
    gate_delta = (
        hidden_grad * up_pre * sigmoid_gate * (1.0 + gate_pre * (1.0 - sigmoid_gate))
    ).astype(jnp.bfloat16)
    up_delta = (hidden_grad * activated).astype(jnp.bfloat16)
    gate_grad = jnp.einsum("erd,erf->edf", inputs, gate_delta, preferred_element_type=jnp.float32)
    up_grad = jnp.einsum("erd,erf->edf", inputs, up_delta, preferred_element_type=jnp.float32)
    return (gate_grad, up_grad, down_grad, gate_delta, up_delta)


def input_rows(gate_delta, up_delta, gate_weight, up_weight):
    input_grad = jnp.einsum(
        "erf,edf->erd", gate_delta, gate_weight, preferred_element_type=jnp.float32
    )
    return input_grad + jnp.einsum(
        "erf,edf->erd", up_delta, up_weight, preferred_element_type=jnp.float32
    )


def state_combine(prior_steps, later):
    return (prior_steps[0] * later[0], later[1] + later[0][:, :, None] * prior_steps[1])


def add_combine(prior_steps, later):
    return prior_steps + later


def mixer_backward(queries, key_rows, value_rows, log_decay, entry, mix_grad, kept=None):
    tokens = queries.shape[0]
    heads = entry.shape[0]
    key_width = entry.shape[1]
    value_width = entry.shape[2]
    blocks = tokens // SPAN
    causal = jnp.tril(jnp.ones((SPAN, SPAN), dtype=bool))

    def split(rows, width):
        return rows.astype(jnp.float32).reshape(blocks, SPAN, heads, width)

    scaled_q = split(queries, key_width) * key_width ** (-0.5)
    key_segment = split(key_rows, key_width)
    value_segment = split(value_rows, value_width)
    decays = split(log_decay, key_width)
    output_gradient = split(mix_grad, value_width)
    value_dots = jnp.where(
        causal[None, None],
        jnp.einsum("nthv,nshv->nhts", output_gradient, value_segment, precision=PRECISION_LEVEL),
        0.0,
    )

    def forward_block(passed_state, block_data):
        query_now, current_key, current_value, decay_now, current_gradient, dots_now = block_data
        running_decay = jnp.cumsum(decay_now, axis=0)
        growth_multiplier = jnp.exp(running_decay)
        block_overall_sum = running_decay[-1]
        state_contribution = growth_multiplier * jnp.einsum(
            "gxb,xqb->gxq", current_gradient, passed_state, precision=PRECISION_LEVEL
        )
        inside = growth_multiplier * jnp.einsum(
            "hts,shk->thk",
            dots_now,
            current_key * jnp.exp(-running_decay),
            precision=PRECISION_LEVEL,
        )
        state_update = jnp.einsum(
            "rsx,rse->sxe",
            current_key * jnp.exp(block_overall_sum - running_decay),
            current_value,
            precision=PRECISION_LEVEL,
        )
        return (
            jnp.exp(block_overall_sum)[:, :, None] * passed_state + state_update,
            state_contribution + inside,
        )

    def reverse_block(passed_state, block_data):
        query_now, current_key, current_value, decay_now, current_gradient, dots_now = block_data
        running_decay = jnp.cumsum(decay_now, axis=0)
        shrink = jnp.exp(-running_decay)
        block_overall_sum = running_decay[-1]
        decay_remaining = jnp.exp(block_overall_sum - running_decay)
        query_raised = query_now * jnp.exp(running_decay)
        key_portion = decay_remaining * jnp.einsum(
            "gxb,xqb->gxq", current_value, passed_state, precision=PRECISION_LEVEL
        )
        key_portion = key_portion + shrink * jnp.einsum(
            "hts,thk->shk", dots_now, query_raised, precision=PRECISION_LEVEL
        )
        scores = jnp.where(
            causal[None],
            jnp.einsum(
                "thk,shk->hts", query_raised, current_key * shrink, precision=PRECISION_LEVEL
            ),
            0.0,
        )
        value_portion = jnp.einsum(
            "qgy,gye->qge", current_key * decay_remaining, passed_state, precision=PRECISION_LEVEL
        )
        value_portion = value_portion + jnp.einsum(
            "hts,thv->shv", scores, current_gradient, precision=PRECISION_LEVEL
        )
        prior_steps = (
            jnp.einsum("rsx,rse->sxe", query_raised, current_gradient, precision=PRECISION_LEVEL)
            + jnp.exp(block_overall_sum)[:, :, None] * passed_state
        )
        return (prior_steps, (key_portion, value_portion))

    block_inputs = (scaled_q, key_segment, value_segment, decays, output_gradient, value_dots)
    _, query_part = lax.scan(forward_block, entry, block_inputs)
    empty_state = jnp.zeros((heads, key_width, value_width), dtype=jnp.float32)
    local_start, (key_portion, value_portion) = lax.scan(
        reverse_block, empty_state, block_inputs, reverse=True
    )
    scaled_flat = scaled_q.reshape(tokens, heads, key_width)
    key_flattened = key_segment.reshape(tokens, heads, key_width)
    value_flattened = value_segment.reshape(tokens, heads, value_width)
    query_flat = query_part.reshape(tokens, heads, key_width)
    local_key = key_portion.reshape(tokens, heads, key_width)
    running_decay = jnp.cumsum(decays.reshape(tokens, heads, key_width), axis=0)
    device_total = running_decay[-1]
    decay_remaining = jnp.exp(device_total - running_decay)
    retain = jnp.exp(device_total)
    ones_head = jnp.ones((heads, key_width), dtype=jnp.float32)
    zeros_head = jnp.zeros((heads, key_width), dtype=jnp.float32)
    scanned = entering((retain, local_start), "sp", state_combine, (ones_head, empty_state), kept)
    following_state = scanned[1]
    key_full = local_key + decay_remaining * jnp.einsum(
        "gxb,xqb->gxq", value_flattened, following_state, precision=PRECISION_LEVEL
    )
    value_full = value_portion.reshape(tokens, heads, value_width)
    value_full = value_full + jnp.einsum(
        "qgy,gye->qge", key_flattened * decay_remaining, following_state, precision=PRECISION_LEVEL
    )
    change = scaled_flat * query_flat - key_flattened * key_full
    later_sum = prefix(jnp.sum(change, axis=0), "sp", add_combine, zeros_head)
    decay_grad = (lax.cumsum(change, axis=0, reverse=True) + later_sum[None]).reshape(
        tokens, heads * key_width
    )
    query_grad = (
        (query_flat * key_width ** (-0.5)).reshape(tokens, heads * key_width).astype(jnp.bfloat16)
    )
    key_grad = key_full.reshape(tokens, heads * key_width).astype(jnp.bfloat16)
    value_grad = value_full.reshape(tokens, heads * value_width).astype(jnp.bfloat16)
    return (query_grad, key_grad, value_grad, decay_grad)


def peers(nz):
    s = lax.axis_index("sp")
    t = lax.axis_index("tp")
    y, x = s // 2, s % 2
    z, c = t // 2, t % 2
    return s, (1 - y) * 2 + x, y * 2 + 1 - x, (1 - y) * 2 + 1 - x, z, c


def greet(devices):
    barrier = pltpu.get_barrier_semaphore()
    for device in devices:
        pl.semaphore_signal(barrier, inc=1, device_id=device, device_id_type=MESH)
    pl.semaphore_wait(barrier, len(devices))


def at(s, t):
    return {"sp": s, "tp": t}


def gather_kernel(
    nz,
    x_ref,
    g_ref,
    w_ref,
    wg_ref,
    wu_ref,
    xo,
    go,
    wo,
    wgo,
    wuo,
    z_send,
    z_recv,
    p_send,
    p_recv,
    d_send,
    d_recv,
    w_send,
    w_recv,
    t_send,
    t_recv,
    own_sem,
):
    s, sy, sx, sd, z, c = peers(nz)
    me, partner = z * 2 + c, z * 2 + 1 - c
    greet(
        [at(s, lax.rem(z + d, nz) * 2 + c) for d in range(1, nz)]
        + [at(sy, me), at(sx, me), at(sd, me), at(s, partner)]
    )
    sources, outs = (x_ref, g_ref), (xo, go)
    first, second = (sy, sx), (sx, sy)
    sent = []

    def copy(src, dst, send, recv, device):
        return pltpu.make_async_remote_copy(
            src_ref=src, dst_ref=dst, send_sem=send, recv_sem=recv, device_id=device, device_id_type=MESH
        )

    def start(*parts):
        made = copy(*parts)
        made.start()
        sent.append(made)

    def column(k):
        return lax.rem(z + k, nz) * 2 + c

    def source(a, k):
        return sources[a] if k == 0 else outs[a].at[s, column(k)]

    def plane(a, k, j, src, row, target):
        start(
            src,
            outs[a].at[row, column(k)],
            p_send.at[a, k, j],
            p_recv.at[a, k, j],
            at(target, me),
        )

    def arrived(a, k, j, row):
        slot = outs[a].at[row, column(k)]
        copy(slot, slot, p_send.at[a, k, j], p_recv.at[a, k, j], at(s, partner)).wait_recv()
        return slot

    def across(a, k, j, src, row):
        start(
            src,
            outs[a].at[row, column(k)],
            d_send.at[a, k, j],
            d_recv.at[a, k, j],
            at(s, partner),
        )

    def open_step(k):
        if k:
            for a in range(2):
                slot = outs[a].at[s, column(k)]
                copy(slot, slot, z_send.at[a, k - 1], z_recv.at[a, k - 1], at(s, partner)).wait_recv()
        for a in range(2):
            plane(a, k, 0, source(a, k), s, first[a])
        for a in range(2):
            plane(a, k, 1, source(a, k), s, second[a])
        for a in range(2):
            across(a, k, 0, source(a, k), s)

    def middle_step(k):
        for a in range(2):
            slot = arrived(a, k, 0, first[a])
            plane(a, k, 2, slot, first[a], second[a])
            across(a, k, 1, slot, first[a])

    def close_step(k):
        for a in range(2):
            across(a, k, 2, arrived(a, k, 1, second[a]), second[a])
        for a in range(2):
            across(a, k, 3, arrived(a, k, 2, sd), sd)

    for j, target in enumerate((sy, sx, sd)):
        start(w_ref, wo.at[s], w_send.at[j], w_recv.at[j], at(target, me))
    open_step(0)
    for d in range(1, nz):
        for a in range(2):
            start(
                sources[a],
                outs[a].at[s, me],
                z_send.at[a, d - 1],
                z_recv.at[a, d - 1],
                at(s, lax.rem(z + nz - d, nz) * 2 + c),
            )
    local = [
        pltpu.make_async_copy(x_ref, xo.at[s, me], own_sem.at[0]),
        pltpu.make_async_copy(g_ref, go.at[s, me], own_sem.at[1]),
        pltpu.make_async_copy(w_ref, wo.at[s], own_sem.at[2]),
    ]
    for one in local:
        one.start()
    for k in range(nz):
        for i, (src, dst) in enumerate(((wg_ref, wgo), (wu_ref, wuo))):
            start(src.at[k, 1 - c], dst.at[k], t_send.at[i, k], t_recv.at[i, k], at(s, partner))
    middle_step(0)
    for k in range(1, nz):
        open_step(k)
        close_step(k - 1)
        middle_step(k)
    close_step(nz - 1)
    for j, row in enumerate((sy, sx, sd)):
        slot = wo.at[row]
        copy(slot, slot, w_send.at[j], w_recv.at[j], at(s, partner)).wait_recv()
    for k in range(nz):
        for i, dst in enumerate((wgo, wuo)):
            slot = dst.at[k]
            copy(slot, slot, t_send.at[i, k], t_recv.at[i, k], at(s, partner)).wait_recv()
        for a in range(2):
            for j, row in enumerate((s, first[a], second[a], sd)):
                slot = outs[a].at[row, lax.rem(z + k, nz) * 2 + 1 - c]
                copy(slot, slot, d_send.at[a, k, j], d_recv.at[a, k, j], at(s, partner)).wait_recv()
    for one in sent:
        one.wait_send()
    for one in local:
        one.wait()


def gather_all(layer_input, out_cotangent, table, gate_rows, up_rows):
    nz = gate_rows.shape[0]
    rows, columns = layer_input.shape
    n_sp = lax.axis_size("sp")
    dma = pltpu.SemaphoreType.DMA
    vmem = pl.BlockSpec(memory_space=pltpu.VMEM)
    anywhere = pl.BlockSpec(memory_space=pl.ANY)
    tokens = jax.ShapeDtypeStruct((n_sp, 2 * nz, rows, columns), layer_input.dtype)
    halves = jax.ShapeDtypeStruct((nz,) + gate_rows.shape[2:], gate_rows.dtype)
    return pl.pallas_call(
        functools.partial(gather_kernel, nz),
        out_shape=(
            tokens,
            tokens,
            jax.ShapeDtypeStruct((n_sp,) + table.shape, table.dtype),
            halves,
            halves,
        ),
        in_specs=[vmem, vmem, vmem, anywhere, anywhere],
        out_specs=(anywhere,) * 5,
        scratch_shapes=[
            dma((2, nz - 1)),
            dma((2, nz - 1)),
            dma((2, nz, 3)),
            dma((2, nz, 3)),
            dma((2, nz, 4)),
            dma((2, nz, 4)),
            dma((3,)),
            dma((3,)),
            dma((2, nz)),
            dma((2, nz)),
            dma((3,)),
        ],
        compiler_params=pltpu.CompilerParams(collective_id=0, has_side_effects=True),
        name="gather_all",
    )(layer_input, out_cotangent, table, gate_rows, up_rows)


def dots(left, right, left_dim, right_dim):
    return lax.dot_general(
        left, right, (((left_dim,), (right_dim,)), ((), ())), preferred_element_type=jnp.float32
    )


def hidden_kernel(
    x_ref, g_ref, w_ref, wg_ref, wu_ref, wd_ref, gd, ud, gdt, udt, ht, gate, up, back
):
    step = pl.program_id(0)
    rows = gate.shape[0]
    columns = x_ref.shape[-1]

    @pl.when(step == 0)
    def _():
        for total in (gate, up, back):
            total[...] = jnp.zeros_like(total)

    x = x_ref[...].reshape(rows, columns)
    pair = (w_ref[...] * g_ref[...].reshape(rows, columns).astype(jnp.float32)).astype(jnp.bfloat16)
    gate[...] += dots(x, wg_ref[...], 1, 0)
    up[...] += dots(x, wu_ref[...], 1, 0)
    back[...] += dots(pair, wd_ref[...], 1, 1)

    @pl.when(step == pl.num_programs(0) - 1)
    def _():
        gate_pre, up_pre, grad = gate[...], up[...], back[...]
        sigmoid_gate = jax.nn.sigmoid(gate_pre)
        activated = gate_pre * sigmoid_gate
        gate_delta = grad * up_pre * sigmoid_gate * (1.0 + gate_pre * (1.0 - sigmoid_gate))
        up_delta = grad * activated
        gd[...] = gate_delta.astype(jnp.bfloat16)
        ud[...] = up_delta.astype(jnp.bfloat16)
        gdt[...] = gate_delta.T.astype(jnp.bfloat16)
        udt[...] = up_delta.T.astype(jnp.bfloat16)
        ht[...] = (activated * up_pre).T.astype(jnp.bfloat16)


def token_spec(tokens):
    return pl.BlockSpec((tokens.shape[0], 1) + tokens.shape[2:], lambda t: (0, t, 0, 0))


def fixed_spec(shape):
    return pl.BlockSpec(shape, lambda t: (0,) * len(shape))


def hidden_deltas(x, g, weight, gate_w, up_w, down_w):
    n_sp, tp, rows, columns = x.shape
    total, hidden = n_sp * rows, gate_w.shape[1]
    tall = jax.ShapeDtypeStruct((total, hidden), jnp.bfloat16)
    wide = jax.ShapeDtypeStruct((hidden, total), jnp.bfloat16)
    down_spec = pl.BlockSpec((hidden, columns), lambda t: (0, t))
    row_spec = pl.BlockSpec((columns, hidden), lambda t: (t, 0))
    return pl.pallas_call(
        hidden_kernel,
        grid=(tp,),
        out_shape=(tall, tall, wide, wide, wide),
        in_specs=[token_spec(x), token_spec(g), fixed_spec((total, 1)), row_spec, row_spec, down_spec],
        out_specs=[fixed_spec(tall.shape)] * 2 + [fixed_spec(wide.shape)] * 3,
        scratch_shapes=[pltpu.VMEM((total, hidden), jnp.float32)] * 3,
        cost_estimate=pl.CostEstimate(
            flops=6 * total * hidden * tp * columns, bytes_accessed=4 * x.size, transcendentals=0
        ),
        name="hidden_deltas",
    )(x, g, weight, gate_w, up_w, down_w)


def weight_kernel(x_ref, g_ref, w_ref, gdt, udt, ht, gate_out, up_out, down_out):
    rows = w_ref.shape[0]
    columns = x_ref.shape[-1]
    x = x_ref[...].reshape(rows, columns)
    pair = (w_ref[...] * g_ref[...].reshape(rows, columns).astype(jnp.float32)).astype(jnp.bfloat16)
    gate_out[...] = dots(gdt[...], x, 1, 0).T.astype(jnp.bfloat16)
    up_out[...] = dots(udt[...], x, 1, 0).T.astype(jnp.bfloat16)
    down_out[...] = dots(ht[...], pair, 1, 0).astype(jnp.bfloat16)


def weight_grads(x, g, weight, gdt, udt, ht):
    n_sp, tp, rows, columns = x.shape
    total, hidden = n_sp * rows, gdt.shape[0]
    tall = jax.ShapeDtypeStruct((tp * columns, hidden), jnp.bfloat16)
    wide = jax.ShapeDtypeStruct((hidden, tp * columns), jnp.bfloat16)
    row_spec = pl.BlockSpec((columns, hidden), lambda t: (t, 0))
    return pl.pallas_call(
        weight_kernel,
        grid=(tp,),
        out_shape=(tall, tall, wide),
        in_specs=[token_spec(x), token_spec(g), fixed_spec((total, 1))] + [fixed_spec(gdt.shape)] * 3,
        out_specs=[row_spec, row_spec, pl.BlockSpec((hidden, columns), lambda t: (0, t))],
        cost_estimate=pl.CostEstimate(
            flops=6 * total * hidden * tp * columns, bytes_accessed=4 * x.size, transcendentals=0
        ),
        name="weight_grads",
    )(x, g, weight, gdt, udt, ht)


def reduce_kernel(
    nz,
    gd,
    ud,
    wg,
    wu,
    wgp,
    wup,
    g_ref,
    out,
    other,
    s1,
    r1,
    keep,
    s2,
    r2,
    zs,
    zr,
    o_send,
    o_recv,
    a_send,
    a_recv,
    b_send,
    b_recv,
    z_send,
    z_recv,
):
    s, sy, sx, sd, z, c = peers(nz)
    me, partner = z * 2 + c, z * 2 + 1 - c
    rows = g_ref.shape[0]
    half = rows // 2
    greet(
        [at(s, lax.rem(z + d, nz) * 2 + c) for d in range(1, nz)]
        + [at(sy, me), at(sx, me), at(s, partner)]
    )
    sent = []

    def start(src, dst, send, recv, device):
        made = pltpu.make_async_remote_copy(
            src_ref=src, dst_ref=dst, send_sem=send, recv_sem=recv, device_id=device, device_id_type=MESH
        )
        made.start()
        sent.append(made)
        return made

    swaps = [
        start(ref, other.at[i], o_send.at[i], o_recv.at[i], at(s, partner))
        for i, ref in enumerate((gd, ud))
    ]
    for one in swaps:
        one.wait_recv()
    first, second = (sy, sx), (sx, sy)
    outgoing, crossing, final = {}, {}, {}

    def compute(k):
        column = lax.rem(z + nz - k, nz)
        weights = (wg[column, c], wu[column, c], wgp[column], wup[column])
        for i, q in enumerate((s, sy, sx, sd)):
            span = pl.ds(pl.multiple_of(q * rows, rows), rows)
            lefts = (gd[span, :], ud[span, :], other[0, span, :], other[1, span, :])
            tile = dots(lefts[0], weights[0], 1, 1)
            for left, weight in zip(lefts[1:], weights[1:]):
                tile = tile + dots(left, weight, 1, 1)
            for a in range(2):
                part = tile[a * half : (a + 1) * half]
                if i == 0:
                    keep[k, a, 0] = part
                elif i == 3:
                    s1[k, a, 1] = part.astype(jnp.bfloat16)
                elif i == 1 + a:
                    s1[k, a, 0] = part.astype(jnp.bfloat16)
                else:
                    keep[k, a, 1] = part
        for a in range(2):
            outgoing[k, a] = start(
                s1.at[k, a], r1.at[k, a], a_send.at[k, a], a_recv.at[k, a], at(first[a], me)
            )

    def middle(k):
        for a in range(2):
            outgoing[k, a].wait_recv()
            s2[k, a] = (keep[k, a, 1] + r1[k, a, 1].astype(jnp.float32)).astype(jnp.bfloat16)
            crossing[k, a] = start(
                s2.at[k, a], r2.at[k, a], b_send.at[k, a], b_recv.at[k, a], at(second[a], me)
            )

    def close(k):
        for a in range(2):
            crossing[k, a].wait_recv()
            total = (
                keep[k, a, 0]
                + r1[k, a, 0].astype(jnp.float32)
                + r2[k, a].astype(jnp.float32)
            )
            if k:
                zs[k - 1, a * half : (a + 1) * half] = total.astype(jnp.bfloat16)
            else:
                keep[k, a, 0] = total
        if k:
            final[k] = start(
                zs.at[k - 1],
                zr.at[k - 1],
                z_send.at[k - 1],
                z_recv.at[k - 1],
                at(s, lax.rem(z + nz - k, nz) * 2 + c),
            )

    order = list(range(1, nz)) + [0]
    for i in range(nz + 2):
        if i < nz:
            compute(order[i])
        if 0 <= i - 2 < nz:
            close(order[i - 2])
        if 0 <= i - 1 < nz:
            middle(order[i - 1])
    for k in range(1, nz):
        final[k].wait_recv()
    for a in range(2):
        span = slice(a * half, (a + 1) * half)
        total = keep[0, a, 0]
        for k in range(1, nz):
            total = total + zr[k - 1, span].astype(jnp.float32)
        out[span] = (g_ref[span].astype(jnp.float32) + total).astype(jnp.bfloat16)
    for one in sent:
        one.wait_send()


def reduce_all(gd, ud, gate_rows, up_rows, gate_other, up_other, out_cotangent):
    nz = gate_rows.shape[0]
    rows, columns = out_cotangent.shape
    half = rows // 2
    dma = pltpu.SemaphoreType.DMA
    vmem = pl.BlockSpec(memory_space=pltpu.VMEM)
    bf16 = jnp.bfloat16
    return pl.pallas_call(
        functools.partial(reduce_kernel, nz),
        out_shape=jax.ShapeDtypeStruct((rows, columns), bf16),
        in_specs=[vmem] * 7,
        out_specs=vmem,
        scratch_shapes=[
            pltpu.VMEM((2,) + gd.shape, bf16),
            pltpu.VMEM((nz, 2, 2, half, columns), bf16),
            pltpu.VMEM((nz, 2, 2, half, columns), bf16),
            pltpu.VMEM((nz, 2, 2, half, columns), jnp.float32),
            pltpu.VMEM((nz, 2, half, columns), bf16),
            pltpu.VMEM((nz, 2, half, columns), bf16),
            pltpu.VMEM((nz - 1, rows, columns), bf16),
            pltpu.VMEM((nz - 1, rows, columns), bf16),
            dma((2,)),
            dma((2,)),
            dma((nz, 2)),
            dma((nz, 2)),
            dma((nz, 2)),
            dma((nz, 2)),
            dma((nz - 1,)),
            dma((nz - 1,)),
        ],
        compiler_params=pltpu.CompilerParams(collective_id=1, has_side_effects=True),
        name="reduce_all",
    )(gd, ud, gate_rows, up_rows, gate_other, up_other, out_cotangent)


def pieces(value):
    if value.dtype == jnp.bfloat16:
        return (value,)
    high = value.astype(jnp.bfloat16)
    return (high, (value - high.astype(jnp.float32)).astype(jnp.bfloat16))


def product(left, right, left_dim, right_dim):
    lefts, rights = pieces(left), pieces(right)
    total = None
    for i, one in enumerate(lefts):
        for j, two in enumerate(rights):
            if i + j < 2:
                part = dots(one, two, left_dim, right_dim)
                total = part if total is None else total + part
    return total


def exact(left, right):
    return lax.dot_general(
        left,
        right,
        (((1,), (0,)), ((), ())),
        precision=lax.Precision.HIGHEST,
        preferred_element_type=jnp.float32,
    )


def triangle(lower):
    row = lax.broadcasted_iota(jnp.int32, (SPAN, SPAN), 0)
    column = lax.broadcasted_iota(jnp.int32, (SPAN, SPAN), 1)
    return row >= column if lower else row <= column


def tail_kernel(
    tg,
    wo,
    mo,
    q_ref,
    k_ref,
    v_ref,
    a_ref,
    s0,
    proj,
    dq,
    dk,
    dv,
    da,
    full,
    tgd,
    moa,
    mg,
    gb,
    grow,
    shrink,
    left,
    raised,
    kshrunk,
    kleft,
    scores,
    states,
    ends,
    dqs,
    dks,
    dvs,
    rout,
    rin,
    following,
    kept_out,
    kept_in,
    sum_out,
    sum_in,
    z_send,
    z_recv,
    p_send,
    p_recv,
    b_send,
    b_recv,
    t_send,
    t_recv,
    m_send,
    m_recv,
    r_send,
    r_recv,
    k_send,
    k_recv,
    u_send,
    u_recv,
):
    s, sy, sx, sd, z, c = peers(4)
    nz = 4
    me, partner = z * 2 + c, z * 2 + 1 - c
    tokens, columns = tg.shape
    blocks = tokens // SPAN
    heads, width, span = s0.shape[0], s0.shape[1], s0.shape[2]
    greet(
        [at(s, lax.rem(z + d, nz) * 2 + c) for d in range(1, nz)]
        + [at(sy, me), at(sx, me), at(sd, me), at(s, partner)]
    )
    sent = []

    def copy(src, dst, send, recv, device):
        return pltpu.make_async_remote_copy(
            src_ref=src, dst_ref=dst, send_sem=send, recv_sem=recv, device_id=device, device_id_type=MESH
        )

    def start(when, *parts):
        def go():
            copy(*parts).start()

        if when is None:
            go()
        else:
            pl.when(when)(go)
        sent.append((when, parts))

    def arrived(slot, recv):
        copy(slot, slot, recv, recv, at(s, partner)).wait_recv()

    def slot(block, core):
        return full.at[block * 2 + core]

    def rows(index):
        return pl.ds(pl.multiple_of(index * tokens, tokens), tokens)

    def spread(when, src, block):
        start(when, src, slot(block, c), b_send.at[block], b_recv.at[block], at(s, partner))
        ok = block != s
        start(
            ok if when is None else when & ok,
            src,
            tgd.at[c, rows(s)],
            p_send.at[block],
            p_recv.at[s],
            at(block, me),
        )

    def hop(when, src, block, way, d):
        step = 1 if way == 0 else -1
        room = z + step < nz if way == 0 else z + step >= 0
        start(
            room if when is None else when & room,
            src,
            slot(block, c),
            z_send.at[way, d],
            z_recv.at[way, d],
            at(s, (z + step) * 2 + c),
        )

    hop(None, tg, z, 0, 0)
    hop(None, tg, z, 1, 0)
    spread(None, tg, z)
    for j, target in enumerate((sy, sx, sd)):
        start(None, mo, moa.at[rows(s)], m_send.at[j], m_recv.at[j], at(target, me))

    lower, upper = triangle(True), triangle(False)
    ones_low = lower.astype(jnp.float32)
    scale = width ** (-0.5)
    for n in range(blocks):
        rn = slice(n * SPAN, (n + 1) * SPAN)
        running = exact(ones_low, a_ref[rn, :])
        end = running[SPAN - 1 : SPAN]
        ends[n : n + 1, :] = end
        kk = k_ref[rn, :].astype(jnp.float32)
        up, down = jnp.exp(running), jnp.exp(-running)
        rest = jnp.exp(end - running)
        grow[rn, :] = up
        shrink[rn, :] = down
        left[rn, :] = rest
        raised[rn, :] = q_ref[rn, :].astype(jnp.float32) * scale * up
        kshrunk[rn, :] = kk * down
        kleft[rn, :] = kk * rest
    later = jnp.zeros((1, ends.shape[1]), jnp.float32)
    laters = [None] * blocks
    for n in reversed(range(blocks)):
        laters[n] = later
        later = later + ends[n : n + 1, :]
    kept_out[...] = jnp.broadcast_to(jnp.exp(later), kept_out.shape)
    for h in range(heads):
        lk, lv = slice(h * width, (h + 1) * width), slice(h * span, (h + 1) * span)
        state = s0[h].T
        for n in range(blocks):
            rn = slice(n * SPAN, (n + 1) * SPAN)
            states[h, n] = state
            score = product(kshrunk[rn, lk], raised[rn, lk], 1, 1)
            scores[h, rn, :] = jnp.where(upper, score, 0.0)
            if n + 1 < blocks:
                state = jnp.exp(ends[n : n + 1, lk]) * state + product(v_ref[rn, lv], kleft[rn, lk], 0, 0)
    for j in range(3):
        start(
            s > j, kept_out, kept_in.at[s], k_send.at[j], k_recv.at[s], at(j, me)
        )

    def mix(block, core, first=False):
        index = block * 2 + core
        part = dots(
            tg[...] if first else full[index],
            wo[pl.ds(pl.multiple_of(index * columns, columns), columns), :],
            1,
            0,
        )
        if first:
            mg[...] = part
        else:
            mg[...] += part

    mix(z, c, True)
    full[me] = tg[...]
    arrived(slot(z, 1 - c), b_recv.at[z])
    mix(z, 1 - c)
    for d in range(1, nz):
        for way in range(2):
            block = z - d if way == 0 else z + d
            here = block >= 0 if way == 0 else block < nz

            @pl.when(here)
            def _():
                arrived(slot(block, c), z_recv.at[way, d - 1])

            if d < nz - 1:
                hop(here, slot(block, c), block, way, d)
            spread(here, slot(block, c), block)

            @pl.when(here)
            def _():
                mix(block, c)
                arrived(slot(block, 1 - c), b_recv.at[block])
                mix(block, 1 - c)

    gb[...] = mg[...].astype(jnp.bfloat16)

    for h in range(heads):
        lk, lv = slice(h * width, (h + 1) * width), slice(h * span, (h + 1) * span)
        carry = jnp.zeros((span, width), jnp.float32)
        for n in reversed(range(blocks)):
            rn = slice(n * SPAN, (n + 1) * SPAN)
            g, v = gb[rn, lv], v_ref[rn, lv]
            down, over = jnp.where(lower, dots(g, v, 1, 1), 0.0), jnp.where(upper, dots(v, g, 1, 1), 0.0)
            dqs[rn, lk] = grow[rn, lk] * (
                product(g, states[h, n], 1, 0) + product(down, kshrunk[rn, lk], 1, 0)
            )
            kpart = shrink[rn, lk] * product(over, raised[rn, lk], 1, 0)
            vpart = product(scores[h, rn, :], g, 1, 0)
            if n + 1 < blocks:
                kpart += left[rn, lk] * product(v, carry, 1, 0)
                vpart += product(kleft[rn, lk], carry, 1, 1)
            dks[rn, lk] = kpart
            dvs[rn, lv] = vpart
            carry = product(g, raised[rn, lk], 0, 0) + jnp.exp(ends[n : n + 1, lk]) * carry
        rout[h] = carry.astype(jnp.bfloat16)
        for j in range(3):
            start(s > j, rout.at[h], rin.at[s, h], r_send.at[h, j], r_recv.at[h, s], at(j, me))

    dq[...] = (dqs[...] * scale).astype(jnp.bfloat16)

    for j, other in enumerate((sy, sx, sd)):
        block = tgd.at[c, rows(other)]
        arrived(block, p_recv.at[other])
        start(None, block, block, t_send.at[j], t_recv.at[j], at(s, partner))
        arrived(moa.at[rows(other)], m_recv.at[j])
    moa[rows(s), :] = mo[...]
    for core in range(2):
        tgd[core, rows(s), :] = full[s * 2 + core]
    for j, other in enumerate((sy, sx, sd)):
        arrived(tgd.at[1 - c, rows(other)], t_recv.at[j])
    for core in range(2):
        proj[core * columns : (core + 1) * columns, :] = dots(tgd[core], moa[...], 0, 0)

    following[...] = jnp.zeros_like(following)
    for source in (3, 2, 1):

        @pl.when(s < source)
        def _():
            arrived(kept_in.at[source], k_recv.at[source])
            for h in range(heads):
                arrived(rin.at[source, h], r_recv.at[h, source])
                keep = kept_in[source, 0:1, h * width : (h + 1) * width]
                following[h] = rin[source, h].astype(jnp.float32) + keep * following[h]

    change = [None] * blocks
    for n in reversed(range(blocks)):
        rn = slice(n * SPAN, (n + 1) * SPAN)
        rest = left[rn, :] * jnp.exp(laters[n])
        kk = k_ref[rn, :].astype(jnp.float32)
        weighted = kk * rest
        for h in range(heads):
            lk, lv = slice(h * width, (h + 1) * width), slice(h * span, (h + 1) * span)
            dks[rn, lk] += rest[:, lk] * product(v_ref[rn, lv], following[h], 1, 0)
            dv[rn, lv] = (dvs[rn, lv] + product(weighted[:, lk], following[h], 1, 1)).astype(jnp.bfloat16)
        full_k = dks[rn, :]
        dk[rn, :] = full_k.astype(jnp.bfloat16)
        dqs[rn, :] = q_ref[rn, :].astype(jnp.float32) * scale * dqs[rn, :] - kk * full_k
    sums = [jnp.sum(dqs[n * SPAN : (n + 1) * SPAN, :], axis=0, keepdims=True) for n in range(blocks)]
    total = sums[0]
    for n in range(1, blocks):
        total = total + sums[n]
    sum_out[...] = jnp.broadcast_to(total, sum_out.shape)
    for j in range(3):
        start(s > j, sum_out, sum_in.at[s], u_send.at[j], u_recv.at[s], at(j, me))
    ones_up = upper.astype(jnp.float32)
    behind = jnp.zeros_like(total)
    for n in reversed(range(blocks)):
        rn = slice(n * SPAN, (n + 1) * SPAN)
        dks[rn, :] = exact(ones_up, dqs[rn, :]) + behind
        behind = behind + sums[n]
    ends[0:1, :] = jnp.zeros_like(total)
    for source in (3, 2, 1):

        @pl.when(s < source)
        def _():
            arrived(sum_in.at[source], u_recv.at[source])
            ends[0:1, :] += sum_in[source, 0:1, :]

    da[...] = dks[...] + ends[0:1, :]
    for when, parts in sent:
        if when is None:
            copy(*parts).wait_send()
        else:

            @pl.when(when)
            def _():
                copy(*parts).wait_send()


def tail(token_grad, out_proj, mixer_output, queries, key_rows, value_rows, log_decay, entry):
    tokens, columns = token_grad.shape
    heads, width, span = entry.shape
    keys = heads * width
    n_sp = lax.axis_size("sp")
    depth = out_proj.shape[0] // n_sp
    blocks = tokens // SPAN
    bf16, f32 = jnp.bfloat16, jnp.float32
    dma = pltpu.SemaphoreType.DMA
    vmem = pl.BlockSpec(memory_space=pltpu.VMEM)
    return pl.pallas_call(
        tail_kernel,
        out_shape=(
            jax.ShapeDtypeStruct((depth, columns), f32),
            jax.ShapeDtypeStruct((tokens, keys), bf16),
            jax.ShapeDtypeStruct((tokens, keys), bf16),
            jax.ShapeDtypeStruct((tokens, columns), bf16),
            jax.ShapeDtypeStruct((tokens, keys), f32),
        ),
        in_specs=[vmem] * 8,
        out_specs=(vmem,) * 5,
        scratch_shapes=[
            pltpu.VMEM((8, tokens, columns), bf16),
            pltpu.VMEM((2, n_sp * tokens, columns), bf16),
            pltpu.VMEM((n_sp * tokens, columns), bf16),
            pltpu.VMEM((tokens, columns), f32),
            pltpu.VMEM((tokens, columns), bf16),
            *[pltpu.VMEM((tokens, keys), f32) for _ in range(6)],
            pltpu.VMEM((heads, tokens, SPAN), f32),
            pltpu.VMEM((heads, blocks, span, width), f32),
            pltpu.VMEM((8, keys), f32),
            pltpu.VMEM((tokens, keys), f32),
            pltpu.VMEM((tokens, keys), f32),
            pltpu.VMEM((tokens, columns), f32),
            pltpu.VMEM((heads, span, width), bf16),
            pltpu.VMEM((n_sp, heads, span, width), bf16),
            pltpu.VMEM((heads, span, width), f32),
            pltpu.VMEM((8, keys), f32),
            pltpu.VMEM((n_sp, 8, keys), f32),
            pltpu.VMEM((8, keys), f32),
            pltpu.VMEM((n_sp, 8, keys), f32),
            dma((2, 3)),
            dma((2, 3)),
            dma((4,)),
            dma((4,)),
            dma((4,)),
            dma((4,)),
            dma((3,)),
            dma((3,)),
            dma((3,)),
            dma((3,)),
            dma((2, 3)),
            dma((2, 4)),
            dma((3,)),
            dma((4,)),
            dma((3,)),
            dma((4,)),
        ],
        compiler_params=pltpu.CompilerParams(
            collective_id=2, has_side_effects=True, vmem_limit_bytes=60 * 1024 * 1024
        ),
        name="tail",
    )(token_grad, out_proj, mixer_output, queries, key_rows, value_rows, log_decay, entry)


def dense_experts(layer_input, out_cotangent, routes, route_weights, gate_proj, up_proj, down_proj, log_decay):
    n_sp, tp = lax.axis_size("sp"), lax.axis_size("tp")
    nz = tp // 2
    columns = layer_input.shape[1]
    hidden = gate_proj.shape[2]
    rows = [
        jnp.sum(jnp.where(routes == e, route_weights, 0.0), axis=1) for e in range(n_sp)
    ] + [jnp.exp(jnp.sum(log_decay, axis=0))]
    table = jnp.pad(jnp.stack(rows), ((0, -len(rows) % 8), (0, 0)))
    gate_rows = gate_proj.reshape(nz, 2, columns, hidden)
    up_rows = up_proj.reshape(nz, 2, columns, hidden)
    x, g, tables, gate_other, up_other = gather_all(
        layer_input, out_cotangent, table, gate_rows, up_rows
    )
    weight = lax.dynamic_index_in_dim(tables, lax.axis_index("sp"), 1, False).reshape(-1, 1)
    gd, ud, gdt, udt, ht = hidden_deltas(x, g, weight, gate_proj[0], up_proj[0], down_proj[0])
    token_grad = reduce_all(gd, ud, gate_rows, up_rows, gate_other, up_other, out_cotangent)
    grads = weight_grads(x, g, weight, gdt, udt, ht)
    return [part[None] for part in grads], token_grad, tables[:, n_sp]


def routed_experts(
    layer_input, out_cotangent, routes, route_weights, gate_proj, up_proj, down_proj
):
    experts = gate_proj.shape[0] * lax.axis_size("sp")
    capacity = 5 * routes.shape[1] * routes.shape[0] // (4 * experts)
    columns = layer_input.shape[1]
    placed, weighted = route_tables(routes, route_weights, experts, capacity)
    input_slots = (
        jnp.einsum(
            "tp,td->pd",
            placed.astype(jnp.bfloat16),
            layer_input,
            preferred_element_type=jnp.float32,
        )
        .astype(jnp.bfloat16)
        .reshape(experts, capacity, columns)
    )
    grad_slots = (
        jnp.einsum(
            "tp,td->pd", weighted, out_cotangent.astype(jnp.float32), precision=PRECISION_LEVEL
        )
        .astype(jnp.bfloat16)
        .reshape(experts, capacity, columns)
    )
    sent = (
        lax.all_to_all(input_slots, "sp", split_axis=0, concat_axis=1, tiled=True),
        lax.all_to_all(grad_slots, "sp", split_axis=0, concat_axis=1, tiled=True),
    )
    inputs = lax.all_gather(sent[0], "tp", axis=2, tiled=True)
    pair_grad = lax.all_gather(sent[1], "tp", axis=2, tiled=True)
    gate_part, up_part, down_part, gate_delta, up_delta = expert_backward(
        inputs, pair_grad, gate_proj, up_proj, down_proj
    )
    input_grad = input_rows(gate_delta, up_delta, gate_proj, up_proj)
    share = lax.psum_scatter(
        input_grad.astype(jnp.bfloat16), "tp", scatter_dimension=2, tiled=True
    ).astype(jnp.float32)
    returned = lax.all_to_all(
        share.astype(jnp.bfloat16), "sp", split_axis=1, concat_axis=0, tiled=True
    ).astype(share.dtype)
    slot_grads = returned.reshape(experts * capacity, columns)
    moe_grad = jnp.einsum("tp,pd->td", placed, slot_grads, precision=PRECISION_LEVEL)
    token_grad = (out_cotangent.astype(jnp.float32) + moe_grad).astype(jnp.bfloat16)
    parts = [part.astype(jnp.bfloat16) for part in (gate_part, up_part, down_part)]
    return parts, token_grad, None


def body(
    layer_input,
    out_cotangent,
    routes,
    route_weights,
    gate_proj,
    up_proj,
    down_proj,
    out_proj,
    mixer_output,
    queries,
    key_rows,
    value_rows,
    log_decay,
    entry_state,
):
    args = (layer_input, out_cotangent, routes, route_weights, gate_proj, up_proj, down_proj)
    paired = lax.axis_size("sp") == 4 and lax.axis_size("tp") % 2 == 0
    square = paired and lax.axis_size("tp") == 8 and gate_proj.shape[0] == 1
    square = square and log_decay.shape[1] == routes.shape[0]
    if square:
        parts, token_grad, kept = dense_experts(*args, log_decay)
    else:
        parts, token_grad, kept = routed_experts(*args)
    if square:
        outs = tail(
            token_grad,
            out_proj,
            mixer_output,
            queries,
            key_rows,
            value_rows,
            log_decay,
            entry_state[0],
        )
        return (*parts, *outs)
    full_grad = lax.all_gather(token_grad, "tp", axis=1, tiled=True)
    partial = jnp.einsum(
        "td,tc->dc", full_grad, mixer_output, preferred_element_type=jnp.float32
    ).astype(jnp.bfloat16)
    partial, full_grad = lax.optimization_barrier((partial, full_grad))
    proj_grad = lax.psum_scatter(partial, "sp", scatter_dimension=0, tiled=True).astype(jnp.float32)
    mix_grad = jnp.dot(full_grad, out_proj, preferred_element_type=jnp.float32).astype(jnp.bfloat16)
    query_grad, key_grad, value_grad, decay_grad = mixer_backward(
        queries, key_rows, value_rows, log_decay, entry_state[0], mix_grad, kept
    )
    return (
        *parts,
        proj_grad,
        query_grad,
        key_grad,
        value_grad,
        decay_grad,
    )


def solution(mesh):
    return jax.shard_map(
        body,
        mesh=mesh,
        in_specs=(
            P("sp", "tp"),
            P("sp", "tp"),
            P("sp", None),
            P("sp", None),
            P("sp", None, "tp"),
            P("sp", None, "tp"),
            P("sp", "tp", None),
            P(None, "tp"),
            P("sp", "tp"),
            P("sp", "tp"),
            P("sp", "tp"),
            P("sp", "tp"),
            P("sp", "tp"),
            P("sp", "tp", None, None),
        ),
        out_specs=(
            P("sp", None, "tp"),
            P("sp", None, "tp"),
            P("sp", "tp", None),
            P("sp", "tp"),
            P("sp", "tp"),
            P("sp", "tp"),
            P("sp", "tp"),
            P("sp", "tp"),
        ),
        check_vma=False,
    )
```

```python
import functools

import jax
import jax.numpy as jnp
from jax import lax
from jax.experimental import pallas as pl
from jax.experimental.pallas import tpu as pltpu
from jax.sharding import PartitionSpec as P

SPAN = 64
MESH = pl.DeviceIdType.MESH


PRECISION_LEVEL = lax.Precision.HIGH


def entering(value, axis, join, neutral, kept=None):
    count = lax.axis_size(axis)
    place = lax.axis_index(axis)
    ahead = count - 1 - place
    if kept is None:
        kept = lax.all_gather(value[0].astype(jnp.bfloat16), axis)
    gathered = (kept, lax.all_gather(value[1].astype(jnp.bfloat16), axis))
    state = jax.tree.map(lambda a, e: jnp.zeros_like(a) + jnp.asarray(e, a.dtype), value, neutral)

    def one(lap, state):
        source = count - 1 - lap
        return join(
            state,
            jax.tree.map(
                lambda a, own: lax.dynamic_index_in_dim(a, source, 0, False).astype(own.dtype),
                gathered,
                value,
            ),
        )

    return lax.fori_loop(0, ahead, one, state)


def prefix(value, axis, join, neutral):
    count, mine = (lax.axis_size(axis), lax.axis_index(axis))
    pieces = lax.all_gather(value, axis)
    pieces = pieces[::-1]
    mine = count - 1 - mine
    subtotal = jnp.full_like(value, 0) + jnp.asarray(neutral, value.dtype)

    def lap(position, subtotal):
        longer = join(subtotal, pieces[position])
        return jnp.where(position < mine, longer, subtotal)

    return lax.fori_loop(0, count - 1, lap, subtotal)


def route_tables(routes, route_weights, experts, capacity):
    tokens = routes.shape[0]
    top_count = routes.shape[1]
    pair_ids = routes.reshape(-1)
    expert_ids = jnp.arange(experts, dtype=jnp.int32)
    onehot = (pair_ids[:, None] == expert_ids[None, :]).astype(jnp.int32)
    slot_rank = jnp.sum((jnp.cumsum(onehot, axis=0) - onehot) * onehot, axis=1)
    target = pair_ids * capacity + slot_rank
    slot_ids = jnp.arange(experts * capacity, dtype=jnp.int32)
    slot_hits = (
        (target[:, None] == slot_ids[None, :])
        .astype(jnp.float32)
        .reshape(tokens, top_count, experts * capacity)
    )
    placed = jnp.sum(slot_hits, axis=1)
    weighted = jnp.einsum("tk,tkp->tp", route_weights, slot_hits, precision=PRECISION_LEVEL)
    return (placed, weighted)


def expert_backward(inputs, pair_grad, gate_proj, up_proj, down_proj):
    gate_pre = jnp.einsum("erd,edf->erf", inputs, gate_proj, preferred_element_type=jnp.float32)
    up_pre = jnp.einsum("erd,edf->erf", inputs, up_proj, preferred_element_type=jnp.float32)
    sigmoid_gate = jax.nn.sigmoid(gate_pre)
    activated = gate_pre * sigmoid_gate
    hidden = (activated * up_pre).astype(jnp.bfloat16)
    down_grad = jnp.einsum("erf,erd->efd", hidden, pair_grad, preferred_element_type=jnp.float32)
    hidden_grad = jnp.einsum(
        "erd,efd->erf", pair_grad, down_proj, preferred_element_type=jnp.float32
    )
    gate_delta = (
        hidden_grad * up_pre * sigmoid_gate * (1.0 + gate_pre * (1.0 - sigmoid_gate))
    ).astype(jnp.bfloat16)
    up_delta = (hidden_grad * activated).astype(jnp.bfloat16)
    gate_grad = jnp.einsum("erd,erf->edf", inputs, gate_delta, preferred_element_type=jnp.float32)
    up_grad = jnp.einsum("erd,erf->edf", inputs, up_delta, preferred_element_type=jnp.float32)
    return (gate_grad, up_grad, down_grad, gate_delta, up_delta)


def input_rows(gate_delta, up_delta, gate_weight, up_weight):
    input_grad = jnp.einsum(
        "erf,edf->erd", gate_delta, gate_weight, preferred_element_type=jnp.float32
    )
    return input_grad + jnp.einsum(
        "erf,edf->erd", up_delta, up_weight, preferred_element_type=jnp.float32
    )


def state_combine(prior_steps, later):
    return (prior_steps[0] * later[0], later[1] + later[0][:, :, None] * prior_steps[1])


def add_combine(prior_steps, later):
    return prior_steps + later


def mixer_backward(queries, key_rows, value_rows, log_decay, entry, mix_grad, kept=None):
    tokens = queries.shape[0]
    heads = entry.shape[0]
    key_width = entry.shape[1]
    value_width = entry.shape[2]
    blocks = tokens // SPAN
    causal = jnp.tril(jnp.ones((SPAN, SPAN), dtype=bool))

    def split(rows, width):
        return rows.astype(jnp.float32).reshape(blocks, SPAN, heads, width)

    scaled_q = split(queries, key_width) * key_width ** (-0.5)
    key_segment = split(key_rows, key_width)
    value_segment = split(value_rows, value_width)
    decays = split(log_decay, key_width)
    output_gradient = split(mix_grad, value_width)
    value_dots = jnp.where(
        causal[None, None],
        jnp.einsum("nthv,nshv->nhts", output_gradient, value_segment, precision=PRECISION_LEVEL),
        0.0,
    )

    def forward_block(passed_state, block_data):
        query_now, current_key, current_value, decay_now, current_gradient, dots_now = block_data
        running_decay = jnp.cumsum(decay_now, axis=0)
        growth_multiplier = jnp.exp(running_decay)
        block_overall_sum = running_decay[-1]
        state_contribution = growth_multiplier * jnp.einsum(
            "gxb,xqb->gxq", current_gradient, passed_state, precision=PRECISION_LEVEL
        )
        inside = growth_multiplier * jnp.einsum(
            "hts,shk->thk",
            dots_now,
            current_key * jnp.exp(-running_decay),
            precision=PRECISION_LEVEL,
        )
        state_update = jnp.einsum(
            "rsx,rse->sxe",
            current_key * jnp.exp(block_overall_sum - running_decay),
            current_value,
            precision=PRECISION_LEVEL,
        )
        return (
            jnp.exp(block_overall_sum)[:, :, None] * passed_state + state_update,
            state_contribution + inside,
        )

    def reverse_block(passed_state, block_data):
        query_now, current_key, current_value, decay_now, current_gradient, dots_now = block_data
        running_decay = jnp.cumsum(decay_now, axis=0)
        shrink = jnp.exp(-running_decay)
        block_overall_sum = running_decay[-1]
        decay_remaining = jnp.exp(block_overall_sum - running_decay)
        query_raised = query_now * jnp.exp(running_decay)
        key_portion = decay_remaining * jnp.einsum(
            "gxb,xqb->gxq", current_value, passed_state, precision=PRECISION_LEVEL
        )
        key_portion = key_portion + shrink * jnp.einsum(
            "hts,thk->shk", dots_now, query_raised, precision=PRECISION_LEVEL
        )
        scores = jnp.where(
            causal[None],
            jnp.einsum(
                "thk,shk->hts", query_raised, current_key * shrink, precision=PRECISION_LEVEL
            ),
            0.0,
        )
        value_portion = jnp.einsum(
            "qgy,gye->qge", current_key * decay_remaining, passed_state, precision=PRECISION_LEVEL
        )
        value_portion = value_portion + jnp.einsum(
            "hts,thv->shv", scores, current_gradient, precision=PRECISION_LEVEL
        )
        prior_steps = (
            jnp.einsum("rsx,rse->sxe", query_raised, current_gradient, precision=PRECISION_LEVEL)
            + jnp.exp(block_overall_sum)[:, :, None] * passed_state
        )
        return (prior_steps, (key_portion, value_portion))

    block_inputs = (scaled_q, key_segment, value_segment, decays, output_gradient, value_dots)
    _, query_part = lax.scan(forward_block, entry, block_inputs)
    empty_state = jnp.zeros((heads, key_width, value_width), dtype=jnp.float32)
    local_start, (key_portion, value_portion) = lax.scan(
        reverse_block, empty_state, block_inputs, reverse=True
    )
    scaled_flat = scaled_q.reshape(tokens, heads, key_width)
    key_flattened = key_segment.reshape(tokens, heads, key_width)
    value_flattened = value_segment.reshape(tokens, heads, value_width)
    query_flat = query_part.reshape(tokens, heads, key_width)
    local_key = key_portion.reshape(tokens, heads, key_width)
    running_decay = jnp.cumsum(decays.reshape(tokens, heads, key_width), axis=0)
    device_total = running_decay[-1]
    decay_remaining = jnp.exp(device_total - running_decay)
    retain = jnp.exp(device_total)
    ones_head = jnp.ones((heads, key_width), dtype=jnp.float32)
    zeros_head = jnp.zeros((heads, key_width), dtype=jnp.float32)
    scanned = entering((retain, local_start), "sp", state_combine, (ones_head, empty_state), kept)
    following_state = scanned[1]
    key_full = local_key + decay_remaining * jnp.einsum(
        "gxb,xqb->gxq", value_flattened, following_state, precision=PRECISION_LEVEL
    )
    value_full = value_portion.reshape(tokens, heads, value_width)
    value_full = value_full + jnp.einsum(
        "qgy,gye->qge", key_flattened * decay_remaining, following_state, precision=PRECISION_LEVEL
    )
    change = scaled_flat * query_flat - key_flattened * key_full
    later_sum = prefix(jnp.sum(change, axis=0), "sp", add_combine, zeros_head)
    decay_grad = (lax.cumsum(change, axis=0, reverse=True) + later_sum[None]).reshape(
        tokens, heads * key_width
    )
    query_grad = (
        (query_flat * key_width ** (-0.5)).reshape(tokens, heads * key_width).astype(jnp.bfloat16)
    )
    key_grad = key_full.reshape(tokens, heads * key_width).astype(jnp.bfloat16)
    value_grad = value_full.reshape(tokens, heads * value_width).astype(jnp.bfloat16)
    return (query_grad, key_grad, value_grad, decay_grad)


def peers(nz):
    s = lax.axis_index("sp")
    t = lax.axis_index("tp")
    y, x = s // 2, s % 2
    z, c = t // 2, t % 2
    return s, (1 - y) * 2 + x, y * 2 + 1 - x, (1 - y) * 2 + 1 - x, z, c


def greet(devices):
    barrier = pltpu.get_barrier_semaphore()
    for device in devices:
        pl.semaphore_signal(barrier, inc=1, device_id=device, device_id_type=MESH)
    pl.semaphore_wait(barrier, len(devices))


def at(s, t):
    return {"sp": s, "tp": t}


def dots(left, right, left_dim, right_dim):
    return lax.dot_general(
        left, right, (((left_dim,), (right_dim,)), ((), ())), preferred_element_type=jnp.float32
    )


def fixed_spec(shape):
    return pl.BlockSpec(shape, lambda t: (0,) * len(shape))


def pieces(value):
    if value.dtype == jnp.bfloat16:
        return (value,)
    high = value.astype(jnp.bfloat16)
    return (high, (value - high.astype(jnp.float32)).astype(jnp.bfloat16))


def product(left, right, left_dim, right_dim):
    lefts, rights = pieces(left), pieces(right)
    total = None
    for i, one in enumerate(lefts):
        for j, two in enumerate(rights):
            if i + j < 2:
                part = dots(one, two, left_dim, right_dim)
                total = part if total is None else total + part
    return total


def exact(left, right):
    return lax.dot_general(
        left,
        right,
        (((1,), (0,)), ((), ())),
        precision=lax.Precision.HIGHEST,
        preferred_element_type=jnp.float32,
    )


def triangle(lower):
    row = lax.broadcasted_iota(jnp.int32, (SPAN, SPAN), 0)
    column = lax.broadcasted_iota(jnp.int32, (SPAN, SPAN), 1)
    return row >= column if lower else row <= column


def tail_kernel(
    tg,
    wo,
    mo,
    q_ref,
    k_ref,
    v_ref,
    a_ref,
    s0,
    proj,
    dq,
    dk,
    dv,
    da,
    full,
    tgd,
    moa,
    mg,
    gb,
    grow,
    shrink,
    left,
    raised,
    kshrunk,
    kleft,
    scores,
    states,
    ends,
    dqs,
    dks,
    dvs,
    rout,
    rin,
    following,
    kept_out,
    kept_in,
    sum_out,
    sum_in,
    z_send,
    z_recv,
    p_send,
    p_recv,
    b_send,
    b_recv,
    t_send,
    t_recv,
    m_send,
    m_recv,
    r_send,
    r_recv,
    k_send,
    k_recv,
    u_send,
    u_recv,
):
    s, sy, sx, sd, z, c = peers(4)
    nz = 4
    me, partner = z * 2 + c, z * 2 + 1 - c
    tokens, columns = tg.shape
    blocks = tokens // SPAN
    heads, width, span = s0.shape[0], s0.shape[1], s0.shape[2]
    greet(
        [at(s, lax.rem(z + d, nz) * 2 + c) for d in range(1, nz)]
        + [at(sy, me), at(sx, me), at(sd, me), at(s, partner)]
    )
    sent = []

    def copy(src, dst, send, recv, device):
        return pltpu.make_async_remote_copy(
            src_ref=src, dst_ref=dst, send_sem=send, recv_sem=recv, device_id=device, device_id_type=MESH
        )

    def start(when, *parts):
        def go():
            copy(*parts).start()

        if when is None:
            go()
        else:
            pl.when(when)(go)
        sent.append((when, parts))

    def arrived(slot, recv):
        copy(slot, slot, recv, recv, at(s, partner)).wait_recv()

    def slot(block, core):
        return full.at[block * 2 + core]

    def rows(index):
        return pl.ds(pl.multiple_of(index * tokens, tokens), tokens)

    def spread(when, src, block):
        start(when, src, slot(block, c), b_send.at[block], b_recv.at[block], at(s, partner))
        ok = block != s
        start(
            ok if when is None else when & ok,
            src,
            tgd.at[c, rows(s)],
            p_send.at[block],
            p_recv.at[s],
            at(block, me),
        )

    def hop(when, src, block, way, d):
        step = 1 if way == 0 else -1
        room = z + step < nz if way == 0 else z + step >= 0
        start(
            room if when is None else when & room,
            src,
            slot(block, c),
            z_send.at[way, d],
            z_recv.at[way, d],
            at(s, (z + step) * 2 + c),
        )

    hop(None, tg, z, 0, 0)
    hop(None, tg, z, 1, 0)
    spread(None, tg, z)
    for j, target in enumerate((sy, sx, sd)):
        start(None, mo, moa.at[rows(s)], m_send.at[j], m_recv.at[j], at(target, me))

    lower, upper = triangle(True), triangle(False)
    ones_low = lower.astype(jnp.float32)
    scale = width ** (-0.5)
    for n in range(blocks):
        rn = slice(n * SPAN, (n + 1) * SPAN)
        running = exact(ones_low, a_ref[rn, :])
        end = running[SPAN - 1 : SPAN]
        ends[n : n + 1, :] = end
        kk = k_ref[rn, :].astype(jnp.float32)
        up, down = jnp.exp(running), jnp.exp(-running)
        rest = jnp.exp(end - running)
        grow[rn, :] = up
        shrink[rn, :] = down
        left[rn, :] = rest
        raised[rn, :] = q_ref[rn, :].astype(jnp.float32) * scale * up
        kshrunk[rn, :] = kk * down
        kleft[rn, :] = kk * rest
    later = jnp.zeros((1, ends.shape[1]), jnp.float32)
    laters = [None] * blocks
    for n in reversed(range(blocks)):
        laters[n] = later
        later = later + ends[n : n + 1, :]
    kept_out[...] = jnp.broadcast_to(jnp.exp(later), kept_out.shape)
    for h in range(heads):
        lk, lv = slice(h * width, (h + 1) * width), slice(h * span, (h + 1) * span)
        state = s0[h].T
        for n in range(blocks):
            rn = slice(n * SPAN, (n + 1) * SPAN)
            states[h, n] = state
            score = product(kshrunk[rn, lk], raised[rn, lk], 1, 1)
            scores[h, rn, :] = jnp.where(upper, score, 0.0)
            if n + 1 < blocks:
                state = jnp.exp(ends[n : n + 1, lk]) * state + product(v_ref[rn, lv], kleft[rn, lk], 0, 0)
    for j in range(3):
        start(
            s > j, kept_out, kept_in.at[s], k_send.at[j], k_recv.at[s], at(j, me)
        )

    def mix(block, core, first=False):
        index = block * 2 + core
        part = dots(
            tg[...] if first else full[index],
            wo[pl.ds(pl.multiple_of(index * columns, columns), columns), :],
            1,
            0,
        )
        if first:
            mg[...] = part
        else:
            mg[...] += part

    mix(z, c, True)
    full[me] = tg[...]
    arrived(slot(z, 1 - c), b_recv.at[z])
    mix(z, 1 - c)
    for d in range(1, nz):
        for way in range(2):
            block = z - d if way == 0 else z + d
            here = block >= 0 if way == 0 else block < nz

            @pl.when(here)
            def _():
                arrived(slot(block, c), z_recv.at[way, d - 1])

            if d < nz - 1:
                hop(here, slot(block, c), block, way, d)
            spread(here, slot(block, c), block)

            @pl.when(here)
            def _():
                mix(block, c)
                arrived(slot(block, 1 - c), b_recv.at[block])
                mix(block, 1 - c)

    gb[...] = mg[...].astype(jnp.bfloat16)

    for h in range(heads):
        lk, lv = slice(h * width, (h + 1) * width), slice(h * span, (h + 1) * span)
        carry = jnp.zeros((span, width), jnp.float32)
        for n in reversed(range(blocks)):
            rn = slice(n * SPAN, (n + 1) * SPAN)
            g, v = gb[rn, lv], v_ref[rn, lv]
            down, over = jnp.where(lower, dots(g, v, 1, 1), 0.0), jnp.where(upper, dots(v, g, 1, 1), 0.0)
            dqs[rn, lk] = grow[rn, lk] * (
                product(g, states[h, n], 1, 0) + product(down, kshrunk[rn, lk], 1, 0)
            )
            kpart = shrink[rn, lk] * product(over, raised[rn, lk], 1, 0)
            vpart = product(scores[h, rn, :], g, 1, 0)
            if n + 1 < blocks:
                kpart += left[rn, lk] * product(v, carry, 1, 0)
                vpart += product(kleft[rn, lk], carry, 1, 1)
            dks[rn, lk] = kpart
            dvs[rn, lv] = vpart
            carry = product(g, raised[rn, lk], 0, 0) + jnp.exp(ends[n : n + 1, lk]) * carry
        rout[h] = carry.astype(jnp.bfloat16)
        for j in range(3):
            start(s > j, rout.at[h], rin.at[s, h], r_send.at[h, j], r_recv.at[h, s], at(j, me))

    dq[...] = (dqs[...] * scale).astype(jnp.bfloat16)

    for j, other in enumerate((sy, sx, sd)):
        block = tgd.at[c, rows(other)]
        arrived(block, p_recv.at[other])
        start(None, block, block, t_send.at[j], t_recv.at[j], at(s, partner))
        arrived(moa.at[rows(other)], m_recv.at[j])
    moa[rows(s), :] = mo[...]
    for core in range(2):
        tgd[core, rows(s), :] = full[s * 2 + core]
    for j, other in enumerate((sy, sx, sd)):
        arrived(tgd.at[1 - c, rows(other)], t_recv.at[j])
    for core in range(2):
        proj[core * columns : (core + 1) * columns, :] = dots(tgd[core], moa[...], 0, 0)

    following[...] = jnp.zeros_like(following)
    for source in (3, 2, 1):

        @pl.when(s < source)
        def _():
            arrived(kept_in.at[source], k_recv.at[source])
            for h in range(heads):
                arrived(rin.at[source, h], r_recv.at[h, source])
                keep = kept_in[source, 0:1, h * width : (h + 1) * width]
                following[h] = rin[source, h].astype(jnp.float32) + keep * following[h]

    change = [None] * blocks
    for n in reversed(range(blocks)):
        rn = slice(n * SPAN, (n + 1) * SPAN)
        rest = left[rn, :] * jnp.exp(laters[n])
        kk = k_ref[rn, :].astype(jnp.float32)
        weighted = kk * rest
        for h in range(heads):
            lk, lv = slice(h * width, (h + 1) * width), slice(h * span, (h + 1) * span)
            dks[rn, lk] += rest[:, lk] * product(v_ref[rn, lv], following[h], 1, 0)
            dv[rn, lv] = (dvs[rn, lv] + product(weighted[:, lk], following[h], 1, 1)).astype(jnp.bfloat16)
        full_k = dks[rn, :]
        dk[rn, :] = full_k.astype(jnp.bfloat16)
        dqs[rn, :] = q_ref[rn, :].astype(jnp.float32) * scale * dqs[rn, :] - kk * full_k
    sums = [jnp.sum(dqs[n * SPAN : (n + 1) * SPAN, :], axis=0, keepdims=True) for n in range(blocks)]
    total = sums[0]
    for n in range(1, blocks):
        total = total + sums[n]
    sum_out[...] = jnp.broadcast_to(total, sum_out.shape)
    for j in range(3):
        start(s > j, sum_out, sum_in.at[s], u_send.at[j], u_recv.at[s], at(j, me))
    ones_up = upper.astype(jnp.float32)
    behind = jnp.zeros_like(total)
    for n in reversed(range(blocks)):
        rn = slice(n * SPAN, (n + 1) * SPAN)
        dks[rn, :] = exact(ones_up, dqs[rn, :]) + behind
        behind = behind + sums[n]
    ends[0:1, :] = jnp.zeros_like(total)
    for source in (3, 2, 1):

        @pl.when(s < source)
        def _():
            arrived(sum_in.at[source], u_recv.at[source])
            ends[0:1, :] += sum_in[source, 0:1, :]

    da[...] = dks[...] + ends[0:1, :]
    for when, parts in sent:
        if when is None:
            copy(*parts).wait_send()
        else:

            @pl.when(when)
            def _():
                copy(*parts).wait_send()


def tail(token_grad, out_proj, mixer_output, queries, key_rows, value_rows, log_decay, entry):
    tokens, columns = token_grad.shape
    heads, width, span = entry.shape
    keys = heads * width
    n_sp = lax.axis_size("sp")
    depth = out_proj.shape[0] // n_sp
    blocks = tokens // SPAN
    bf16, f32 = jnp.bfloat16, jnp.float32
    dma = pltpu.SemaphoreType.DMA
    vmem = pl.BlockSpec(memory_space=pltpu.VMEM)
    return pl.pallas_call(
        tail_kernel,
        out_shape=(
            jax.ShapeDtypeStruct((depth, columns), f32),
            jax.ShapeDtypeStruct((tokens, keys), bf16),
            jax.ShapeDtypeStruct((tokens, keys), bf16),
            jax.ShapeDtypeStruct((tokens, columns), bf16),
            jax.ShapeDtypeStruct((tokens, keys), f32),
        ),
        in_specs=[vmem] * 8,
        out_specs=(vmem,) * 5,
        scratch_shapes=[
            pltpu.VMEM((8, tokens, columns), bf16),
            pltpu.VMEM((2, n_sp * tokens, columns), bf16),
            pltpu.VMEM((n_sp * tokens, columns), bf16),
            pltpu.VMEM((tokens, columns), f32),
            pltpu.VMEM((tokens, columns), bf16),
            *[pltpu.VMEM((tokens, keys), f32) for _ in range(6)],
            pltpu.VMEM((heads, tokens, SPAN), f32),
            pltpu.VMEM((heads, blocks, span, width), f32),
            pltpu.VMEM((8, keys), f32),
            pltpu.VMEM((tokens, keys), f32),
            pltpu.VMEM((tokens, keys), f32),
            pltpu.VMEM((tokens, columns), f32),
            pltpu.VMEM((heads, span, width), bf16),
            pltpu.VMEM((n_sp, heads, span, width), bf16),
            pltpu.VMEM((heads, span, width), f32),
            pltpu.VMEM((8, keys), f32),
            pltpu.VMEM((n_sp, 8, keys), f32),
            pltpu.VMEM((8, keys), f32),
            pltpu.VMEM((n_sp, 8, keys), f32),
            dma((2, 3)),
            dma((2, 3)),
            dma((4,)),
            dma((4,)),
            dma((4,)),
            dma((4,)),
            dma((3,)),
            dma((3,)),
            dma((3,)),
            dma((3,)),
            dma((2, 3)),
            dma((2, 4)),
            dma((3,)),
            dma((4,)),
            dma((3,)),
            dma((4,)),
        ],
        compiler_params=pltpu.CompilerParams(
            collective_id=2, has_side_effects=True, vmem_limit_bytes=60 * 1024 * 1024
        ),
        name="tail",
    )(token_grad, out_proj, mixer_output, queries, key_rows, value_rows, log_decay, entry)


def front_kernel(
    cap,
    x_ref,
    g_ref,
    routes,
    weights,
    wg_hbm,
    wu_hbm,
    wd_hbm,
    out,
    x_out,
    g_out,
    gdt,
    udt,
    ht,
    wg,
    wu,
    wd,
    wgp,
    wup,
    tok,
    snd,
    xr,
    gr,
    pick,
    back_pick,
    share,
    gate,
    up,
    back,
    delta,
    other,
    tiles,
    landed,
    keep,
    zs,
    zr,
    w_sem,
    h_sem,
    z_send,
    z_recv,
    p_send,
    p_recv,
    o_send,
    o_recv,
    t_send,
    t_recv,
    d_send,
    d_recv,
    a_send,
    a_recv,
    b_send,
    b_recv,
):
    nz = 4
    s, sy, sx, sd, z, c = peers(nz)
    me, partner = z * 2 + c, z * 2 + 1 - c
    tokens, columns = x_ref.shape
    greet(
        [at(s, lax.rem(z + d, nz) * 2 + c) for d in range(1, nz)]
        + [at(sy, me), at(sx, me), at(sd, me), at(s, partner)]
    )
    sent, local = [], []
    around = (sd, sy, sx)
    rows_of = (xr, gr)

    def copy(src, dst, send, recv, device):
        return pltpu.make_async_remote_copy(
            src_ref=src, dst_ref=dst, send_sem=send, recv_sem=recv, device_id=device, device_id_type=MESH
        )

    def start(when, *parts):
        def go():
            copy(*parts).start()

        if when is None:
            go()
        else:
            pl.when(when)(go)
        sent.append((when, parts))

    def arrived(slot, recv):
        copy(slot, slot, recv, recv, at(s, partner)).wait_recv()

    def slots(index):
        return pl.ds(pl.multiple_of(index * cap, 32), cap)

    def lines(index):
        return pl.ds(pl.multiple_of(index * columns, columns), columns)

    turns = [(z, 0 * z)]
    turns.append((jnp.where(z == 0, 1, z - 1), jnp.where(z == 0, 1, 0)))
    turns.append(
        (
            jnp.where(z == 0, 2, jnp.where(z == nz - 1, z - 2, z + 1)),
            jnp.where(z == nz - 1, 0, 1),
        )
    )
    turns.append((jnp.where(z < 2, 3, 0), jnp.where(z < 2, 1, 0)))

    def hop(when, src, a, block, way):
        target = z + 1 - 2 * way
        room = (target >= 0) & (target < nz)
        start(
            room if when is None else when & room,
            src,
            tok.at[a, block],
            z_send.at[a, way, block],
            z_recv.at[a, block],
            at(s, target * 2 + c),
        )

    for way in range(2):
        hop(None, x_ref, 0, z, way)
        hop(None, g_ref, 1, z, way)
    loads = [
        pltpu.make_async_copy(src.at[0], dst, w_sem.at[i])
        for i, (src, dst) in enumerate(((wg_hbm, wg), (wu_hbm, wu), (wd_hbm, wd)))
    ]
    for one in loads:
        one.start()

    expert = lax.broadcasted_iota(jnp.int32, (8, tokens), 0)
    first, second = routes[0:1, :] == expert, routes[1:2, :] == expert
    named = jnp.where(first | second, 1.0, 0.0)
    worth = jnp.where(first, weights[0:1, :], 0.0) + jnp.where(second, weights[1:2, :], 0.0)
    earlier = lax.broadcasted_iota(jnp.int32, (tokens, tokens), 0) < lax.broadcasted_iota(
        jnp.int32, (tokens, tokens), 1
    )
    rank = dots(
        named.astype(jnp.bfloat16), jnp.where(earlier, 1.0, 0.0).astype(jnp.bfloat16), 1, 0
    )
    rank = jnp.where(named > 0.5, rank, -1.0)
    place = lax.broadcasted_iota(jnp.int32, (cap, tokens), 0).astype(jnp.float32)
    for e in range(4):
        hit = rank[e : e + 1, :] == place
        chosen = jnp.where(hit, 1.0, 0.0)
        pick[e * cap : (e + 1) * cap, :] = chosen.astype(jnp.bfloat16)
        back_pick[e] = chosen.T.astype(jnp.bfloat16)
        share[e * cap : (e + 1) * cap, :] = jnp.broadcast_to(
            jnp.sum(jnp.where(hit, worth[e : e + 1, :], 0.0), axis=1, keepdims=True), (cap, 128)
        )

    def pieces_of(src, a, e):
        rows = dots(pick[slots(e), :], src, 1, 0)
        if a:
            rows = rows * share[slots(e), 0:1]
        return rows.astype(jnp.bfloat16)

    def dispatch(i):
        block, way = turns[i]
        mine = block * 2 + c
        for a in range(2):
            if i:
                arrived(tok.at[a, block], z_recv.at[a, block])
                hop(None, tok.at[a, block], a, block, way)
        for a in range(2):
            src = (x_ref, g_ref)[a][...] if i == 0 else tok[a, block]
            for j, e in enumerate(around):
                snd[i, a, j] = pieces_of(src, a, e)
                start(
                    None,
                    snd.at[i, a, j],
                    rows_of[a].at[mine, slots(s)],
                    p_send.at[i, a, j],
                    p_recv.at[i, a, j],
                    at(e, me),
                )
            rows_of[a][mine, slots(s), :] = pieces_of(src, a, s)
            hand(i, a, 3, s)

    def hand(i, a, j, row):
        spot = rows_of[a].at[turns[i][0] * 2 + c, slots(row)]
        start(None, spot, spot, o_send.at[i, a, j], o_recv.at[i, a, j], at(s, partner))

    def receive(i):
        for a in range(2):
            for j, e in enumerate(around):
                arrived(rows_of[a].at[turns[i][0] * 2 + c, slots(e)], p_recv.at[i, a, j])
                hand(i, a, j, e)

    def compute(i, side):
        block = turns[i][0] * 2 + (1 - c if side else c)
        if side:
            for a in range(2):
                for j, e in enumerate(around + (s,)):
                    arrived(rows_of[a].at[block, slots(e)], o_recv.at[i, a, j])
        sums = (
            dots(xr[block], wg[lines(block), :], 1, 0),
            dots(xr[block], wu[lines(block), :], 1, 0),
            dots(gr[block], wd[:, lines(block)], 1, 1),
        )
        for total, part in zip((gate, up, back), sums):
            if i == 0 and side == 0:
                total[...] = part
            else:
                total[...] += part
        for a, (src, dst) in enumerate(((xr, x_out), (gr, g_out))):
            made = pltpu.make_async_copy(src.at[block], dst.at[block], h_sem.at[i, side, a])
            made.start()
            local.append(made)

    dispatch(0)
    for one in loads:
        one.wait()
    for k in range(nz):
        for i, (src, dst) in enumerate(((wg, wgp), (wu, wup))):
            start(
                None, src.at[lines(k * 2 + 1 - c)], dst.at[k], t_send.at[i, k], t_recv.at[i, k], at(s, partner)
            )
    for i in range(1, nz):
        dispatch(i)
        receive(i - 1)
        compute(i - 1, 0)
        compute(i - 1, 1)
    receive(nz - 1)
    compute(nz - 1, 0)
    compute(nz - 1, 1)

    gate_pre, up_pre, grad = gate[...], up[...], back[...]
    sigmoid_gate = jax.nn.sigmoid(gate_pre)
    activated = gate_pre * sigmoid_gate
    gate_delta = grad * up_pre * sigmoid_gate * (1.0 + gate_pre * (1.0 - sigmoid_gate))
    up_delta = grad * activated
    delta[0] = gate_delta.astype(jnp.bfloat16)
    delta[1] = up_delta.astype(jnp.bfloat16)
    gate[...] = gate_delta
    up[...] = up_delta
    back[...] = activated * up_pre
    for i in range(2):
        start(None, delta.at[i], other.at[i], d_send.at[i], d_recv.at[i], at(s, partner))
    gdt[...] = gate[...].T.astype(jnp.bfloat16)
    udt[...] = up[...].T.astype(jnp.bfloat16)
    ht[...] = back[...].T.astype(jnp.bfloat16)
    for k in range(nz):
        for i, dst in enumerate((wgp, wup)):
            arrived(dst.at[k], t_recv.at[i, k])
    for i in range(2):
        arrived(other.at[i], d_recv.at[i])

    order = list(range(1, nz)) + [0]

    def target(k):
        return lax.rem(z + k, nz)

    def produce(i):
        column = target(order[i])
        here = lines(column * 2 + c)
        pairs = (
            (delta.at[0], wg[here, :]),
            (delta.at[1], wu[here, :]),
            (other.at[0], wgp[column]),
            (other.at[1], wup[column]),
        )
        for j, e in enumerate(around + (s,)):
            tile = None
            for left, right in pairs:
                part = dots(left[slots(e), :], right, 1, 1)
                tile = part if tile is None else tile + part
            if j < 3:
                tiles[i, j] = tile.astype(jnp.bfloat16)
                start(
                    None,
                    tiles.at[i, j],
                    landed.at[i, slots(s)],
                    a_send.at[i, j],
                    a_recv.at[i, j],
                    at(e, me),
                )
            else:
                landed[i, slots(s), :] = tile.astype(jnp.bfloat16)

    def collect(i):
        k = order[i]
        for j, e in enumerate(around):
            arrived(landed.at[i, slots(e)], a_recv.at[i, j])
        total = None
        for e in range(4):
            part = dots(back_pick[e], landed[i, e * cap : (e + 1) * cap, :], 1, 0)
            total = part if total is None else total + part
        if k:
            zs[k - 1] = total.astype(jnp.bfloat16)
            start(
                None,
                zs.at[k - 1],
                zr.at[k - 1],
                b_send.at[k - 1],
                b_recv.at[k - 1],
                at(s, target(k) * 2 + c),
            )
        else:
            keep[...] = total

    produce(0)
    for i in range(1, nz):
        produce(i)
        collect(i - 1)
    collect(nz - 1)
    total = g_ref[...].astype(jnp.float32) + keep[...]
    for k in range(1, nz):
        arrived(zr.at[k - 1], b_recv.at[k - 1])
        total = total + zr[k - 1].astype(jnp.float32)
    out[...] = total.astype(jnp.bfloat16)
    for one in local:
        one.wait()
    for when, parts in sent:
        if when is None:
            copy(*parts).wait_send()
        else:

            @pl.when(when)
            def _():
                copy(*parts).wait_send()


def front(layer_input, out_cotangent, routes, route_weights, gate_proj, up_proj, down_proj):
    tokens, columns = layer_input.shape
    width, hidden = gate_proj.shape[1:]
    tp = width // columns
    cap = 5 * routes.shape[1] * tokens // (4 * lax.axis_size("sp"))
    total = 4 * cap
    bf16, f32 = jnp.bfloat16, jnp.float32
    dma = pltpu.SemaphoreType.DMA
    vmem = pl.BlockSpec(memory_space=pltpu.VMEM)
    anywhere = pl.BlockSpec(memory_space=pl.ANY)
    rows = jax.ShapeDtypeStruct((tp, total, columns), bf16)
    wide = jax.ShapeDtypeStruct((hidden, total), bf16)
    return pl.pallas_call(
        functools.partial(front_kernel, cap),
        out_shape=(jax.ShapeDtypeStruct((tokens, columns), bf16), rows, rows, wide, wide, wide),
        in_specs=[vmem] * 4 + [anywhere] * 3,
        out_specs=(vmem, anywhere, anywhere, vmem, vmem, vmem),
        scratch_shapes=[
            pltpu.VMEM((width, hidden), bf16),
            pltpu.VMEM((width, hidden), bf16),
            pltpu.VMEM((hidden, width), bf16),
            pltpu.VMEM((4, columns, hidden), bf16),
            pltpu.VMEM((4, columns, hidden), bf16),
            pltpu.VMEM((2, 4, tokens, columns), bf16),
            pltpu.VMEM((4, 2, 3, cap, columns), bf16),
            pltpu.VMEM((tp, total, columns), bf16),
            pltpu.VMEM((tp, total, columns), bf16),
            pltpu.VMEM((total, tokens), bf16),
            pltpu.VMEM((4, tokens, cap), bf16),
            pltpu.VMEM((total, 128), f32),
            pltpu.VMEM((total, hidden), f32),
            pltpu.VMEM((total, hidden), f32),
            pltpu.VMEM((total, hidden), f32),
            pltpu.VMEM((2, total, hidden), bf16),
            pltpu.VMEM((2, total, hidden), bf16),
            pltpu.VMEM((4, 3, cap, columns), bf16),
            pltpu.VMEM((4, total, columns), bf16),
            pltpu.VMEM((tokens, columns), f32),
            pltpu.VMEM((3, tokens, columns), bf16),
            pltpu.VMEM((3, tokens, columns), bf16),
            dma((3,)),
            dma((4, 2, 2)),
            dma((2, 2, 4)),
            dma((2, 4)),
            dma((4, 2, 3)),
            dma((4, 2, 3)),
            dma((4, 2, 4)),
            dma((4, 2, 4)),
            dma((2, 4)),
            dma((2, 4)),
            dma((2,)),
            dma((2,)),
            dma((4, 3)),
            dma((4, 3)),
            dma((3,)),
            dma((3,)),
        ],
        compiler_params=pltpu.CompilerParams(
            collective_id=0, has_side_effects=True, vmem_limit_bytes=60 * 1024 * 1024
        ),
        name="front",
    )(layer_input, out_cotangent, routes.T, route_weights.T, gate_proj, up_proj, down_proj)


def weight_kernel(x_ref, g_ref, gdt, udt, ht, gate_out, up_out, down_out):
    x, pair = x_ref[0], g_ref[0]
    gate_out[...] = dots(gdt[...], x, 1, 0).T.astype(jnp.bfloat16)
    up_out[...] = dots(udt[...], x, 1, 0).T.astype(jnp.bfloat16)
    down_out[...] = dots(ht[...], pair, 1, 0).astype(jnp.bfloat16)


def weight_grads(x, g, gdt, udt, ht):
    tp, rows, columns = x.shape
    hidden = gdt.shape[0]
    tall = jax.ShapeDtypeStruct((tp * columns, hidden), jnp.bfloat16)
    wide = jax.ShapeDtypeStruct((hidden, tp * columns), jnp.bfloat16)
    row_spec = pl.BlockSpec((columns, hidden), lambda t: (t, 0))
    token = pl.BlockSpec((1, rows, columns), lambda t: (t, 0, 0))
    return pl.pallas_call(
        weight_kernel,
        grid=(tp,),
        out_shape=(tall, tall, wide),
        in_specs=[token, token] + [fixed_spec(gdt.shape)] * 3,
        out_specs=[row_spec, row_spec, pl.BlockSpec((hidden, columns), lambda t: (0, t))],
        cost_estimate=pl.CostEstimate(
            flops=6 * rows * hidden * tp * columns, bytes_accessed=4 * x.size, transcendentals=0
        ),
        name="weight_grads",
    )(x, g, gdt, udt, ht)


def dense_experts(layer_input, out_cotangent, routes, route_weights, gate_proj, up_proj, down_proj):
    token_grad, x, g, gdt, udt, ht = front(
        layer_input, out_cotangent, routes, route_weights, gate_proj, up_proj, down_proj
    )
    grads = weight_grads(x, g, gdt, udt, ht)
    return [part[None] for part in grads], token_grad, None


def routed_experts(
    layer_input, out_cotangent, routes, route_weights, gate_proj, up_proj, down_proj
):
    experts = gate_proj.shape[0] * lax.axis_size("sp")
    capacity = 5 * routes.shape[1] * routes.shape[0] // (4 * experts)
    columns = layer_input.shape[1]
    placed, weighted = route_tables(routes, route_weights, experts, capacity)
    input_slots = (
        jnp.einsum(
            "tp,td->pd",
            placed.astype(jnp.bfloat16),
            layer_input,
            preferred_element_type=jnp.float32,
        )
        .astype(jnp.bfloat16)
        .reshape(experts, capacity, columns)
    )
    grad_slots = (
        jnp.einsum(
            "tp,td->pd", weighted, out_cotangent.astype(jnp.float32), precision=PRECISION_LEVEL
        )
        .astype(jnp.bfloat16)
        .reshape(experts, capacity, columns)
    )
    sent = (
        lax.all_to_all(input_slots, "sp", split_axis=0, concat_axis=1, tiled=True),
        lax.all_to_all(grad_slots, "sp", split_axis=0, concat_axis=1, tiled=True),
    )
    inputs = lax.all_gather(sent[0], "tp", axis=2, tiled=True)
    pair_grad = lax.all_gather(sent[1], "tp", axis=2, tiled=True)
    gate_part, up_part, down_part, gate_delta, up_delta = expert_backward(
        inputs, pair_grad, gate_proj, up_proj, down_proj
    )
    input_grad = input_rows(gate_delta, up_delta, gate_proj, up_proj)
    share = lax.psum_scatter(
        input_grad.astype(jnp.bfloat16), "tp", scatter_dimension=2, tiled=True
    ).astype(jnp.float32)
    returned = lax.all_to_all(
        share.astype(jnp.bfloat16), "sp", split_axis=1, concat_axis=0, tiled=True
    ).astype(share.dtype)
    slot_grads = returned.reshape(experts * capacity, columns)
    moe_grad = jnp.einsum("tp,pd->td", placed, slot_grads, precision=PRECISION_LEVEL)
    token_grad = (out_cotangent.astype(jnp.float32) + moe_grad).astype(jnp.bfloat16)
    parts = [part.astype(jnp.bfloat16) for part in (gate_part, up_part, down_part)]
    return parts, token_grad, None


def body(
    layer_input,
    out_cotangent,
    routes,
    route_weights,
    gate_proj,
    up_proj,
    down_proj,
    out_proj,
    mixer_output,
    queries,
    key_rows,
    value_rows,
    log_decay,
    entry_state,
):
    args = (layer_input, out_cotangent, routes, route_weights, gate_proj, up_proj, down_proj)
    paired = lax.axis_size("sp") == 4 and lax.axis_size("tp") % 2 == 0
    square = paired and lax.axis_size("tp") == 8 and gate_proj.shape[0] == 1
    square = square and log_decay.shape[1] == routes.shape[0]
    if square:
        parts, token_grad, kept = dense_experts(*args)
    else:
        parts, token_grad, kept = routed_experts(*args)
    if square:
        outs = tail(
            token_grad,
            out_proj,
            mixer_output,
            queries,
            key_rows,
            value_rows,
            log_decay,
            entry_state[0],
        )
        return (*parts, *outs)
    full_grad = lax.all_gather(token_grad, "tp", axis=1, tiled=True)
    partial = jnp.einsum(
        "td,tc->dc", full_grad, mixer_output, preferred_element_type=jnp.float32
    ).astype(jnp.bfloat16)
    partial, full_grad = lax.optimization_barrier((partial, full_grad))
    proj_grad = lax.psum_scatter(partial, "sp", scatter_dimension=0, tiled=True).astype(jnp.float32)
    mix_grad = jnp.dot(full_grad, out_proj, preferred_element_type=jnp.float32).astype(jnp.bfloat16)
    query_grad, key_grad, value_grad, decay_grad = mixer_backward(
        queries, key_rows, value_rows, log_decay, entry_state[0], mix_grad, kept
    )
    return (
        *parts,
        proj_grad,
        query_grad,
        key_grad,
        value_grad,
        decay_grad,
    )


def solution(mesh):
    return jax.shard_map(
        body,
        mesh=mesh,
        in_specs=(
            P("sp", "tp"),
            P("sp", "tp"),
            P("sp", None),
            P("sp", None),
            P("sp", None, "tp"),
            P("sp", None, "tp"),
            P("sp", "tp", None),
            P(None, "tp"),
            P("sp", "tp"),
            P("sp", "tp"),
            P("sp", "tp"),
            P("sp", "tp"),
            P("sp", "tp"),
            P("sp", "tp", None, None),
        ),
        out_specs=(
            P("sp", None, "tp"),
            P("sp", None, "tp"),
            P("sp", "tp", None),
            P("sp", "tp"),
            P("sp", "tp"),
            P("sp", "tp"),
            P("sp", "tp"),
            P("sp", "tp"),
        ),
        check_vma=False,
    )
```

```python
import functools

import jax
import jax.numpy as jnp
from jax import lax
from jax.experimental import pallas as pl
from jax.experimental.pallas import tpu as pltpu
from jax.sharding import PartitionSpec as P

SPAN = 64
MESH = pl.DeviceIdType.MESH


PRECISION_LEVEL = lax.Precision.HIGH


def entering(value, axis, join, neutral, kept=None):
    count = lax.axis_size(axis)
    place = lax.axis_index(axis)
    ahead = count - 1 - place
    if kept is None:
        kept = lax.all_gather(value[0].astype(jnp.bfloat16), axis)
    gathered = (kept, lax.all_gather(value[1].astype(jnp.bfloat16), axis))
    state = jax.tree.map(lambda a, e: jnp.zeros_like(a) + jnp.asarray(e, a.dtype), value, neutral)

    def one(lap, state):
        source = count - 1 - lap
        return join(
            state,
            jax.tree.map(
                lambda a, own: lax.dynamic_index_in_dim(a, source, 0, False).astype(own.dtype),
                gathered,
                value,
            ),
        )

    return lax.fori_loop(0, ahead, one, state)


def prefix(value, axis, join, neutral):
    count, mine = (lax.axis_size(axis), lax.axis_index(axis))
    pieces = lax.all_gather(value, axis)
    pieces = pieces[::-1]
    mine = count - 1 - mine
    subtotal = jnp.full_like(value, 0) + jnp.asarray(neutral, value.dtype)

    def lap(position, subtotal):
        longer = join(subtotal, pieces[position])
        return jnp.where(position < mine, longer, subtotal)

    return lax.fori_loop(0, count - 1, lap, subtotal)


def route_tables(routes, route_weights, experts, capacity):
    tokens = routes.shape[0]
    top_count = routes.shape[1]
    pair_ids = routes.reshape(-1)
    expert_ids = jnp.arange(experts, dtype=jnp.int32)
    onehot = (pair_ids[:, None] == expert_ids[None, :]).astype(jnp.int32)
    slot_rank = jnp.sum((jnp.cumsum(onehot, axis=0) - onehot) * onehot, axis=1)
    target = pair_ids * capacity + slot_rank
    slot_ids = jnp.arange(experts * capacity, dtype=jnp.int32)
    slot_hits = (
        (target[:, None] == slot_ids[None, :])
        .astype(jnp.float32)
        .reshape(tokens, top_count, experts * capacity)
    )
    placed = jnp.sum(slot_hits, axis=1)
    weighted = jnp.einsum("tk,tkp->tp", route_weights, slot_hits, precision=PRECISION_LEVEL)
    return (placed, weighted)


def expert_backward(inputs, pair_grad, gate_proj, up_proj, down_proj):
    gate_pre = jnp.einsum("erd,edf->erf", inputs, gate_proj, preferred_element_type=jnp.float32)
    up_pre = jnp.einsum("erd,edf->erf", inputs, up_proj, preferred_element_type=jnp.float32)
    sigmoid_gate = jax.nn.sigmoid(gate_pre)
    activated = gate_pre * sigmoid_gate
    hidden = (activated * up_pre).astype(jnp.bfloat16)
    down_grad = jnp.einsum("erf,erd->efd", hidden, pair_grad, preferred_element_type=jnp.float32)
    hidden_grad = jnp.einsum(
        "erd,efd->erf", pair_grad, down_proj, preferred_element_type=jnp.float32
    )
    gate_delta = (
        hidden_grad * up_pre * sigmoid_gate * (1.0 + gate_pre * (1.0 - sigmoid_gate))
    ).astype(jnp.bfloat16)
    up_delta = (hidden_grad * activated).astype(jnp.bfloat16)
    gate_grad = jnp.einsum("erd,erf->edf", inputs, gate_delta, preferred_element_type=jnp.float32)
    up_grad = jnp.einsum("erd,erf->edf", inputs, up_delta, preferred_element_type=jnp.float32)
    return (gate_grad, up_grad, down_grad, gate_delta, up_delta)


def input_rows(gate_delta, up_delta, gate_weight, up_weight):
    input_grad = jnp.einsum(
        "erf,edf->erd", gate_delta, gate_weight, preferred_element_type=jnp.float32
    )
    return input_grad + jnp.einsum(
        "erf,edf->erd", up_delta, up_weight, preferred_element_type=jnp.float32
    )


def state_combine(prior_steps, later):
    return (prior_steps[0] * later[0], later[1] + later[0][:, :, None] * prior_steps[1])


def add_combine(prior_steps, later):
    return prior_steps + later


def mixer_backward(queries, key_rows, value_rows, log_decay, entry, mix_grad, kept=None):
    tokens = queries.shape[0]
    heads = entry.shape[0]
    key_width = entry.shape[1]
    value_width = entry.shape[2]
    blocks = tokens // SPAN
    causal = jnp.tril(jnp.ones((SPAN, SPAN), dtype=bool))

    def split(rows, width):
        return rows.astype(jnp.float32).reshape(blocks, SPAN, heads, width)

    scaled_q = split(queries, key_width) * key_width ** (-0.5)
    key_segment = split(key_rows, key_width)
    value_segment = split(value_rows, value_width)
    decays = split(log_decay, key_width)
    output_gradient = split(mix_grad, value_width)
    value_dots = jnp.where(
        causal[None, None],
        jnp.einsum("nthv,nshv->nhts", output_gradient, value_segment, precision=PRECISION_LEVEL),
        0.0,
    )

    def forward_block(passed_state, block_data):
        query_now, current_key, current_value, decay_now, current_gradient, dots_now = block_data
        running_decay = jnp.cumsum(decay_now, axis=0)
        growth_multiplier = jnp.exp(running_decay)
        block_overall_sum = running_decay[-1]
        state_contribution = growth_multiplier * jnp.einsum(
            "gxb,xqb->gxq", current_gradient, passed_state, precision=PRECISION_LEVEL
        )
        inside = growth_multiplier * jnp.einsum(
            "hts,shk->thk",
            dots_now,
            current_key * jnp.exp(-running_decay),
            precision=PRECISION_LEVEL,
        )
        state_update = jnp.einsum(
            "rsx,rse->sxe",
            current_key * jnp.exp(block_overall_sum - running_decay),
            current_value,
            precision=PRECISION_LEVEL,
        )
        return (
            jnp.exp(block_overall_sum)[:, :, None] * passed_state + state_update,
            state_contribution + inside,
        )

    def reverse_block(passed_state, block_data):
        query_now, current_key, current_value, decay_now, current_gradient, dots_now = block_data
        running_decay = jnp.cumsum(decay_now, axis=0)
        shrink = jnp.exp(-running_decay)
        block_overall_sum = running_decay[-1]
        decay_remaining = jnp.exp(block_overall_sum - running_decay)
        query_raised = query_now * jnp.exp(running_decay)
        key_portion = decay_remaining * jnp.einsum(
            "gxb,xqb->gxq", current_value, passed_state, precision=PRECISION_LEVEL
        )
        key_portion = key_portion + shrink * jnp.einsum(
            "hts,thk->shk", dots_now, query_raised, precision=PRECISION_LEVEL
        )
        scores = jnp.where(
            causal[None],
            jnp.einsum(
                "thk,shk->hts", query_raised, current_key * shrink, precision=PRECISION_LEVEL
            ),
            0.0,
        )
        value_portion = jnp.einsum(
            "qgy,gye->qge", current_key * decay_remaining, passed_state, precision=PRECISION_LEVEL
        )
        value_portion = value_portion + jnp.einsum(
            "hts,thv->shv", scores, current_gradient, precision=PRECISION_LEVEL
        )
        prior_steps = (
            jnp.einsum("rsx,rse->sxe", query_raised, current_gradient, precision=PRECISION_LEVEL)
            + jnp.exp(block_overall_sum)[:, :, None] * passed_state
        )
        return (prior_steps, (key_portion, value_portion))

    block_inputs = (scaled_q, key_segment, value_segment, decays, output_gradient, value_dots)
    _, query_part = lax.scan(forward_block, entry, block_inputs)
    empty_state = jnp.zeros((heads, key_width, value_width), dtype=jnp.float32)
    local_start, (key_portion, value_portion) = lax.scan(
        reverse_block, empty_state, block_inputs, reverse=True
    )
    scaled_flat = scaled_q.reshape(tokens, heads, key_width)
    key_flattened = key_segment.reshape(tokens, heads, key_width)
    value_flattened = value_segment.reshape(tokens, heads, value_width)
    query_flat = query_part.reshape(tokens, heads, key_width)
    local_key = key_portion.reshape(tokens, heads, key_width)
    running_decay = jnp.cumsum(decays.reshape(tokens, heads, key_width), axis=0)
    device_total = running_decay[-1]
    decay_remaining = jnp.exp(device_total - running_decay)
    retain = jnp.exp(device_total)
    ones_head = jnp.ones((heads, key_width), dtype=jnp.float32)
    zeros_head = jnp.zeros((heads, key_width), dtype=jnp.float32)
    scanned = entering((retain, local_start), "sp", state_combine, (ones_head, empty_state), kept)
    following_state = scanned[1]
    key_full = local_key + decay_remaining * jnp.einsum(
        "gxb,xqb->gxq", value_flattened, following_state, precision=PRECISION_LEVEL
    )
    value_full = value_portion.reshape(tokens, heads, value_width)
    value_full = value_full + jnp.einsum(
        "qgy,gye->qge", key_flattened * decay_remaining, following_state, precision=PRECISION_LEVEL
    )
    change = scaled_flat * query_flat - key_flattened * key_full
    later_sum = prefix(jnp.sum(change, axis=0), "sp", add_combine, zeros_head)
    decay_grad = (lax.cumsum(change, axis=0, reverse=True) + later_sum[None]).reshape(
        tokens, heads * key_width
    )
    query_grad = (
        (query_flat * key_width ** (-0.5)).reshape(tokens, heads * key_width).astype(jnp.bfloat16)
    )
    key_grad = key_full.reshape(tokens, heads * key_width).astype(jnp.bfloat16)
    value_grad = value_full.reshape(tokens, heads * value_width).astype(jnp.bfloat16)
    return (query_grad, key_grad, value_grad, decay_grad)


def peers(nz):
    s = lax.axis_index("sp")
    t = lax.axis_index("tp")
    y, x = s // 2, s % 2
    z, c = t // 2, t % 2
    return s, (1 - y) * 2 + x, y * 2 + 1 - x, (1 - y) * 2 + 1 - x, z, c


def greet(devices):
    barrier = pltpu.get_barrier_semaphore()
    for device in devices:
        pl.semaphore_signal(barrier, inc=1, device_id=device, device_id_type=MESH)
    pl.semaphore_wait(barrier, len(devices))


def at(s, t):
    return {"sp": s, "tp": t}


def dots(left, right, left_dim, right_dim):
    return lax.dot_general(
        left, right, (((left_dim,), (right_dim,)), ((), ())), preferred_element_type=jnp.float32
    )


def pieces(value):
    if value.dtype == jnp.bfloat16:
        return (value,)
    high = value.astype(jnp.bfloat16)
    return (high, (value - high.astype(jnp.float32)).astype(jnp.bfloat16))


def product(left, right, left_dim, right_dim):
    lefts, rights = pieces(left), pieces(right)
    total = None
    for i, one in enumerate(lefts):
        for j, two in enumerate(rights):
            if i + j < 2:
                part = dots(one, two, left_dim, right_dim)
                total = part if total is None else total + part
    return total


def exact(left, right):
    return lax.dot_general(
        left,
        right,
        (((1,), (0,)), ((), ())),
        precision=lax.Precision.HIGHEST,
        preferred_element_type=jnp.float32,
    )


def triangle(lower):
    row = lax.broadcasted_iota(jnp.int32, (SPAN, SPAN), 0)
    column = lax.broadcasted_iota(jnp.int32, (SPAN, SPAN), 1)
    return row >= column if lower else row <= column


def tail_kernel(
    tg,
    wo,
    mo,
    q_ref,
    k_ref,
    v_ref,
    a_ref,
    s0,
    proj,
    dq,
    dk,
    dv,
    da,
    full,
    tgd,
    moa,
    mg,
    gb,
    grow,
    shrink,
    left,
    raised,
    kshrunk,
    kleft,
    scores,
    states,
    ends,
    dqs,
    dks,
    dvs,
    rout,
    rin,
    following,
    kept_out,
    kept_in,
    sum_out,
    sum_in,
    z_send,
    z_recv,
    p_send,
    p_recv,
    b_send,
    b_recv,
    t_send,
    t_recv,
    m_send,
    m_recv,
    r_send,
    r_recv,
    k_send,
    k_recv,
    u_send,
    u_recv,
):
    s, sy, sx, sd, z, c = peers(4)
    nz = 4
    me, partner = z * 2 + c, z * 2 + 1 - c
    tokens, columns = tg.shape
    blocks = tokens // SPAN
    heads, width, span = s0.shape[0], s0.shape[1], s0.shape[2]
    greet(
        [at(s, lax.rem(z + d, nz) * 2 + c) for d in range(1, nz)]
        + [at(sy, me), at(sx, me), at(sd, me), at(s, partner)]
    )
    sent = []

    def copy(src, dst, send, recv, device):
        return pltpu.make_async_remote_copy(
            src_ref=src, dst_ref=dst, send_sem=send, recv_sem=recv, device_id=device, device_id_type=MESH
        )

    def start(when, *parts):
        def go():
            copy(*parts).start()

        if when is None:
            go()
        else:
            pl.when(when)(go)
        sent.append((when, parts))

    def arrived(slot, recv):
        copy(slot, slot, recv, recv, at(s, partner)).wait_recv()

    half = tokens // 2

    def slot(block, core, part):
        return full.at[block * 2 + core, part * half : (part + 1) * half]

    def rows(index):
        return pl.ds(pl.multiple_of(index * tokens, tokens), tokens)

    def half_rows(index, part):
        return pl.ds(pl.multiple_of(index * tokens + part * half, half), half)

    def spread(when, src, block, part):
        start(
            when,
            src,
            slot(block, c, part),
            b_send.at[block, part],
            b_recv.at[block, part],
            at(s, partner),
        )
        ok = block != s
        start(
            ok if when is None else when & ok,
            src,
            tgd.at[c, half_rows(s, part)],
            p_send.at[block, part],
            p_recv.at[s, part],
            at(block, me),
        )

    def hop(when, src, block, way, d, part):
        step = 1 if way == 0 else -1
        room = z + step < nz if way == 0 else z + step >= 0
        start(
            room if when is None else when & room,
            src,
            slot(block, c, part),
            z_send.at[way, d, part],
            z_recv.at[way, d, part],
            at(s, (z + step) * 2 + c),
        )

    for part in range(2):
        own = tg.at[part * half : (part + 1) * half]
        hop(None, own, z, 0, 0, part)
        hop(None, own, z, 1, 0, part)
        spread(None, own, z, part)
    for j, target in enumerate((sy, sx, sd)):
        start(None, mo, moa.at[rows(s)], m_send.at[j], m_recv.at[j], at(target, me))

    lower, upper = triangle(True), triangle(False)
    ones_low = lower.astype(jnp.float32)
    scale = width ** (-0.5)
    for n in range(blocks):
        rn = slice(n * SPAN, (n + 1) * SPAN)
        running = exact(ones_low, a_ref[rn, :])
        end = running[SPAN - 1 : SPAN]
        ends[n : n + 1, :] = end
        kk = k_ref[rn, :].astype(jnp.float32)
        up, down = jnp.exp(running), jnp.exp(-running)
        rest = jnp.exp(end - running)
        grow[rn, :] = up
        shrink[rn, :] = down
        left[rn, :] = rest
        raised[rn, :] = q_ref[rn, :].astype(jnp.float32) * scale * up
        kshrunk[rn, :] = kk * down
        kleft[rn, :] = kk * rest
    later = jnp.zeros((1, ends.shape[1]), jnp.float32)
    laters = [None] * blocks
    for n in reversed(range(blocks)):
        laters[n] = later
        later = later + ends[n : n + 1, :]
    kept_out[...] = jnp.broadcast_to(jnp.exp(later), kept_out.shape)
    for h in range(heads):
        lk, lv = slice(h * width, (h + 1) * width), slice(h * span, (h + 1) * span)
        state = s0[h].T
        for n in range(blocks):
            rn = slice(n * SPAN, (n + 1) * SPAN)
            states[h, n] = state
            score = product(kshrunk[rn, lk], raised[rn, lk], 1, 1)
            scores[h, rn, :] = jnp.where(upper, score, 0.0)
            if n + 1 < blocks:
                state = jnp.exp(ends[n : n + 1, lk]) * state + product(v_ref[rn, lv], kleft[rn, lk], 0, 0)
    for j in range(3):
        start(
            s > j, kept_out, kept_in.at[s], k_send.at[j], k_recv.at[s], at(j, me)
        )

    def mix(block, core, first=False):
        index = block * 2 + core
        part = dots(
            tg[...] if first else full[index],
            wo[pl.ds(pl.multiple_of(index * columns, columns), columns), :],
            1,
            0,
        )
        if first:
            mg[...] = part
        else:
            mg[...] += part

    def crossed(block):
        for part in range(2):
            arrived(slot(block, 1 - c, part), b_recv.at[block, part])

    mix(z, c, True)
    full[me] = tg[...]
    crossed(z)
    mix(z, 1 - c)
    for d in range(1, nz):
        for way in range(2):
            block = z - d if way == 0 else z + d
            here = block >= 0 if way == 0 else block < nz

            for part in range(2):
                spot = slot(block, c, part)

                @pl.when(here)
                def _():
                    arrived(spot, z_recv.at[way, d - 1, part])

                if d < nz - 1:
                    hop(here, spot, block, way, d, part)
                spread(here, spot, block, part)

            @pl.when(here)
            def _():
                mix(block, c)
                crossed(block)
                mix(block, 1 - c)

    gb[...] = mg[...].astype(jnp.bfloat16)

    for h in range(heads):
        lk, lv = slice(h * width, (h + 1) * width), slice(h * span, (h + 1) * span)
        carry = jnp.zeros((span, width), jnp.float32)
        for n in reversed(range(blocks)):
            rn = slice(n * SPAN, (n + 1) * SPAN)
            g, v = gb[rn, lv], v_ref[rn, lv]
            down, over = jnp.where(lower, dots(g, v, 1, 1), 0.0), jnp.where(upper, dots(v, g, 1, 1), 0.0)
            dqs[rn, lk] = grow[rn, lk] * (
                product(g, states[h, n], 1, 0) + product(down, kshrunk[rn, lk], 1, 0)
            )
            kpart = shrink[rn, lk] * product(over, raised[rn, lk], 1, 0)
            vpart = product(scores[h, rn, :], g, 1, 0)
            if n + 1 < blocks:
                kpart += left[rn, lk] * product(v, carry, 1, 0)
                vpart += product(kleft[rn, lk], carry, 1, 1)
            dks[rn, lk] = kpart
            dvs[rn, lv] = vpart
            carry = product(g, raised[rn, lk], 0, 0) + jnp.exp(ends[n : n + 1, lk]) * carry
        rout[h] = carry.astype(jnp.bfloat16)
        for j in range(3):
            start(s > j, rout.at[h], rin.at[s, h], r_send.at[h, j], r_recv.at[h, s], at(j, me))

    dq[...] = (dqs[...] * scale).astype(jnp.bfloat16)

    for j, other in enumerate((sy, sx, sd)):
        block = tgd.at[c, rows(other)]
        for part in range(2):
            arrived(tgd.at[c, half_rows(other, part)], p_recv.at[other, part])
        start(None, block, block, t_send.at[j], t_recv.at[j], at(s, partner))
        arrived(moa.at[rows(other)], m_recv.at[j])
    moa[rows(s), :] = mo[...]
    for core in range(2):
        tgd[core, rows(s), :] = full[s * 2 + core]
    for j, other in enumerate((sy, sx, sd)):
        arrived(tgd.at[1 - c, rows(other)], t_recv.at[j])
    for core in range(2):
        proj[core * columns : (core + 1) * columns, :] = dots(tgd[core], moa[...], 0, 0)

    following[...] = jnp.zeros_like(following)
    for source in (3, 2, 1):

        @pl.when(s < source)
        def _():
            arrived(kept_in.at[source], k_recv.at[source])
            for h in range(heads):
                arrived(rin.at[source, h], r_recv.at[h, source])
                keep = kept_in[source, 0:1, h * width : (h + 1) * width]
                following[h] = rin[source, h].astype(jnp.float32) + keep * following[h]

    change = [None] * blocks
    for n in reversed(range(blocks)):
        rn = slice(n * SPAN, (n + 1) * SPAN)
        rest = left[rn, :] * jnp.exp(laters[n])
        kk = k_ref[rn, :].astype(jnp.float32)
        weighted = kk * rest
        for h in range(heads):
            lk, lv = slice(h * width, (h + 1) * width), slice(h * span, (h + 1) * span)
            dks[rn, lk] += rest[:, lk] * product(v_ref[rn, lv], following[h], 1, 0)
            dv[rn, lv] = (dvs[rn, lv] + product(weighted[:, lk], following[h], 1, 1)).astype(jnp.bfloat16)
        full_k = dks[rn, :]
        dk[rn, :] = full_k.astype(jnp.bfloat16)
        dqs[rn, :] = q_ref[rn, :].astype(jnp.float32) * scale * dqs[rn, :] - kk * full_k
    sums = [jnp.sum(dqs[n * SPAN : (n + 1) * SPAN, :], axis=0, keepdims=True) for n in range(blocks)]
    total = sums[0]
    for n in range(1, blocks):
        total = total + sums[n]
    sum_out[...] = jnp.broadcast_to(total, sum_out.shape)
    for j in range(3):
        start(s > j, sum_out, sum_in.at[s], u_send.at[j], u_recv.at[s], at(j, me))
    ones_up = upper.astype(jnp.float32)
    behind = jnp.zeros_like(total)
    for n in reversed(range(blocks)):
        rn = slice(n * SPAN, (n + 1) * SPAN)
        dks[rn, :] = exact(ones_up, dqs[rn, :]) + behind
        behind = behind + sums[n]
    ends[0:1, :] = jnp.zeros_like(total)
    for source in (3, 2, 1):

        @pl.when(s < source)
        def _():
            arrived(sum_in.at[source], u_recv.at[source])
            ends[0:1, :] += sum_in[source, 0:1, :]

    da[...] = dks[...] + ends[0:1, :]
    for when, parts in sent:
        if when is None:
            copy(*parts).wait_send()
        else:

            @pl.when(when)
            def _():
                copy(*parts).wait_send()


def tail(token_grad, out_proj, mixer_output, queries, key_rows, value_rows, log_decay, entry):
    tokens, columns = token_grad.shape
    heads, width, span = entry.shape
    keys = heads * width
    n_sp = lax.axis_size("sp")
    depth = out_proj.shape[0] // n_sp
    blocks = tokens // SPAN
    bf16, f32 = jnp.bfloat16, jnp.float32
    dma = pltpu.SemaphoreType.DMA
    vmem = pl.BlockSpec(memory_space=pltpu.VMEM)
    return pl.pallas_call(
        tail_kernel,
        out_shape=(
            jax.ShapeDtypeStruct((depth, columns), f32),
            jax.ShapeDtypeStruct((tokens, keys), bf16),
            jax.ShapeDtypeStruct((tokens, keys), bf16),
            jax.ShapeDtypeStruct((tokens, columns), bf16),
            jax.ShapeDtypeStruct((tokens, keys), f32),
        ),
        in_specs=[vmem] * 8,
        out_specs=(vmem,) * 5,
        scratch_shapes=[
            pltpu.VMEM((8, tokens, columns), bf16),
            pltpu.VMEM((2, n_sp * tokens, columns), bf16),
            pltpu.VMEM((n_sp * tokens, columns), bf16),
            pltpu.VMEM((tokens, columns), f32),
            pltpu.VMEM((tokens, columns), bf16),
            *[pltpu.VMEM((tokens, keys), f32) for _ in range(6)],
            pltpu.VMEM((heads, tokens, SPAN), f32),
            pltpu.VMEM((heads, blocks, span, width), f32),
            pltpu.VMEM((8, keys), f32),
            pltpu.VMEM((tokens, keys), f32),
            pltpu.VMEM((tokens, keys), f32),
            pltpu.VMEM((tokens, columns), f32),
            pltpu.VMEM((heads, span, width), bf16),
            pltpu.VMEM((n_sp, heads, span, width), bf16),
            pltpu.VMEM((heads, span, width), f32),
            pltpu.VMEM((8, keys), f32),
            pltpu.VMEM((n_sp, 8, keys), f32),
            pltpu.VMEM((8, keys), f32),
            pltpu.VMEM((n_sp, 8, keys), f32),
            dma((2, 3, 2)),
            dma((2, 3, 2)),
            dma((4, 2)),
            dma((4, 2)),
            dma((4, 2)),
            dma((4, 2)),
            dma((3,)),
            dma((3,)),
            dma((3,)),
            dma((3,)),
            dma((2, 3)),
            dma((2, 4)),
            dma((3,)),
            dma((4,)),
            dma((3,)),
            dma((4,)),
        ],
        compiler_params=pltpu.CompilerParams(
            collective_id=2, has_side_effects=True, vmem_limit_bytes=24 * 1024 * 1024
        ),
        name="tail",
    )(token_grad, out_proj, mixer_output, queries, key_rows, value_rows, log_decay, entry)


def front_kernel(
    cap,
    x_ref,
    g_ref,
    routes,
    weights,
    wg_hbm,
    wu_hbm,
    wd_hbm,
    out,
    gate_out,
    up_out,
    down_out,
    gdt,
    udt,
    ht,
    gate_grad,
    up_grad,
    down_grad,
    wg,
    wu,
    wd,
    wgp,
    wup,
    tok,
    snd,
    xr,
    gr,
    pick,
    back_pick,
    share,
    gate,
    up,
    back,
    delta,
    other,
    tiles,
    landed,
    keep,
    zs,
    zr,
    w_sem,
    h_sem,
    z_send,
    z_recv,
    y_send,
    y_recv,
    p_send,
    p_recv,
    o_send,
    o_recv,
    t_send,
    t_recv,
    d_send,
    d_recv,
    a_send,
    a_recv,
    b_send,
    b_recv,
):
    nz = 4
    s, sy, sx, sd, z, c = peers(nz)
    me, partner = z * 2 + c, z * 2 + 1 - c
    tokens, columns = x_ref.shape
    greet(
        [at(s, lax.rem(z + d, nz) * 2 + c) for d in range(1, nz)]
        + [at(sy, me), at(sx, me), at(sd, me), at(s, partner)]
    )
    sent = []
    around = (sd, sy, sx)
    rows_of = (xr, gr)

    def copy(src, dst, send, recv, device):
        return pltpu.make_async_remote_copy(
            src_ref=src, dst_ref=dst, send_sem=send, recv_sem=recv, device_id=device, device_id_type=MESH
        )

    def start(when, *parts):
        def go():
            copy(*parts).start()

        if when is None:
            go()
        else:
            pl.when(when)(go)
        sent.append((when, parts))

    def arrived(slot, recv):
        copy(slot, slot, recv, recv, at(s, partner)).wait_recv()

    def slots(index):
        return pl.ds(pl.multiple_of(index * cap, 32), cap)

    def lines(index):
        return pl.ds(pl.multiple_of(index * columns, columns), columns)

    turns = [(z, 0 * z)]
    turns.append((jnp.where(z == 0, 1, z - 1), jnp.where(z == 0, 1, 0)))
    turns.append(
        (
            jnp.where(z == 0, 2, jnp.where(z == nz - 1, z - 2, z + 1)),
            jnp.where(z == nz - 1, 0, 1),
        )
    )
    turns.append((jnp.where(z < 2, 3, 0), jnp.where(z < 2, 1, 0)))

    middle = (z > 0) & (z < nz - 1)

    def room(way):
        target = z + 1 - 2 * way
        return (target >= 0) & (target < nz)

    def hop(src, a, block, way):
        return (
            src,
            tok.at[a, block],
            z_send.at[a, way, block],
            z_recv.at[a, block],
            at(s, (z + 1 - 2 * way) * 2 + c),
        )

    def relay_hop(block, way):
        spot = gr.at[block * 2 + c, slots(sd)]
        return (spot, spot, y_send.at[way, block], y_recv.at[block], at(s, (z + 1 - 2 * way) * 2 + c))

    for way in range(2):
        start(room(way), *hop(x_ref, 0, z, way))
        start(room(way), *hop(g_ref, 1, z, way))
    loads = [
        pltpu.make_async_copy(src.at[0], dst, w_sem.at[i])
        for i, (src, dst) in enumerate(((wg_hbm, wg), (wu_hbm, wu), (wd_hbm, wd)))
    ]
    for one in loads:
        one.start()

    expert = lax.broadcasted_iota(jnp.int32, (8, tokens), 0)
    first, second = routes[0:1, :] == expert, routes[1:2, :] == expert
    named = jnp.where(first | second, 1.0, 0.0)
    worth = jnp.where(first, weights[0:1, :], 0.0) + jnp.where(second, weights[1:2, :], 0.0)
    earlier = lax.broadcasted_iota(jnp.int32, (tokens, tokens), 0) < lax.broadcasted_iota(
        jnp.int32, (tokens, tokens), 1
    )
    rank = dots(
        named.astype(jnp.bfloat16), jnp.where(earlier, 1.0, 0.0).astype(jnp.bfloat16), 1, 0
    )
    rank = jnp.where(named > 0.5, rank, -1.0)
    place = lax.broadcasted_iota(jnp.int32, (cap, tokens), 0).astype(jnp.float32)
    for e in range(4):
        hit = rank[e : e + 1, :] == place
        chosen = jnp.where(hit, 1.0, 0.0)
        pick[e * cap : (e + 1) * cap, :] = chosen.astype(jnp.bfloat16)
        back_pick[e] = chosen.T.astype(jnp.bfloat16)
        share[e * cap : (e + 1) * cap, :] = jnp.broadcast_to(
            jnp.sum(jnp.where(hit, worth[e : e + 1, :], 0.0), axis=1, keepdims=True), (cap, 128)
        )

    def pieces_of(src, a, e):
        rows = dots(pick[slots(e), :], src, 1, 0)
        if a:
            rows = rows * share[slots(e), 0:1]
        return rows.astype(jnp.bfloat16)

    def guarded(when, go):
        if when is None:
            go()
        else:
            pl.when(when)(go)

    def take(when, i, a):
        block, way = turns[i]
        parts = hop(tok.at[a, block], a, block, way)

        def go():
            arrived(tok.at[a, block], z_recv.at[a, block])
            pl.when(room(way))(lambda: copy(*parts).start())

        guarded(when, go)

    def relay(when, i):
        block, way = turns[i]
        spot = gr.at[block * 2 + c, slots(sd)]

        def go():
            if i == 0:
                arrived(spot, p_recv.at[0, 1, 0])
                for both in range(2):
                    parts = relay_hop(block, both)
                    pl.when(room(both))(lambda parts=parts: copy(*parts).start())
            else:
                arrived(spot, y_recv.at[block])
                parts = relay_hop(block, way)
                pl.when(room(way))(lambda: copy(*parts).start())
            copy(*handed(i, 1, 0, sd)).start()

        guarded(when, go)

    def dispatch(i, a):
        mine = turns[i][0] * 2 + c
        src = (x_ref, g_ref)[a][...] if i == 0 else tok[a, turns[i][0]]
        for j, e in enumerate(around):
            if i and a and j == 0:
                continue
            snd[i, a, j] = pieces_of(src, a, e)
            start(
                None,
                snd.at[i, a, j],
                rows_of[a].at[mine, slots(s)],
                p_send.at[i, a, j],
                p_recv.at[i, a, j],
                at(e, me),
            )
        rows_of[a][mine, slots(s), :] = pieces_of(src, a, s)
        hand(i, a, 3, s)

    def handed(i, a, j, row):
        spot = rows_of[a].at[turns[i][0] * 2 + c, slots(row)]
        return (spot, spot, o_send.at[i, a, j], o_recv.at[i, a, j], at(s, partner))

    def hand(i, a, j, row):
        start(None, *handed(i, a, j, row))

    for i in range(nz):
        block, way = turns[i]
        if i:
            for a in range(2):
                sent.append((room(way), hop(tok.at[a, block], a, block, way)))
        for one in range(2) if i == 0 else (way,):
            sent.append((room(one), relay_hop(block, one)))
        sent.append((None, handed(i, 1, 0, sd)))

    def receive(i, a):
        for j, e in enumerate(around):
            if a and j == 0:
                continue
            arrived(rows_of[a].at[turns[i][0] * 2 + c, slots(e)], p_recv.at[i, a, j])
            hand(i, a, j, e)

    def compute(i, side, a):
        block = turns[i][0] * 2 + (1 - c if side else c)
        if side:
            for j, e in enumerate(around + (s,)):
                arrived(rows_of[a].at[block, slots(e)], o_recv.at[i, a, j])
        if a:
            sums = ((back, dots(gr[block], wd[:, lines(block)], 1, 1)),)
        else:
            sums = tuple(
                (total, dots(xr[block], w[lines(block), :], 1, 0)) for total, w in ((gate, wg), (up, wu))
            )
        for total, part in sums:
            if i == 0 and side == 0:
                total[...] = part
            else:
                total[...] += part

    def finish_block(i):
        for a in range(2):
            receive(i, a)
            compute(i, 0, a)
            compute(i, 1, a)

    dispatch(0, 0)
    dispatch(0, 1)
    for one in loads:
        one.wait()
    for k in range(nz):
        for i, (src, dst) in enumerate(((wg, wgp), (wu, wup))):
            start(
                None, src.at[lines(k * 2 + 1 - c)], dst.at[k], t_send.at[i, k], t_recv.at[i, k], at(s, partner)
            )
    ends = jnp.logical_not(middle)
    for a in range(2):
        take(None, 1, a)
        dispatch(1, a)
    for a in range(2):
        take(middle, 2, a)
    relay(None, 0)
    finish_block(0)
    for a in range(2):
        take(ends, 2, a)
        dispatch(2, a)
    for a in range(2):
        take(middle, 3, a)
    relay(None, 1)
    finish_block(1)
    for a in range(2):
        take(ends, 3, a)
        dispatch(3, a)
    relay(None, 2)
    relay(middle, 3)
    finish_block(2)
    relay(ends, 3)
    finish_block(3)

    gate_pre, up_pre, grad = gate[...], up[...], back[...]
    sigmoid_gate = jax.nn.sigmoid(gate_pre)
    activated = gate_pre * sigmoid_gate
    gate_delta = grad * up_pre * sigmoid_gate * (1.0 + gate_pre * (1.0 - sigmoid_gate))
    up_delta = grad * activated
    delta[0] = gate_delta.astype(jnp.bfloat16)
    delta[1] = up_delta.astype(jnp.bfloat16)
    gate[...] = gate_delta
    up[...] = up_delta
    back[...] = activated * up_pre
    for i in range(2):
        start(None, delta.at[i], other.at[i], d_send.at[i], d_recv.at[i], at(s, partner))
    gdt[...] = gate[...].T.astype(jnp.bfloat16)
    udt[...] = up[...].T.astype(jnp.bfloat16)
    ht[...] = back[...].T.astype(jnp.bfloat16)
    for k in range(nz):
        for i, dst in enumerate((wgp, wup)):
            arrived(dst.at[k], t_recv.at[i, k])
    for i in range(2):
        arrived(other.at[i], d_recv.at[i])

    order = list(range(1, nz)) + [0]

    def target(k):
        return lax.rem(z + k, nz)

    def produce(i):
        column = target(order[i])
        here = lines(column * 2 + c)
        pairs = (
            (delta.at[0], wg[here, :]),
            (delta.at[1], wu[here, :]),
            (other.at[0], wgp[column]),
            (other.at[1], wup[column]),
        )
        for j, e in enumerate(around + (s,)):
            tile = None
            for left, right in pairs:
                part = dots(left[slots(e), :], right, 1, 1)
                tile = part if tile is None else tile + part
            if j < 3:
                tiles[i, j] = tile.astype(jnp.bfloat16)
                start(
                    None,
                    tiles.at[i, j],
                    landed.at[i, slots(s)],
                    a_send.at[i, j],
                    a_recv.at[i, j],
                    at(e, me),
                )
            else:
                landed[i, slots(s), :] = tile.astype(jnp.bfloat16)

    def collect(i):
        k = order[i]
        for j, e in enumerate(around):
            arrived(landed.at[i, slots(e)], a_recv.at[i, j])
        total = None
        for e in range(4):
            part = dots(back_pick[e], landed[i, e * cap : (e + 1) * cap, :], 1, 0)
            total = part if total is None else total + part
        if k:
            zs[k - 1] = total.astype(jnp.bfloat16)
            start(
                None,
                zs.at[k - 1],
                zr.at[k - 1],
                b_send.at[k - 1],
                b_recv.at[k - 1],
                at(s, target(k) * 2 + c),
            )
        else:
            keep[...] = total

    def saves(block):
        return (
            (gate_grad.at[lines(block), :], gate_out.at[lines(block), :], h_sem.at[0, block]),
            (up_grad.at[lines(block), :], up_out.at[lines(block), :], h_sem.at[1, block]),
            (down_grad.at[block], down_out.at[:, lines(block)], h_sem.at[2, block]),
        )

    def weigh(block, _):
        x, pair = xr[block], gr[block]
        gate_grad[lines(block), :] = dots(gdt[...], x, 1, 0).T.astype(jnp.bfloat16)
        up_grad[lines(block), :] = dots(udt[...], x, 1, 0).T.astype(jnp.bfloat16)
        down_grad[block] = dots(ht[...], pair, 1, 0).astype(jnp.bfloat16)
        for one in saves(block):
            pltpu.make_async_copy(*one).start()
        return 0

    for i in range(nz):
        produce(i)
    for i in range(nz):
        lax.fori_loop(2 * i, 2 * i + 2, weigh, 0)
        collect(i)
    total = g_ref[...].astype(jnp.float32) + keep[...]
    for k in range(1, nz):
        arrived(zr.at[k - 1], b_recv.at[k - 1])
        total = total + zr[k - 1].astype(jnp.float32)
    out[...] = total.astype(jnp.bfloat16)
    for block in range(2 * nz):
        for one in saves(block):
            pltpu.make_async_copy(*one).wait()
    for when, parts in sent:
        if when is None:
            copy(*parts).wait_send()
        else:

            @pl.when(when)
            def _():
                copy(*parts).wait_send()


def front(layer_input, out_cotangent, routes, route_weights, gate_proj, up_proj, down_proj):
    tokens, columns = layer_input.shape
    width, hidden = gate_proj.shape[1:]
    tp = width // columns
    cap = 5 * routes.shape[1] * tokens // (4 * lax.axis_size("sp"))
    total = 4 * cap
    bf16, f32 = jnp.bfloat16, jnp.float32
    dma = pltpu.SemaphoreType.DMA
    vmem = pl.BlockSpec(memory_space=pltpu.VMEM)
    anywhere = pl.BlockSpec(memory_space=pl.ANY)
    return pl.pallas_call(
        functools.partial(front_kernel, cap),
        out_shape=(
            jax.ShapeDtypeStruct((tokens, columns), bf16),
            jax.ShapeDtypeStruct((width, hidden), bf16),
            jax.ShapeDtypeStruct((width, hidden), bf16),
            jax.ShapeDtypeStruct((hidden, width), bf16),
        ),
        in_specs=[vmem] * 4 + [anywhere] * 3,
        out_specs=(vmem, anywhere, anywhere, anywhere),
        scratch_shapes=[
            pltpu.VMEM((hidden, total), bf16),
            pltpu.VMEM((hidden, total), bf16),
            pltpu.VMEM((hidden, total), bf16),
            pltpu.VMEM((width, hidden), bf16),
            pltpu.VMEM((width, hidden), bf16),
            pltpu.VMEM((tp, hidden, columns), bf16),
            pltpu.VMEM((width, hidden), bf16),
            pltpu.VMEM((width, hidden), bf16),
            pltpu.VMEM((hidden, width), bf16),
            pltpu.VMEM((4, columns, hidden), bf16),
            pltpu.VMEM((4, columns, hidden), bf16),
            pltpu.VMEM((2, 4, tokens, columns), bf16),
            pltpu.VMEM((4, 2, 3, cap, columns), bf16),
            pltpu.VMEM((tp, total, columns), bf16),
            pltpu.VMEM((tp, total, columns), bf16),
            pltpu.VMEM((total, tokens), bf16),
            pltpu.VMEM((4, tokens, cap), bf16),
            pltpu.VMEM((total, 128), f32),
            pltpu.VMEM((total, hidden), f32),
            pltpu.VMEM((total, hidden), f32),
            pltpu.VMEM((total, hidden), f32),
            pltpu.VMEM((2, total, hidden), bf16),
            pltpu.VMEM((2, total, hidden), bf16),
            pltpu.VMEM((4, 3, cap, columns), bf16),
            pltpu.VMEM((4, total, columns), bf16),
            pltpu.VMEM((tokens, columns), f32),
            pltpu.VMEM((3, tokens, columns), bf16),
            pltpu.VMEM((3, tokens, columns), bf16),
            dma((3,)),
            dma((3, 8)),
            dma((2, 2, 4)),
            dma((2, 4)),
            dma((2, 4)),
            dma((4,)),
            dma((4, 2, 3)),
            dma((4, 2, 3)),
            dma((4, 2, 4)),
            dma((4, 2, 4)),
            dma((2, 4)),
            dma((2, 4)),
            dma((2,)),
            dma((2,)),
            dma((4, 3)),
            dma((4, 3)),
            dma((3,)),
            dma((3,)),
        ],
        compiler_params=pltpu.CompilerParams(
            collective_id=0, has_side_effects=True, vmem_limit_bytes=52 * 1024 * 1024
        ),
        name="front",
    )(layer_input, out_cotangent, routes.T, route_weights.T, gate_proj, up_proj, down_proj)


def finish_kernel(*refs):
    count = len(refs) // 2
    sems = refs[-1]
    moves = [
        pltpu.make_async_copy(src, dst, sems.at[n])
        for n, (src, dst) in enumerate(zip(refs[:count], refs[count : 2 * count]))
    ]
    for one in moves:
        one.start()
    for one in moves:
        one.wait()


def finish(*arrays):
    anywhere = pl.BlockSpec(memory_space=pl.ANY)
    return pl.pallas_call(
        finish_kernel,
        out_shape=tuple(jax.ShapeDtypeStruct(one.shape, one.dtype) for one in arrays),
        in_specs=[pl.BlockSpec(memory_space=pltpu.VMEM)] * len(arrays),
        out_specs=(anywhere,) * len(arrays),
        scratch_shapes=[pltpu.SemaphoreType.DMA((len(arrays),))],
        compiler_params=pltpu.CompilerParams(vmem_limit_bytes=16 * 1024 * 1024),
        name="finish",
    )(*arrays)


def routed_experts(
    layer_input, out_cotangent, routes, route_weights, gate_proj, up_proj, down_proj
):
    experts = gate_proj.shape[0] * lax.axis_size("sp")
    capacity = 5 * routes.shape[1] * routes.shape[0] // (4 * experts)
    columns = layer_input.shape[1]
    placed, weighted = route_tables(routes, route_weights, experts, capacity)
    input_slots = (
        jnp.einsum(
            "tp,td->pd",
            placed.astype(jnp.bfloat16),
            layer_input,
            preferred_element_type=jnp.float32,
        )
        .astype(jnp.bfloat16)
        .reshape(experts, capacity, columns)
    )
    grad_slots = (
        jnp.einsum(
            "tp,td->pd", weighted, out_cotangent.astype(jnp.float32), precision=PRECISION_LEVEL
        )
        .astype(jnp.bfloat16)
        .reshape(experts, capacity, columns)
    )
    sent = (
        lax.all_to_all(input_slots, "sp", split_axis=0, concat_axis=1, tiled=True),
        lax.all_to_all(grad_slots, "sp", split_axis=0, concat_axis=1, tiled=True),
    )
    inputs = lax.all_gather(sent[0], "tp", axis=2, tiled=True)
    pair_grad = lax.all_gather(sent[1], "tp", axis=2, tiled=True)
    gate_part, up_part, down_part, gate_delta, up_delta = expert_backward(
        inputs, pair_grad, gate_proj, up_proj, down_proj
    )
    input_grad = input_rows(gate_delta, up_delta, gate_proj, up_proj)
    share = lax.psum_scatter(
        input_grad.astype(jnp.bfloat16), "tp", scatter_dimension=2, tiled=True
    ).astype(jnp.float32)
    returned = lax.all_to_all(
        share.astype(jnp.bfloat16), "sp", split_axis=1, concat_axis=0, tiled=True
    ).astype(share.dtype)
    slot_grads = returned.reshape(experts * capacity, columns)
    moe_grad = jnp.einsum("tp,pd->td", placed, slot_grads, precision=PRECISION_LEVEL)
    token_grad = (out_cotangent.astype(jnp.float32) + moe_grad).astype(jnp.bfloat16)
    parts = [part.astype(jnp.bfloat16) for part in (gate_part, up_part, down_part)]
    return parts, token_grad, None


def body(
    layer_input,
    out_cotangent,
    routes,
    route_weights,
    gate_proj,
    up_proj,
    down_proj,
    out_proj,
    mixer_output,
    queries,
    key_rows,
    value_rows,
    log_decay,
    entry_state,
):
    args = (layer_input, out_cotangent, routes, route_weights, gate_proj, up_proj, down_proj)
    paired = lax.axis_size("sp") == 4 and lax.axis_size("tp") % 2 == 0
    square = paired and lax.axis_size("tp") == 8 and gate_proj.shape[0] == 1
    square = square and log_decay.shape[1] == routes.shape[0]
    if square:
        token_grad, *parts = front(*args)
    else:
        parts, token_grad, kept = routed_experts(*args)
    if square:
        outs = tail(
            token_grad,
            out_proj,
            mixer_output,
            queries,
            key_rows,
            value_rows,
            log_decay,
            entry_state[0],
        )
        outs = finish(*parts, *outs)
        return (*[part[None] for part in outs[:3]], *outs[3:])
    full_grad = lax.all_gather(token_grad, "tp", axis=1, tiled=True)
    partial = jnp.einsum(
        "td,tc->dc", full_grad, mixer_output, preferred_element_type=jnp.float32
    ).astype(jnp.bfloat16)
    partial, full_grad = lax.optimization_barrier((partial, full_grad))
    proj_grad = lax.psum_scatter(partial, "sp", scatter_dimension=0, tiled=True).astype(jnp.float32)
    mix_grad = jnp.dot(full_grad, out_proj, preferred_element_type=jnp.float32).astype(jnp.bfloat16)
    query_grad, key_grad, value_grad, decay_grad = mixer_backward(
        queries, key_rows, value_rows, log_decay, entry_state[0], mix_grad, kept
    )
    return (
        *parts,
        proj_grad,
        query_grad,
        key_grad,
        value_grad,
        decay_grad,
    )


def solution(mesh):
    return jax.shard_map(
        body,
        mesh=mesh,
        in_specs=(
            P("sp", "tp"),
            P("sp", "tp"),
            P("sp", None),
            P("sp", None),
            P("sp", None, "tp"),
            P("sp", None, "tp"),
            P("sp", "tp", None),
            P(None, "tp"),
            P("sp", "tp"),
            P("sp", "tp"),
            P("sp", "tp"),
            P("sp", "tp"),
            P("sp", "tp"),
            P("sp", "tp", None, None),
        ),
        out_specs=(
            P("sp", None, "tp"),
            P("sp", None, "tp"),
            P("sp", "tp", None),
            P("sp", "tp"),
            P("sp", "tp"),
            P("sp", "tp"),
            P("sp", "tp"),
            P("sp", "tp"),
        ),
        check_vma=False,
    )
```

```python
import functools

import jax
import jax.numpy as jnp
from jax import lax
from jax.experimental import pallas as pl
from jax.experimental.pallas import tpu as pltpu
from jax.sharding import PartitionSpec as P

SPAN = 64
MESH = pl.DeviceIdType.MESH


PRECISION_LEVEL = lax.Precision.HIGH


def entering(value, axis, join, neutral, kept=None):
    count = lax.axis_size(axis)
    place = lax.axis_index(axis)
    ahead = count - 1 - place
    if kept is None:
        kept = lax.all_gather(value[0].astype(jnp.bfloat16), axis)
    gathered = (kept, lax.all_gather(value[1].astype(jnp.bfloat16), axis))
    state = jax.tree.map(lambda a, e: jnp.zeros_like(a) + jnp.asarray(e, a.dtype), value, neutral)

    def one(lap, state):
        source = count - 1 - lap
        return join(
            state,
            jax.tree.map(
                lambda a, own: lax.dynamic_index_in_dim(a, source, 0, False).astype(own.dtype),
                gathered,
                value,
            ),
        )

    return lax.fori_loop(0, ahead, one, state)


def prefix(value, axis, join, neutral):
    count, mine = (lax.axis_size(axis), lax.axis_index(axis))
    pieces = lax.all_gather(value, axis)
    pieces = pieces[::-1]
    mine = count - 1 - mine
    subtotal = jnp.full_like(value, 0) + jnp.asarray(neutral, value.dtype)

    def lap(position, subtotal):
        longer = join(subtotal, pieces[position])
        return jnp.where(position < mine, longer, subtotal)

    return lax.fori_loop(0, count - 1, lap, subtotal)


def route_tables(routes, route_weights, experts, capacity):
    tokens = routes.shape[0]
    top_count = routes.shape[1]
    pair_ids = routes.reshape(-1)
    expert_ids = jnp.arange(experts, dtype=jnp.int32)
    onehot = (pair_ids[:, None] == expert_ids[None, :]).astype(jnp.int32)
    slot_rank = jnp.sum((jnp.cumsum(onehot, axis=0) - onehot) * onehot, axis=1)
    target = pair_ids * capacity + slot_rank
    slot_ids = jnp.arange(experts * capacity, dtype=jnp.int32)
    slot_hits = (
        (target[:, None] == slot_ids[None, :])
        .astype(jnp.float32)
        .reshape(tokens, top_count, experts * capacity)
    )
    placed = jnp.sum(slot_hits, axis=1)
    weighted = jnp.einsum("tk,tkp->tp", route_weights, slot_hits, precision=PRECISION_LEVEL)
    return (placed, weighted)


def expert_backward(inputs, pair_grad, gate_proj, up_proj, down_proj):
    gate_pre = jnp.einsum("erd,edf->erf", inputs, gate_proj, preferred_element_type=jnp.float32)
    up_pre = jnp.einsum("erd,edf->erf", inputs, up_proj, preferred_element_type=jnp.float32)
    sigmoid_gate = jax.nn.sigmoid(gate_pre)
    activated = gate_pre * sigmoid_gate
    hidden = (activated * up_pre).astype(jnp.bfloat16)
    down_grad = jnp.einsum("erf,erd->efd", hidden, pair_grad, preferred_element_type=jnp.float32)
    hidden_grad = jnp.einsum(
        "erd,efd->erf", pair_grad, down_proj, preferred_element_type=jnp.float32
    )
    gate_delta = (
        hidden_grad * up_pre * sigmoid_gate * (1.0 + gate_pre * (1.0 - sigmoid_gate))
    ).astype(jnp.bfloat16)
    up_delta = (hidden_grad * activated).astype(jnp.bfloat16)
    gate_grad = jnp.einsum("erd,erf->edf", inputs, gate_delta, preferred_element_type=jnp.float32)
    up_grad = jnp.einsum("erd,erf->edf", inputs, up_delta, preferred_element_type=jnp.float32)
    return (gate_grad, up_grad, down_grad, gate_delta, up_delta)


def input_rows(gate_delta, up_delta, gate_weight, up_weight):
    input_grad = jnp.einsum(
        "erf,edf->erd", gate_delta, gate_weight, preferred_element_type=jnp.float32
    )
    return input_grad + jnp.einsum(
        "erf,edf->erd", up_delta, up_weight, preferred_element_type=jnp.float32
    )


def state_combine(prior_steps, later):
    return (prior_steps[0] * later[0], later[1] + later[0][:, :, None] * prior_steps[1])


def add_combine(prior_steps, later):
    return prior_steps + later


def mixer_backward(queries, key_rows, value_rows, log_decay, entry, mix_grad, kept=None):
    tokens = queries.shape[0]
    heads = entry.shape[0]
    key_width = entry.shape[1]
    value_width = entry.shape[2]
    blocks = tokens // SPAN
    causal = jnp.tril(jnp.ones((SPAN, SPAN), dtype=bool))

    def split(rows, width):
        return rows.astype(jnp.float32).reshape(blocks, SPAN, heads, width)

    scaled_q = split(queries, key_width) * key_width ** (-0.5)
    key_segment = split(key_rows, key_width)
    value_segment = split(value_rows, value_width)
    decays = split(log_decay, key_width)
    output_gradient = split(mix_grad, value_width)
    value_dots = jnp.where(
        causal[None, None],
        jnp.einsum("nthv,nshv->nhts", output_gradient, value_segment, precision=PRECISION_LEVEL),
        0.0,
    )

    def forward_block(passed_state, block_data):
        query_now, current_key, current_value, decay_now, current_gradient, dots_now = block_data
        running_decay = jnp.cumsum(decay_now, axis=0)
        growth_multiplier = jnp.exp(running_decay)
        block_overall_sum = running_decay[-1]
        state_contribution = growth_multiplier * jnp.einsum(
            "gxb,xqb->gxq", current_gradient, passed_state, precision=PRECISION_LEVEL
        )
        inside = growth_multiplier * jnp.einsum(
            "hts,shk->thk",
            dots_now,
            current_key * jnp.exp(-running_decay),
            precision=PRECISION_LEVEL,
        )
        state_update = jnp.einsum(
            "rsx,rse->sxe",
            current_key * jnp.exp(block_overall_sum - running_decay),
            current_value,
            precision=PRECISION_LEVEL,
        )
        return (
            jnp.exp(block_overall_sum)[:, :, None] * passed_state + state_update,
            state_contribution + inside,
        )

    def reverse_block(passed_state, block_data):
        query_now, current_key, current_value, decay_now, current_gradient, dots_now = block_data
        running_decay = jnp.cumsum(decay_now, axis=0)
        shrink = jnp.exp(-running_decay)
        block_overall_sum = running_decay[-1]
        decay_remaining = jnp.exp(block_overall_sum - running_decay)
        query_raised = query_now * jnp.exp(running_decay)
        key_portion = decay_remaining * jnp.einsum(
            "gxb,xqb->gxq", current_value, passed_state, precision=PRECISION_LEVEL
        )
        key_portion = key_portion + shrink * jnp.einsum(
            "hts,thk->shk", dots_now, query_raised, precision=PRECISION_LEVEL
        )
        scores = jnp.where(
            causal[None],
            jnp.einsum(
                "thk,shk->hts", query_raised, current_key * shrink, precision=PRECISION_LEVEL
            ),
            0.0,
        )
        value_portion = jnp.einsum(
            "qgy,gye->qge", current_key * decay_remaining, passed_state, precision=PRECISION_LEVEL
        )
        value_portion = value_portion + jnp.einsum(
            "hts,thv->shv", scores, current_gradient, precision=PRECISION_LEVEL
        )
        prior_steps = (
            jnp.einsum("rsx,rse->sxe", query_raised, current_gradient, precision=PRECISION_LEVEL)
            + jnp.exp(block_overall_sum)[:, :, None] * passed_state
        )
        return (prior_steps, (key_portion, value_portion))

    block_inputs = (scaled_q, key_segment, value_segment, decays, output_gradient, value_dots)
    _, query_part = lax.scan(forward_block, entry, block_inputs)
    empty_state = jnp.zeros((heads, key_width, value_width), dtype=jnp.float32)
    local_start, (key_portion, value_portion) = lax.scan(
        reverse_block, empty_state, block_inputs, reverse=True
    )
    scaled_flat = scaled_q.reshape(tokens, heads, key_width)
    key_flattened = key_segment.reshape(tokens, heads, key_width)
    value_flattened = value_segment.reshape(tokens, heads, value_width)
    query_flat = query_part.reshape(tokens, heads, key_width)
    local_key = key_portion.reshape(tokens, heads, key_width)
    running_decay = jnp.cumsum(decays.reshape(tokens, heads, key_width), axis=0)
    device_total = running_decay[-1]
    decay_remaining = jnp.exp(device_total - running_decay)
    retain = jnp.exp(device_total)
    ones_head = jnp.ones((heads, key_width), dtype=jnp.float32)
    zeros_head = jnp.zeros((heads, key_width), dtype=jnp.float32)
    scanned = entering((retain, local_start), "sp", state_combine, (ones_head, empty_state), kept)
    following_state = scanned[1]
    key_full = local_key + decay_remaining * jnp.einsum(
        "gxb,xqb->gxq", value_flattened, following_state, precision=PRECISION_LEVEL
    )
    value_full = value_portion.reshape(tokens, heads, value_width)
    value_full = value_full + jnp.einsum(
        "qgy,gye->qge", key_flattened * decay_remaining, following_state, precision=PRECISION_LEVEL
    )
    change = scaled_flat * query_flat - key_flattened * key_full
    later_sum = prefix(jnp.sum(change, axis=0), "sp", add_combine, zeros_head)
    decay_grad = (lax.cumsum(change, axis=0, reverse=True) + later_sum[None]).reshape(
        tokens, heads * key_width
    )
    query_grad = (
        (query_flat * key_width ** (-0.5)).reshape(tokens, heads * key_width).astype(jnp.bfloat16)
    )
    key_grad = key_full.reshape(tokens, heads * key_width).astype(jnp.bfloat16)
    value_grad = value_full.reshape(tokens, heads * value_width).astype(jnp.bfloat16)
    return (query_grad, key_grad, value_grad, decay_grad)


def peers(nz):
    s = lax.axis_index("sp")
    t = lax.axis_index("tp")
    y, x = s // 2, s % 2
    z, c = t // 2, t % 2
    return s, (1 - y) * 2 + x, y * 2 + 1 - x, (1 - y) * 2 + 1 - x, z, c


def greet(devices):
    barrier = pltpu.get_barrier_semaphore()
    for device in devices:
        pl.semaphore_signal(barrier, inc=1, device_id=device, device_id_type=MESH)
    pl.semaphore_wait(barrier, len(devices))


def at(s, t):
    return {"sp": s, "tp": t}


def dots(left, right, left_dim, right_dim):
    return lax.dot_general(
        left, right, (((left_dim,), (right_dim,)), ((), ())), preferred_element_type=jnp.float32
    )


def pieces(value):
    if value.dtype == jnp.bfloat16:
        return (value,)
    high = value.astype(jnp.bfloat16)
    return (high, (value - high.astype(jnp.float32)).astype(jnp.bfloat16))


def product(left, right, left_dim, right_dim):
    lefts, rights = pieces(left), pieces(right)
    total = None
    for i, one in enumerate(lefts):
        for j, two in enumerate(rights):
            if i + j < 2:
                part = dots(one, two, left_dim, right_dim)
                total = part if total is None else total + part
    return total


def exact(left, right):
    return lax.dot_general(
        left,
        right,
        (((1,), (0,)), ((), ())),
        precision=lax.Precision.HIGHEST,
        preferred_element_type=jnp.float32,
    )


def triangle(lower):
    row = lax.broadcasted_iota(jnp.int32, (SPAN, SPAN), 0)
    column = lax.broadcasted_iota(jnp.int32, (SPAN, SPAN), 1)
    return row >= column if lower else row <= column


def tail_kernel(
    tg,
    wo,
    mo,
    q_ref,
    k_ref,
    v_ref,
    a_ref,
    s0,
    proj,
    dq,
    dk,
    dv,
    da,
    full,
    tgd,
    moa,
    mg,
    gb,
    grow,
    shrink,
    left,
    raised,
    kshrunk,
    kleft,
    scores,
    states,
    ends,
    dqs,
    dks,
    dvs,
    rout,
    rin,
    following,
    kept_out,
    kept_in,
    sum_out,
    sum_in,
    z_send,
    z_recv,
    p_send,
    p_recv,
    b_send,
    b_recv,
    t_send,
    t_recv,
    m_send,
    m_recv,
    r_send,
    r_recv,
    k_send,
    k_recv,
    u_send,
    u_recv,
):
    s, sy, sx, sd, z, c = peers(4)
    nz = 4
    me, partner = z * 2 + c, z * 2 + 1 - c
    tokens, columns = tg.shape
    blocks = tokens // SPAN
    heads, width, span = s0.shape[0], s0.shape[1], s0.shape[2]
    greet(
        [at(s, lax.rem(z + d, nz) * 2 + c) for d in range(1, nz)]
        + [at(sy, me), at(sx, me), at(sd, me), at(s, partner)]
    )
    sent = []

    def copy(src, dst, send, recv, device):
        return pltpu.make_async_remote_copy(
            src_ref=src, dst_ref=dst, send_sem=send, recv_sem=recv, device_id=device, device_id_type=MESH
        )

    def start(when, *parts):
        def go():
            copy(*parts).start()

        if when is None:
            go()
        else:
            pl.when(when)(go)
        sent.append((when, parts))

    def arrived(slot, recv):
        copy(slot, slot, recv, recv, at(s, partner)).wait_recv()

    half = tokens // 2

    def slot(block, core, part):
        return full.at[block * 2 + core, part * half : (part + 1) * half]

    def rows(index):
        return pl.ds(pl.multiple_of(index * tokens, tokens), tokens)

    def half_rows(index, part):
        return pl.ds(pl.multiple_of(index * tokens + part * half, half), half)

    def spread(when, src, block, part):
        start(
            when,
            src,
            slot(block, c, part),
            b_send.at[block, part],
            b_recv.at[block, part],
            at(s, partner),
        )
        ok = block != s
        start(
            ok if when is None else when & ok,
            src,
            tgd.at[c, half_rows(s, part)],
            p_send.at[block, part],
            p_recv.at[s, part],
            at(block, me),
        )

    def hop(when, src, block, way, d, part):
        step = 1 if way == 0 else -1
        room = z + step < nz if way == 0 else z + step >= 0
        start(
            room if when is None else when & room,
            src,
            slot(block, c, part),
            z_send.at[way, d, part],
            z_recv.at[way, d, part],
            at(s, (z + step) * 2 + c),
        )

    for part in range(2):
        own = tg.at[part * half : (part + 1) * half]
        hop(None, own, z, 0, 0, part)
        hop(None, own, z, 1, 0, part)
        spread(None, own, z, part)
    for j, target in enumerate((sy, sx, sd)):
        start(None, mo, moa.at[rows(s)], m_send.at[j], m_recv.at[j], at(target, me))

    lower, upper = triangle(True), triangle(False)
    ones_low = lower.astype(jnp.float32)
    scale = width ** (-0.5)
    for n in range(blocks):
        rn = slice(n * SPAN, (n + 1) * SPAN)
        running = exact(ones_low, a_ref[rn, :])
        end = running[SPAN - 1 : SPAN]
        ends[n : n + 1, :] = end
        kk = k_ref[rn, :].astype(jnp.float32)
        up, down = jnp.exp(running), jnp.exp(-running)
        rest = jnp.exp(end - running)
        grow[rn, :] = up
        shrink[rn, :] = down
        left[rn, :] = rest
        raised[rn, :] = q_ref[rn, :].astype(jnp.float32) * scale * up
        kshrunk[rn, :] = kk * down
        kleft[rn, :] = kk * rest
    later = jnp.zeros((1, ends.shape[1]), jnp.float32)
    laters = [None] * blocks
    for n in reversed(range(blocks)):
        laters[n] = later
        later = later + ends[n : n + 1, :]
    kept_out[...] = jnp.broadcast_to(jnp.exp(later), kept_out.shape)
    for h in range(heads):
        lk, lv = slice(h * width, (h + 1) * width), slice(h * span, (h + 1) * span)
        state = s0[h].T
        for n in range(blocks):
            rn = slice(n * SPAN, (n + 1) * SPAN)
            states[h, n] = state
            score = product(kshrunk[rn, lk], raised[rn, lk], 1, 1)
            scores[h, rn, :] = jnp.where(upper, score, 0.0)
            if n + 1 < blocks:
                state = jnp.exp(ends[n : n + 1, lk]) * state + product(v_ref[rn, lv], kleft[rn, lk], 0, 0)
    for j in range(3):
        start(
            s > j, kept_out, kept_in.at[s], k_send.at[j], k_recv.at[s], at(j, me)
        )

    def mix(block, core, first=False):
        index = block * 2 + core
        part = dots(
            tg[...] if first else full[index],
            wo[pl.ds(pl.multiple_of(index * columns, columns), columns), :],
            1,
            0,
        )
        if first:
            mg[...] = part
        else:
            mg[...] += part

    def crossed(block):
        for part in range(2):
            arrived(slot(block, 1 - c, part), b_recv.at[block, part])

    mix(z, c, True)
    full[me] = tg[...]
    crossed(z)
    mix(z, 1 - c)
    for d in range(1, nz):
        for way in range(2):
            block = z - d if way == 0 else z + d
            here = block >= 0 if way == 0 else block < nz

            for part in range(2):
                spot = slot(block, c, part)

                @pl.when(here)
                def _():
                    arrived(spot, z_recv.at[way, d - 1, part])

                if d < nz - 1:
                    hop(here, spot, block, way, d, part)
                spread(here, spot, block, part)

            @pl.when(here)
            def _():
                mix(block, c)
                crossed(block)
                mix(block, 1 - c)

    gb[...] = mg[...].astype(jnp.bfloat16)

    for h in range(heads):
        lk, lv = slice(h * width, (h + 1) * width), slice(h * span, (h + 1) * span)
        carry = jnp.zeros((span, width), jnp.float32)
        for n in reversed(range(blocks)):
            rn = slice(n * SPAN, (n + 1) * SPAN)
            g, v = gb[rn, lv], v_ref[rn, lv]
            down, over = jnp.where(lower, dots(g, v, 1, 1), 0.0), jnp.where(upper, dots(v, g, 1, 1), 0.0)
            dqs[rn, lk] = grow[rn, lk] * (
                product(g, states[h, n], 1, 0) + product(down, kshrunk[rn, lk], 1, 0)
            )
            kpart = shrink[rn, lk] * product(over, raised[rn, lk], 1, 0)
            vpart = product(scores[h, rn, :], g, 1, 0)
            if n + 1 < blocks:
                kpart += left[rn, lk] * product(v, carry, 1, 0)
                vpart += product(kleft[rn, lk], carry, 1, 1)
            dks[rn, lk] = kpart
            dvs[rn, lv] = vpart
            carry = product(g, raised[rn, lk], 0, 0) + jnp.exp(ends[n : n + 1, lk]) * carry
        rout[h] = carry.astype(jnp.bfloat16)
        for j in range(3):
            start(s > j, rout.at[h], rin.at[s, h], r_send.at[h, j], r_recv.at[h, s], at(j, me))

    dq[...] = (dqs[...] * scale).astype(jnp.bfloat16)

    for j, other in enumerate((sy, sx, sd)):
        block = tgd.at[c, rows(other)]
        for part in range(2):
            arrived(tgd.at[c, half_rows(other, part)], p_recv.at[other, part])
        start(None, block, block, t_send.at[j], t_recv.at[j], at(s, partner))
        arrived(moa.at[rows(other)], m_recv.at[j])
    moa[rows(s), :] = mo[...]
    for core in range(2):
        tgd[core, rows(s), :] = full[s * 2 + core]
    for j, other in enumerate((sy, sx, sd)):
        arrived(tgd.at[1 - c, rows(other)], t_recv.at[j])
    for core in range(2):
        proj[core * columns : (core + 1) * columns, :] = dots(tgd[core], moa[...], 0, 0)

    following[...] = jnp.zeros_like(following)
    for source in (3, 2, 1):

        @pl.when(s < source)
        def _():
            arrived(kept_in.at[source], k_recv.at[source])
            for h in range(heads):
                arrived(rin.at[source, h], r_recv.at[h, source])
                keep = kept_in[source, 0:1, h * width : (h + 1) * width]
                following[h] = rin[source, h].astype(jnp.float32) + keep * following[h]

    change = [None] * blocks
    for n in reversed(range(blocks)):
        rn = slice(n * SPAN, (n + 1) * SPAN)
        rest = left[rn, :] * jnp.exp(laters[n])
        kk = k_ref[rn, :].astype(jnp.float32)
        weighted = kk * rest
        for h in range(heads):
            lk, lv = slice(h * width, (h + 1) * width), slice(h * span, (h + 1) * span)
            dks[rn, lk] += rest[:, lk] * product(v_ref[rn, lv], following[h], 1, 0)
            dv[rn, lv] = (dvs[rn, lv] + product(weighted[:, lk], following[h], 1, 1)).astype(jnp.bfloat16)
        full_k = dks[rn, :]
        dk[rn, :] = full_k.astype(jnp.bfloat16)
        dqs[rn, :] = q_ref[rn, :].astype(jnp.float32) * scale * dqs[rn, :] - kk * full_k
    sums = [jnp.sum(dqs[n * SPAN : (n + 1) * SPAN, :], axis=0, keepdims=True) for n in range(blocks)]
    total = sums[0]
    for n in range(1, blocks):
        total = total + sums[n]
    sum_out[...] = jnp.broadcast_to(total, sum_out.shape)
    for j in range(3):
        start(s > j, sum_out, sum_in.at[s], u_send.at[j], u_recv.at[s], at(j, me))
    ones_up = upper.astype(jnp.float32)
    behind = jnp.zeros_like(total)
    for n in reversed(range(blocks)):
        rn = slice(n * SPAN, (n + 1) * SPAN)
        dks[rn, :] = exact(ones_up, dqs[rn, :]) + behind
        behind = behind + sums[n]
    ends[0:1, :] = jnp.zeros_like(total)
    for source in (3, 2, 1):

        @pl.when(s < source)
        def _():
            arrived(sum_in.at[source], u_recv.at[source])
            ends[0:1, :] += sum_in[source, 0:1, :]

    da[...] = dks[...] + ends[0:1, :]
    for when, parts in sent:
        if when is None:
            copy(*parts).wait_send()
        else:

            @pl.when(when)
            def _():
                copy(*parts).wait_send()


def tail(token_grad, out_proj, mixer_output, queries, key_rows, value_rows, log_decay, entry):
    tokens, columns = token_grad.shape
    heads, width, span = entry.shape
    keys = heads * width
    n_sp = lax.axis_size("sp")
    depth = out_proj.shape[0] // n_sp
    blocks = tokens // SPAN
    bf16, f32 = jnp.bfloat16, jnp.float32
    dma = pltpu.SemaphoreType.DMA
    vmem = pl.BlockSpec(memory_space=pltpu.VMEM)
    return pl.pallas_call(
        tail_kernel,
        out_shape=(
            jax.ShapeDtypeStruct((depth, columns), f32),
            jax.ShapeDtypeStruct((tokens, keys), bf16),
            jax.ShapeDtypeStruct((tokens, keys), bf16),
            jax.ShapeDtypeStruct((tokens, columns), bf16),
            jax.ShapeDtypeStruct((tokens, keys), f32),
        ),
        in_specs=[vmem] * 8,
        out_specs=(vmem,) * 5,
        scratch_shapes=[
            pltpu.VMEM((8, tokens, columns), bf16),
            pltpu.VMEM((2, n_sp * tokens, columns), bf16),
            pltpu.VMEM((n_sp * tokens, columns), bf16),
            pltpu.VMEM((tokens, columns), f32),
            pltpu.VMEM((tokens, columns), bf16),
            *[pltpu.VMEM((tokens, keys), f32) for _ in range(6)],
            pltpu.VMEM((heads, tokens, SPAN), f32),
            pltpu.VMEM((heads, blocks, span, width), f32),
            pltpu.VMEM((8, keys), f32),
            pltpu.VMEM((tokens, keys), f32),
            pltpu.VMEM((tokens, keys), f32),
            pltpu.VMEM((tokens, columns), f32),
            pltpu.VMEM((heads, span, width), bf16),
            pltpu.VMEM((n_sp, heads, span, width), bf16),
            pltpu.VMEM((heads, span, width), f32),
            pltpu.VMEM((8, keys), f32),
            pltpu.VMEM((n_sp, 8, keys), f32),
            pltpu.VMEM((8, keys), f32),
            pltpu.VMEM((n_sp, 8, keys), f32),
            dma((2, 3, 2)),
            dma((2, 3, 2)),
            dma((4, 2)),
            dma((4, 2)),
            dma((4, 2)),
            dma((4, 2)),
            dma((3,)),
            dma((3,)),
            dma((3,)),
            dma((3,)),
            dma((2, 3)),
            dma((2, 4)),
            dma((3,)),
            dma((4,)),
            dma((3,)),
            dma((4,)),
        ],
        compiler_params=pltpu.CompilerParams(
            collective_id=2, has_side_effects=True, vmem_limit_bytes=24 * 1024 * 1024
        ),
        name="tail",
    )(token_grad, out_proj, mixer_output, queries, key_rows, value_rows, log_decay, entry)


def front_kernel(
    cap,
    x_ref,
    g_ref,
    routes,
    weights,
    wg_hbm,
    wu_hbm,
    wd_hbm,
    out,
    gate_out,
    up_out,
    down_out,
    gdt,
    udt,
    ht,
    gate_grad,
    up_grad,
    down_grad,
    wg,
    wu,
    wd,
    wgp,
    wup,
    tok,
    snd,
    xr,
    gr,
    pick,
    back_pick,
    share,
    gate,
    up,
    back,
    delta,
    other,
    tiles,
    landed,
    keep,
    zs,
    zr,
    w_sem,
    h_sem,
    z_send,
    z_recv,
    y_send,
    y_recv,
    p_send,
    p_recv,
    o_send,
    o_recv,
    t_send,
    t_recv,
    d_send,
    d_recv,
    a_send,
    a_recv,
    b_send,
    b_recv,
):
    nz = 4
    s, sy, sx, sd, z, c = peers(nz)
    me, partner = z * 2 + c, z * 2 + 1 - c
    tokens, columns = x_ref.shape
    greet(
        [at(s, lax.rem(z + d, nz) * 2 + c) for d in range(1, nz)]
        + [at(sy, me), at(sx, me), at(sd, me), at(s, partner)]
    )
    sent = []
    around = (sd, sy, sx)
    rows_of = (xr, gr)

    def copy(src, dst, send, recv, device):
        return pltpu.make_async_remote_copy(
            src_ref=src, dst_ref=dst, send_sem=send, recv_sem=recv, device_id=device, device_id_type=MESH
        )

    def start(when, *parts):
        def go():
            copy(*parts).start()

        if when is None:
            go()
        else:
            pl.when(when)(go)
        sent.append((when, parts))

    def arrived(slot, recv):
        copy(slot, slot, recv, recv, at(s, partner)).wait_recv()

    def slots(index):
        return pl.ds(pl.multiple_of(index * cap, 32), cap)

    def lines(index):
        return pl.ds(pl.multiple_of(index * columns, columns), columns)

    turns = [(z, 0 * z)]
    turns.append((jnp.where(z == 0, 1, z - 1), jnp.where(z == 0, 1, 0)))
    turns.append(
        (
            jnp.where(z == 0, 2, jnp.where(z == nz - 1, z - 2, z + 1)),
            jnp.where(z == nz - 1, 0, 1),
        )
    )
    turns.append((jnp.where(z < 2, 3, 0), jnp.where(z < 2, 1, 0)))

    middle = (z > 0) & (z < nz - 1)

    def room(way):
        target = z + 1 - 2 * way
        return (target >= 0) & (target < nz)

    def hop(src, a, block, way):
        return (
            src,
            tok.at[a, block],
            z_send.at[a, way, block],
            z_recv.at[a, block],
            at(s, (z + 1 - 2 * way) * 2 + c),
        )

    def relay_hop(block, way):
        spot = gr.at[block * 2 + c, slots(sd)]
        return (spot, spot, y_send.at[way, block], y_recv.at[block], at(s, (z + 1 - 2 * way) * 2 + c))

    for way in range(2):
        start(room(way), *hop(x_ref, 0, z, way))
        start(room(way), *hop(g_ref, 1, z, way))
    loads = [
        pltpu.make_async_copy(src.at[0], dst, w_sem.at[i])
        for i, (src, dst) in enumerate(((wg_hbm, wg), (wu_hbm, wu), (wd_hbm, wd)))
    ]
    for one in loads:
        one.start()

    expert = lax.broadcasted_iota(jnp.int32, (8, tokens), 0)
    first, second = routes[0:1, :] == expert, routes[1:2, :] == expert
    named = jnp.where(first | second, 1.0, 0.0)
    worth = jnp.where(first, weights[0:1, :], 0.0) + jnp.where(second, weights[1:2, :], 0.0)
    earlier = lax.broadcasted_iota(jnp.int32, (tokens, tokens), 0) < lax.broadcasted_iota(
        jnp.int32, (tokens, tokens), 1
    )
    rank = dots(
        named.astype(jnp.bfloat16), jnp.where(earlier, 1.0, 0.0).astype(jnp.bfloat16), 1, 0
    )
    rank = jnp.where(named > 0.5, rank, -1.0)
    place = lax.broadcasted_iota(jnp.int32, (cap, tokens), 0).astype(jnp.float32)
    for e in range(4):
        hit = rank[e : e + 1, :] == place
        chosen = jnp.where(hit, 1.0, 0.0)
        pick[e * cap : (e + 1) * cap, :] = chosen.astype(jnp.bfloat16)
        back_pick[e] = chosen.T.astype(jnp.bfloat16)
        share[e * cap : (e + 1) * cap, :] = jnp.broadcast_to(
            jnp.sum(jnp.where(hit, worth[e : e + 1, :], 0.0), axis=1, keepdims=True), (cap, 128)
        )

    def pieces_of(src, a, e):
        rows = dots(pick[slots(e), :], src, 1, 0)
        if a:
            rows = rows * share[slots(e), 0:1]
        return rows.astype(jnp.bfloat16)

    def guarded(when, go):
        if when is None:
            go()
        else:
            pl.when(when)(go)

    def take(when, i, a):
        block, way = turns[i]
        parts = hop(tok.at[a, block], a, block, way)

        def go():
            arrived(tok.at[a, block], z_recv.at[a, block])
            pl.when(room(way))(lambda: copy(*parts).start())

        guarded(when, go)

    def relay(when, i):
        block, way = turns[i]
        spot = gr.at[block * 2 + c, slots(sd)]

        def go():
            if i == 0:
                arrived(spot, p_recv.at[0, 1, 0])
                for both in range(2):
                    parts = relay_hop(block, both)
                    pl.when(room(both))(lambda parts=parts: copy(*parts).start())
            else:
                arrived(spot, y_recv.at[block])
                parts = relay_hop(block, way)
                pl.when(room(way))(lambda: copy(*parts).start())
            copy(*handed(i, 1, 0, sd)).start()

        guarded(when, go)

    def dispatch(i, a):
        mine = turns[i][0] * 2 + c
        src = (x_ref, g_ref)[a][...] if i == 0 else tok[a, turns[i][0]]
        for j, e in enumerate(around):
            if i and a and j == 0:
                continue
            snd[i, a, j] = pieces_of(src, a, e)
            start(
                None,
                snd.at[i, a, j],
                rows_of[a].at[mine, slots(s)],
                p_send.at[i, a, j],
                p_recv.at[i, a, j],
                at(e, me),
            )
        rows_of[a][mine, slots(s), :] = pieces_of(src, a, s)
        hand(i, a, 3, s)

    def handed(i, a, j, row):
        spot = rows_of[a].at[turns[i][0] * 2 + c, slots(row)]
        return (spot, spot, o_send.at[i, a, j], o_recv.at[i, a, j], at(s, partner))

    def hand(i, a, j, row):
        start(None, *handed(i, a, j, row))

    for i in range(nz):
        block, way = turns[i]
        if i:
            for a in range(2):
                sent.append((room(way), hop(tok.at[a, block], a, block, way)))
        for one in range(2) if i == 0 else (way,):
            sent.append((room(one), relay_hop(block, one)))
        sent.append((None, handed(i, 1, 0, sd)))

    def receive(i, a):
        for j, e in enumerate(around):
            if a and j == 0:
                continue
            arrived(rows_of[a].at[turns[i][0] * 2 + c, slots(e)], p_recv.at[i, a, j])
            hand(i, a, j, e)

    def compute(i, side, a):
        block = turns[i][0] * 2 + (1 - c if side else c)
        if side:
            for j, e in enumerate(around + (s,)):
                arrived(rows_of[a].at[block, slots(e)], o_recv.at[i, a, j])
        if a:
            sums = ((back, dots(gr[block], wd[:, lines(block)], 1, 1)),)
        else:
            sums = tuple(
                (total, dots(xr[block], w[lines(block), :], 1, 0)) for total, w in ((gate, wg), (up, wu))
            )
        for total, part in sums:
            if i == 0 and side == 0:
                total[...] = part
            else:
                total[...] += part

    def finish_block(i):
        for a in range(2):
            receive(i, a)
            compute(i, 0, a)
            compute(i, 1, a)

    dispatch(0, 0)
    dispatch(0, 1)
    for one in loads:
        one.wait()
    for k in range(nz):
        for i, (src, dst) in enumerate(((wg, wgp), (wu, wup))):
            start(
                None, src.at[lines(k * 2 + 1 - c)], dst.at[k], t_send.at[i, k], t_recv.at[i, k], at(s, partner)
            )
    ends = jnp.logical_not(middle)
    for a in range(2):
        take(None, 1, a)
        dispatch(1, a)
    for a in range(2):
        take(middle, 2, a)
    relay(None, 0)
    finish_block(0)
    for a in range(2):
        take(ends, 2, a)
        dispatch(2, a)
    for a in range(2):
        take(middle, 3, a)
    relay(None, 1)
    finish_block(1)
    for a in range(2):
        take(ends, 3, a)
        dispatch(3, a)
    relay(None, 2)
    relay(middle, 3)
    finish_block(2)
    relay(ends, 3)
    finish_block(3)

    gate_pre, up_pre, grad = gate[...], up[...], back[...]
    sigmoid_gate = jax.nn.sigmoid(gate_pre)
    activated = gate_pre * sigmoid_gate
    gate_delta = grad * up_pre * sigmoid_gate * (1.0 + gate_pre * (1.0 - sigmoid_gate))
    up_delta = grad * activated
    delta[0] = gate_delta.astype(jnp.bfloat16)
    delta[1] = up_delta.astype(jnp.bfloat16)
    gate[...] = gate_delta
    up[...] = up_delta
    back[...] = activated * up_pre
    for i in range(2):
        start(None, delta.at[i], other.at[i], d_send.at[i], d_recv.at[i], at(s, partner))
    gdt[...] = gate[...].T.astype(jnp.bfloat16)
    udt[...] = up[...].T.astype(jnp.bfloat16)
    ht[...] = back[...].T.astype(jnp.bfloat16)
    for k in range(nz):
        for i, dst in enumerate((wgp, wup)):
            arrived(dst.at[k], t_recv.at[i, k])
    for i in range(2):
        arrived(other.at[i], d_recv.at[i])

    order = list(range(1, nz)) + [0]

    def target(k):
        return lax.rem(z + k, nz)

    def produce(i):
        column = target(order[i])
        here = lines(column * 2 + c)
        pairs = (
            (delta.at[0], wg[here, :]),
            (delta.at[1], wu[here, :]),
            (other.at[0], wgp[column]),
            (other.at[1], wup[column]),
        )
        for j, e in enumerate(around + (s,)):
            tile = None
            for left, right in pairs:
                part = dots(left[slots(e), :], right, 1, 1)
                tile = part if tile is None else tile + part
            if j < 3:
                tiles[i, j] = tile.astype(jnp.bfloat16)
                start(
                    None,
                    tiles.at[i, j],
                    landed.at[i, slots(s)],
                    a_send.at[i, j],
                    a_recv.at[i, j],
                    at(e, me),
                )
            else:
                landed[i, slots(s), :] = tile.astype(jnp.bfloat16)

    def collect(i):
        k = order[i]
        for j, e in enumerate(around):
            arrived(landed.at[i, slots(e)], a_recv.at[i, j])
        total = None
        for e in range(4):
            part = dots(back_pick[e], landed[i, e * cap : (e + 1) * cap, :], 1, 0)
            total = part if total is None else total + part
        if k:
            zs[k - 1] = total.astype(jnp.bfloat16)
            start(
                None,
                zs.at[k - 1],
                zr.at[k - 1],
                b_send.at[k - 1],
                b_recv.at[k - 1],
                at(s, target(k) * 2 + c),
            )
        else:
            keep[...] = total

    def saves(block):
        return (
            (gate_grad.at[lines(block), :], gate_out.at[lines(block), :], h_sem.at[0, block]),
            (up_grad.at[lines(block), :], up_out.at[lines(block), :], h_sem.at[1, block]),
            (down_grad.at[block], down_out.at[:, lines(block)], h_sem.at[2, block]),
        )

    def weigh(block, _):
        x, pair = xr[block], gr[block]
        gate_grad[lines(block), :] = dots(gdt[...], x, 1, 0).T.astype(jnp.bfloat16)
        up_grad[lines(block), :] = dots(udt[...], x, 1, 0).T.astype(jnp.bfloat16)
        down_grad[block] = dots(ht[...], pair, 1, 0).astype(jnp.bfloat16)
        for one in saves(block):
            pltpu.make_async_copy(*one).start()
        return 0

    for i in range(nz):
        produce(i)
    for i in range(nz):
        lax.fori_loop(2 * i, 2 * i + 2, weigh, 0)
        collect(i)
    total = g_ref[...].astype(jnp.float32) + keep[...]
    for k in range(1, nz):
        arrived(zr.at[k - 1], b_recv.at[k - 1])
        total = total + zr[k - 1].astype(jnp.float32)
    out[...] = total.astype(jnp.bfloat16)
    for block in range(2 * nz):
        for one in saves(block):
            pltpu.make_async_copy(*one).wait()
    for when, parts in sent:
        if when is None:
            copy(*parts).wait_send()
        else:

            @pl.when(when)
            def _():
                copy(*parts).wait_send()


def front(layer_input, out_cotangent, routes, route_weights, gate_proj, up_proj, down_proj):
    tokens, columns = layer_input.shape
    width, hidden = gate_proj.shape[1:]
    tp = width // columns
    cap = 5 * routes.shape[1] * tokens // (4 * lax.axis_size("sp"))
    total = 4 * cap
    bf16, f32 = jnp.bfloat16, jnp.float32
    dma = pltpu.SemaphoreType.DMA
    vmem = pl.BlockSpec(memory_space=pltpu.VMEM)
    anywhere = pl.BlockSpec(memory_space=pl.ANY)
    return pl.pallas_call(
        functools.partial(front_kernel, cap),
        out_shape=(
            jax.ShapeDtypeStruct((tokens, columns), bf16),
            jax.ShapeDtypeStruct((width, hidden), bf16),
            jax.ShapeDtypeStruct((width, hidden), bf16),
            jax.ShapeDtypeStruct((hidden, width), bf16),
        ),
        in_specs=[vmem] * 4 + [anywhere] * 3,
        out_specs=(vmem, anywhere, anywhere, anywhere),
        scratch_shapes=[
            pltpu.VMEM((hidden, total), bf16),
            pltpu.VMEM((hidden, total), bf16),
            pltpu.VMEM((hidden, total), bf16),
            pltpu.VMEM((width, hidden), bf16),
            pltpu.VMEM((width, hidden), bf16),
            pltpu.VMEM((tp, hidden, columns), bf16),
            pltpu.VMEM((width, hidden), bf16),
            pltpu.VMEM((width, hidden), bf16),
            pltpu.VMEM((hidden, width), bf16),
            pltpu.VMEM((4, columns, hidden), bf16),
            pltpu.VMEM((4, columns, hidden), bf16),
            pltpu.VMEM((2, 4, tokens, columns), bf16),
            pltpu.VMEM((4, 2, 3, cap, columns), bf16),
            pltpu.VMEM((tp, total, columns), bf16),
            pltpu.VMEM((tp, total, columns), bf16),
            pltpu.VMEM((total, tokens), bf16),
            pltpu.VMEM((4, tokens, cap), bf16),
            pltpu.VMEM((total, 128), f32),
            pltpu.VMEM((total, hidden), f32),
            pltpu.VMEM((total, hidden), f32),
            pltpu.VMEM((total, hidden), f32),
            pltpu.VMEM((2, total, hidden), bf16),
            pltpu.VMEM((2, total, hidden), bf16),
            pltpu.VMEM((4, 3, cap, columns), bf16),
            pltpu.VMEM((4, total, columns), bf16),
            pltpu.VMEM((tokens, columns), f32),
            pltpu.VMEM((3, tokens, columns), bf16),
            pltpu.VMEM((3, tokens, columns), bf16),
            dma((3,)),
            dma((3, 8)),
            dma((2, 2, 4)),
            dma((2, 4)),
            dma((2, 4)),
            dma((4,)),
            dma((4, 2, 3)),
            dma((4, 2, 3)),
            dma((4, 2, 4)),
            dma((4, 2, 4)),
            dma((2, 4)),
            dma((2, 4)),
            dma((2,)),
            dma((2,)),
            dma((4, 3)),
            dma((4, 3)),
            dma((3,)),
            dma((3,)),
        ],
        compiler_params=pltpu.CompilerParams(
            collective_id=0, has_side_effects=True, vmem_limit_bytes=58 * 1024 * 1024
        ),
        name="front",
    )(layer_input, out_cotangent, routes.T, route_weights.T, gate_proj, up_proj, down_proj)


def finish_kernel(*refs):
    count = len(refs) // 2
    sems = refs[-1]
    moves = [
        pltpu.make_async_copy(src, dst, sems.at[n])
        for n, (src, dst) in enumerate(zip(refs[:count], refs[count : 2 * count]))
    ]
    for one in moves:
        one.start()
    for one in moves:
        one.wait()


def finish(*arrays):
    anywhere = pl.BlockSpec(memory_space=pl.ANY)
    return pl.pallas_call(
        finish_kernel,
        out_shape=tuple(jax.ShapeDtypeStruct(one.shape, one.dtype) for one in arrays),
        in_specs=[pl.BlockSpec(memory_space=pltpu.VMEM)] * len(arrays),
        out_specs=(anywhere,) * len(arrays),
        scratch_shapes=[pltpu.SemaphoreType.DMA((len(arrays),))],
        compiler_params=pltpu.CompilerParams(vmem_limit_bytes=16 * 1024 * 1024),
        name="finish",
    )(*arrays)


def routed_experts(
    layer_input, out_cotangent, routes, route_weights, gate_proj, up_proj, down_proj
):
    experts = gate_proj.shape[0] * lax.axis_size("sp")
    capacity = 5 * routes.shape[1] * routes.shape[0] // (4 * experts)
    columns = layer_input.shape[1]
    placed, weighted = route_tables(routes, route_weights, experts, capacity)
    input_slots = (
        jnp.einsum(
            "tp,td->pd",
            placed.astype(jnp.bfloat16),
            layer_input,
            preferred_element_type=jnp.float32,
        )
        .astype(jnp.bfloat16)
        .reshape(experts, capacity, columns)
    )
    grad_slots = (
        jnp.einsum(
            "tp,td->pd", weighted, out_cotangent.astype(jnp.float32), precision=PRECISION_LEVEL
        )
        .astype(jnp.bfloat16)
        .reshape(experts, capacity, columns)
    )
    sent = (
        lax.all_to_all(input_slots, "sp", split_axis=0, concat_axis=1, tiled=True),
        lax.all_to_all(grad_slots, "sp", split_axis=0, concat_axis=1, tiled=True),
    )
    inputs = lax.all_gather(sent[0], "tp", axis=2, tiled=True)
    pair_grad = lax.all_gather(sent[1], "tp", axis=2, tiled=True)
    gate_part, up_part, down_part, gate_delta, up_delta = expert_backward(
        inputs, pair_grad, gate_proj, up_proj, down_proj
    )
    input_grad = input_rows(gate_delta, up_delta, gate_proj, up_proj)
    share = lax.psum_scatter(
        input_grad.astype(jnp.bfloat16), "tp", scatter_dimension=2, tiled=True
    ).astype(jnp.float32)
    returned = lax.all_to_all(
        share.astype(jnp.bfloat16), "sp", split_axis=1, concat_axis=0, tiled=True
    ).astype(share.dtype)
    slot_grads = returned.reshape(experts * capacity, columns)
    moe_grad = jnp.einsum("tp,pd->td", placed, slot_grads, precision=PRECISION_LEVEL)
    token_grad = (out_cotangent.astype(jnp.float32) + moe_grad).astype(jnp.bfloat16)
    parts = [part.astype(jnp.bfloat16) for part in (gate_part, up_part, down_part)]
    return parts, token_grad, None


def body(
    layer_input,
    out_cotangent,
    routes,
    route_weights,
    gate_proj,
    up_proj,
    down_proj,
    out_proj,
    mixer_output,
    queries,
    key_rows,
    value_rows,
    log_decay,
    entry_state,
):
    args = (layer_input, out_cotangent, routes, route_weights, gate_proj, up_proj, down_proj)
    paired = lax.axis_size("sp") == 4 and lax.axis_size("tp") % 2 == 0
    square = paired and lax.axis_size("tp") == 8 and gate_proj.shape[0] == 1
    square = square and log_decay.shape[1] == routes.shape[0]
    if square:
        token_grad, *parts = front(*args)
    else:
        parts, token_grad, kept = routed_experts(*args)
    if square:
        outs = tail(
            token_grad,
            out_proj,
            mixer_output,
            queries,
            key_rows,
            value_rows,
            log_decay,
            entry_state[0],
        )
        outs = finish(*parts, *outs)
        return (*[part[None] for part in outs[:3]], *outs[3:])
    full_grad = lax.all_gather(token_grad, "tp", axis=1, tiled=True)
    partial = jnp.einsum(
        "td,tc->dc", full_grad, mixer_output, preferred_element_type=jnp.float32
    ).astype(jnp.bfloat16)
    partial, full_grad = lax.optimization_barrier((partial, full_grad))
    proj_grad = lax.psum_scatter(partial, "sp", scatter_dimension=0, tiled=True).astype(jnp.float32)
    mix_grad = jnp.dot(full_grad, out_proj, preferred_element_type=jnp.float32).astype(jnp.bfloat16)
    query_grad, key_grad, value_grad, decay_grad = mixer_backward(
        queries, key_rows, value_rows, log_decay, entry_state[0], mix_grad, kept
    )
    return (
        *parts,
        proj_grad,
        query_grad,
        key_grad,
        value_grad,
        decay_grad,
    )


def solution(mesh):
    return jax.shard_map(
        body,
        mesh=mesh,
        in_specs=(
            P("sp", "tp"),
            P("sp", "tp"),
            P("sp", None),
            P("sp", None),
            P("sp", None, "tp"),
            P("sp", None, "tp"),
            P("sp", "tp", None),
            P(None, "tp"),
            P("sp", "tp"),
            P("sp", "tp"),
            P("sp", "tp"),
            P("sp", "tp"),
            P("sp", "tp"),
            P("sp", "tp", None, None),
        ),
        out_specs=(
            P("sp", None, "tp"),
            P("sp", None, "tp"),
            P("sp", "tp", None),
            P("sp", "tp"),
            P("sp", "tp"),
            P("sp", "tp"),
            P("sp", "tp"),
            P("sp", "tp"),
        ),
        check_vma=False,
    )
```
